32 devices in a mesh: sp: 8 (over z, x), tp: 4 (over y, core).
Axes of the slice: x: 2, y: 2, z: 4, core: 2. Of those that a mesh axis runs over, the one named last changes fastest.
Arguments:
- stream: bfloat16 [1024, 2048], P('sp', 'tp')
- norm_gain: float32 [2048], P('tp'), may hold values from 0.1 to 1.9
- w_value: bfloat16 [2048, 512], P(None, 'tp'), may hold values from -0.125 to 0.125
- w_mix: bfloat16 [2048, 512], P(None, 'tp'), may hold values from -0.125 to 0.125
- w_gate: bfloat16 [2048, 512], P(None, 'tp'), may hold values from -0.125 to 0.125
- w_state: bfloat16 [2048, 512], P(None, 'tp'), may hold values from -0.125 to 0.125
- conv_taps: float32 [3, 512], P(None, 'tp'), may hold values from -3 to 3
- skip_gain: float32 [512], P('tp'), may hold values from -3 to 3
- decay_rate: float32 [2, 32, 64], P(None, 'tp'), as said below
- turn_rate: float32 [2, 32, 64], P(None, 'tp'), may hold values from 0.25 to 1.5
- input_real: float32 [2, 32, 64, 16], P(None, 'tp')
- input_imag: float32 [2, 32, 64, 16], P(None, 'tp')
- read_real: float32 [2, 32, 16, 64], P(None, 'tp'), may hold values from -0.75 to 0.75
- read_imag: float32 [2, 32, 16, 64], P(None, 'tp'), may hold values from -0.75 to 0.75
- initial_state: float32 [2, 2, 32, 64], P(None, None, 'tp'), may hold values from -5 to 5
- intervals: float32 [1024], P('sp'), as said below
- proj_conv: bfloat16 [512, 2048], P('tp'), may hold values from -0.1875 to 0.1875
- proj_state: bfloat16 [512, 2048], P('tp'), may hold values from -0.1875 to 0.1875
Outputs:
- mixed: bfloat16 [1024, 2048], P('sp', 'tp')
The draws below stay inside these ranges and needn't reach their ends.
Inputs may be any that keep to these rules, and one draw needn't show every extreme that they name: `decay_rate`: Positive. `intervals`: Positive.
All inputs are finite; a program needn't handle non-finite values.
Results may differ from the reference program's by a relative error of at most 0.024.
Values may be sent and summed in bfloat16 or wider, within the bound.
A program may use at most 64 MiB of HBM per device.

```python
import math
import jax
import jax.numpy as jnp
from jax import lax

D = 2048
CONV_W = 512
SSM_W = 512
GSIZE = 16
STATE = 64
MIXER_GROUPS = 32
TOK_DEV = 128
TOKEN_COUNT = 1024
N_TP = 4


def rate_table(key):
    slow_share = 0.5
    slow_flags = jax.random.uniform(jax.random.fold_in(key, 101), (2, MIXER_GROUPS, 1)) < slow_share
    quantile = jax.random.uniform(jax.random.fold_in(key, 102), (2, MIXER_GROUPS, STATE))
    slow_rates = jnp.exp(math.log(0.4) + quantile * math.log(0.9 / 0.4)) / TOKEN_COUNT
    fast_rates = jnp.exp(math.log(0.01) + quantile * math.log(1.0 / 30.0 / 0.01))
    return jnp.where(slow_flags, slow_rates, fast_rates).astype(jnp.float32)


def driven_matrix(key, salt):
    decay_rates = rate_table(key)
    normal_part = jnp.clip(jax.random.normal(jax.random.fold_in(key, salt), (2, MIXER_GROUPS, STATE, GSIZE)), -5.0, 5.0)
    return (normal_part * jnp.sqrt(decay_rates / GSIZE)[..., None]).astype(jnp.float32)


def draw_decay_rate(key, part):
    return rate_table(key)


def draw_input_real(key, part):
    return driven_matrix(key, 103)


def draw_input_imag(key, part):
    return driven_matrix(key, 104)


def draw_intervals(key, part):
    blocks = TOKEN_COUNT // TOK_DEV
    factor = jnp.exp(jax.random.uniform(jax.random.fold_in(key, 1), (blocks, 1), minval=math.log(0.5), maxval=math.log(2.0)))
    jitter = jax.random.uniform(jax.random.fold_in(key, 2), (blocks, TOK_DEV), minval=0.5, maxval=1.5)
    evenly_spaced = (factor * jitter).reshape(TOKEN_COUNT)
    spike_locations = jax.random.randint(jax.random.fold_in(key, 3), (2,), 0, TOKEN_COUNT)
    slot_indices = jnp.arange(TOKEN_COUNT)
    spike_mask = (slot_indices == spike_locations[0]) | (slot_indices == spike_locations[1])
    return jnp.where(spike_mask, 0.5 * TOKEN_COUNT, evenly_spaced).astype(jnp.float32)


def draw_stream(key, part):
    normal_part = jnp.clip(jax.random.normal(jax.random.fold_in(key, 11), (TOKEN_COUNT, D)), -5.0, 5.0)
    rise = 3.0
    row_scale = jnp.exp(jax.random.uniform(jax.random.fold_in(key, 12), (TOKEN_COUNT, 1), minval=math.log(0.3), maxval=math.log(3.0)))
    column_scale = jnp.exp(jax.random.uniform(jax.random.fold_in(key, 13), (1, D), minval=math.log(0.5), maxval=math.log(1.6)))
    column_block = (jnp.arange(D) // (D // N_TP)).astype(jnp.float32)
    trend = rise ** (column_block / max(N_TP - 1, 1))
    return (normal_part * row_scale * column_scale * trend[None, :]).astype(jnp.bfloat16)


def steps_of(key, extent, split, least, top_value):
    gain, own = 1.0, jax.random.fold_in(key, 6)
    for axis_at, parts in split:
        steps = jnp.exp(jax.random.uniform(jax.random.fold_in(own, axis_at), (parts,), jnp.float32, least / len(split), top_value / len(split)))
        gain = gain * jnp.repeat(steps, extent[axis_at] // parts).reshape([-1 if axis == axis_at else 1 for axis in range(len(extent))])
    return gain


def noise(key, shape, deviation, most, shards=(), held_as=jnp.bfloat16):
    loudness = steps_of(key, shape, shards, -0.22, 0.18) if shards else 1.0
    drawn = jax.random.normal(key, shape, jnp.float32) * deviation * loudness
    return jnp.minimum(jnp.maximum(drawn, -most), most).astype(held_as)


def setup_inputs(seed: int = 0) -> dict:
    keys = jax.random.split(jax.random.key(seed), 19)
    return {
        "stream": draw_stream(jax.random.fold_in(keys[18], 71), 0),
        "norm_gain": jnp.clip(1.0 + 0.18 * jax.random.normal(keys[1], (D,), jnp.float32), 0.1, 1.9),
        "w_value": noise(keys[2], (D, CONV_W), D ** -0.5, 0.125, ((1, 4),)),
        "w_mix": noise(keys[3], (D, CONV_W), D ** -0.5, 0.125, ((1, 4),)),
        "w_gate": noise(keys[4], (D, CONV_W), D ** -0.5, 0.125, ((1, 4),)),
        "w_state": noise(keys[5], (D, SSM_W), D ** -0.5, 0.125, ((1, 4),)),
        "conv_taps": noise(keys[6], (3, CONV_W), 0.5, 3.0, ((1, 4),), jnp.float32),
        "skip_gain": noise(keys[7], (SSM_W,), 0.5, 3.0, ((0, 4),), jnp.float32),
        "decay_rate": draw_decay_rate(jax.random.fold_in(keys[18], 71), 0),
        "turn_rate": jnp.clip(0.25 + 1.25 * jax.random.uniform(keys[9], (2, MIXER_GROUPS, STATE), jnp.float32) ** steps_of(keys[9], (2, MIXER_GROUPS, STATE), ((1, 4),), -0.2, 0.2), 0.25, 1.5),
        "input_real": draw_input_real(jax.random.fold_in(keys[18], 71), 0),
        "input_imag": draw_input_imag(jax.random.fold_in(keys[18], 71), 0),
        "read_real": noise(keys[12], (2, MIXER_GROUPS, GSIZE, STATE), STATE ** -0.5, 0.75, ((1, 4),), jnp.float32),
        "read_imag": noise(keys[13], (2, MIXER_GROUPS, GSIZE, STATE), STATE ** -0.5, 0.75, ((1, 4),), jnp.float32),
        "initial_state": noise(keys[14], (2, 2, MIXER_GROUPS, STATE), 1.0, 5.0, ((2, 4),), jnp.float32),
        "intervals": draw_intervals(jax.random.fold_in(keys[18], 71), 0),
        "proj_conv": noise(keys[16], (CONV_W, D), (CONV_W + SSM_W) ** -0.5, 0.1875, ((0, 4),)),
        "proj_state": noise(keys[17], (SSM_W, D), (CONV_W + SSM_W) ** -0.5, 0.1875, ((0, 4),)),
    }


EPSILON = 1e-06
HIGH = lax.Precision.HIGHEST

def step_factors(decay_rate, turn_rate, interval):
    damping = -decay_rate * interval
    angle = turn_rate * interval
    magnitude = jnp.exp(damping)
    factor_re = magnitude * jnp.cos(angle)
    factor_im = magnitude * jnp.sin(angle)
    half_sine = jnp.sin(0.5 * angle)
    lift_re = jnp.expm1(damping) * jnp.cos(angle) - 2.0 * half_sine * half_sine
    denominator = decay_rate * decay_rate + turn_rate * turn_rate
    gain_real = (turn_rate * factor_im - decay_rate * lift_re) / denominator
    gain_im = -(decay_rate * factor_im + turn_rate * lift_re) / denominator
    return (factor_re, factor_im, gain_real, gain_im)

def state_direction(inputs, intervals, decay_rate, turn_rate, input_real, input_imag, read_real, read_imag, start_re, start_im, backward):
    block_count = TOKEN_COUNT // TOK_DEV
    input_blocks = inputs.reshape(block_count, TOK_DEV, MIXER_GROUPS, GSIZE)
    interval_blocks = intervals.reshape(block_count, TOK_DEV)

    def advance_block(boundary, block_items):
        block_inputs, block_steps = block_items
        factor_re, factor_im, gain_real, gain_im = step_factors(decay_rate, turn_rate, block_steps[:, None, None])
        driven_re = jnp.einsum('tgh,gph->tgp', block_inputs, input_real, precision=HIGH)
        driven_im = jnp.einsum('tgh,gph->tgp', block_inputs, input_imag, precision=HIGH)
        push_re = gain_real * driven_re - gain_im * driven_im
        push_im = gain_real * driven_im + gain_im * driven_re

        def advance_position(current, step_items):
            step_re, step_im, add_re, add_im = step_items
            new_re = step_re * current[0] - step_im * current[1] + add_re
            new_im = step_re * current[1] + step_im * current[0] + add_im
            return ((new_re, new_im), (new_re, new_im))
        boundary, history = lax.scan(advance_position, boundary, (factor_re, factor_im, push_re, push_im), reverse=backward)
        reading = jnp.einsum('ghp,tgp->tgh', read_real, history[0], precision=HIGH)
        reading = reading - jnp.einsum('ghp,tgp->tgh', read_imag, history[1], precision=HIGH)
        return (boundary, reading)
    _, readings = lax.scan(advance_block, (start_re, start_im), (input_blocks, interval_blocks), reverse=backward)
    return readings.reshape(TOKEN_COUNT, MIXER_GROUPS, GSIZE)

def reference(stream, norm_gain, w_value, w_mix, w_gate, w_state, conv_taps, skip_gain, decay_rate, turn_rate, input_real, input_imag, read_real, read_imag, initial_state, intervals, proj_conv, proj_state):
    widened = stream.astype(jnp.float32)
    inv_rms = lax.rsqrt(lax.optimization_barrier(jnp.mean(widened * widened, axis=1, keepdims=True)) + EPSILON)
    normed = (widened * inv_rms * norm_gain).astype(jnp.bfloat16)
    conv_value = jnp.dot(normed, w_value, preferred_element_type=jnp.float32).astype(jnp.bfloat16)
    conv_mix = jnp.dot(normed, w_mix, preferred_element_type=jnp.float32).astype(jnp.bfloat16)
    conv_gate = jnp.dot(normed, w_gate, preferred_element_type=jnp.float32).astype(jnp.bfloat16)
    state_input = jnp.dot(normed, w_state, preferred_element_type=jnp.float32).astype(jnp.bfloat16)
    source = (conv_mix.astype(jnp.float32) * conv_value.astype(jnp.float32)).astype(jnp.bfloat16)
    padded = jnp.pad(source.astype(jnp.float32), ((1, 1), (0, 0)))
    filtered = conv_taps[0] * padded[:-2] + conv_taps[1] * padded[1:-1] + conv_taps[2] * padded[2:]
    conv_out = (conv_gate.astype(jnp.float32) * filtered).astype(jnp.bfloat16)
    state_float = state_input.astype(jnp.float32).reshape(TOKEN_COUNT, MIXER_GROUPS, GSIZE)
    responses = skip_gain.reshape(MIXER_GROUPS, GSIZE) * state_float
    for direction in range(2):
        responses = responses + state_direction(state_float, intervals, decay_rate[direction], turn_rate[direction], input_real[direction], input_imag[direction], read_real[direction], read_imag[direction], initial_state[direction, 0], initial_state[direction, 1], direction == 1)
    state_out = jax.nn.gelu(responses.reshape(TOKEN_COUNT, SSM_W)).astype(jnp.bfloat16)
    total = jnp.dot(conv_out, proj_conv, preferred_element_type=jnp.float32)
    total = total + jnp.dot(state_out, proj_state, preferred_element_type=jnp.float32)
    return total.astype(jnp.bfloat16)
```

```python
import functools

import jax
import jax.numpy as jnp
from jax import lax
from jax.experimental import pallas as pl
from jax.experimental.pallas import tpu as pltpu
from jax.sharding import PartitionSpec as P

EPSILON = 1e-06
MESH = pl.DeviceIdType.MESH
F32 = jnp.float32
BF16 = jnp.bfloat16
CHUNKS = 4


def dot(a, b):
    return jnp.dot(a, b, preferred_element_type=F32)


def dot_t(a, b):
    return lax.dot_general(a, b, (((1,), (1,)), ((), ())), preferred_element_type=F32)


def half_turns(angle):
    theta = 0.5 * angle
    n = jnp.floor(theta * 0.6366197723675814 + 0.5)
    r = theta - n * 1.5703125
    r = r - n * 0.00048351287841796875
    r = r - n * 3.1385570764541626e-07
    r = r - n * 6.077100627776710e-11
    odd = (n - 2.0 * jnp.floor(0.5 * n)) > 0.5
    z = r * r
    s = r + r * z * ((-1.9515295891e-4 * z + 8.3321608736e-3) * z - 1.6666654611e-1)
    c = 1.0 - 0.5 * z + z * z * (
        (2.443315711809948e-5 * z - 1.388731625493765e-3) * z + 4.166664568298827e-2
    )
    square = jnp.where(odd, c * c, s * s)
    double = 2.0 * s * c
    return square, jnp.where(odd, -double, double)


def expm1_of(x, e):
    p = 1.0 + x * (1.0 / 7.0)
    for k in (6.0, 5.0, 4.0, 3.0, 2.0):
        p = 1.0 + x * p * (1.0 / k)
    return jnp.where(x > -0.35, x * p, e - 1.0)


def repeat(lo, hi, body):
    if hi - lo <= 16:
        for i in range(lo, hi):
            body(i)
    else:
        def step(i, carry):
            body(i)
            return carry
        lax.fori_loop(lo, hi, step, 0)


def fold(lo, hi, body, init):
    if hi - lo <= 16:
        for i in range(lo, hi):
            init = body(i, init)
        return init
    return lax.fori_loop(lo, hi, body, init)


def kernel(
    n_sp, n_tp,
    x_hbm, gain_hbm, wv, wm, wg, ws, taps_hbm, skip_hbm, decay_hbm, turn_hbm,
    inr, ini, rdr, rdi, init_hbm, iv_hbm, pc, ps,
    out_ref,
    x_ref, gain_ref, taps_ref, skip_ref, decay_ref, turn_ref, init_ref, iv_s,
    w_all, pc_v, ps_v, in_v, rd_v, x_full, gains, el_all, fr_ref, fi_ref, gr_ref, gi_ref,
    dr_ref, di_ref, hr_ref, hi_ref, kr_ref, ki_ref, k_row, d_row, p_row,
    bt_ref, rt_ref, rc_ref, cc_ref, src_ref, halo_ref, e_out, e_all,
    span_ref, wa_ref, wb_ref, p1_out, p1_in, p2_out, p2_in, c_out, c_in, acc_ref, so_ref, so_all,
    load_sem, as_sem, ar_sem, bs_sem, br_sem, fs_sem, fwr_sem, gs_sem, grv_sem,
    is_sem, ir_sem, hs_sem, hr_sem, es_sem, er_sem, ps_sem, pr_sem, ws_sem, wr_sem, ss_sem, sr_sem, greet_sem,
):
    tp, sp = lax.axis_index("tp"), lax.axis_index("sp")
    rows, width = x_hbm.shape
    channels = wv.shape[1]
    y, core = tp // 2, tp % 2
    sib = y * 2 + 1 - core
    oth = (1 - y) * 2 + core
    diag = (1 - y) * 2 + 1 - core
    cw = width // CHUNKS

    loads = {}

    def load(name, src, dst):
        copy = pltpu.make_async_copy(src, dst, load_sem.at[len(loads)])
        copy.start()
        loads[name] = copy

    def loaded(*names):
        for name in names:
            loads[name].wait()

    def near(step, act):
        for s in (-step, step):
            @pl.when((sp + s >= 0) & (sp + s < n_sp))
            def _():
                act(sp + s)

    def near_count(step):
        return jnp.where(sp - step >= 0, 1, 0) + jnp.where(sp + step < n_sp, 1, 0)

    def greet(k):
        near(1 << k, lambda where: pl.semaphore_signal(
            greet_sem.at[k], inc=1, device_id={"sp": where}, device_id_type=MESH))

    def greeted(k):
        pl.semaphore_wait(greet_sem.at[k], near_count(1 << k))

    rounds = greet_sem.shape[0]
    barrier = pltpu.get_barrier_semaphore()
    for j in range(1, n_tp):
        pl.semaphore_signal(barrier, inc=1, device_id={"tp": (tp + j) % n_tp}, device_id_type=MESH)
    near(1, lambda where: pl.semaphore_signal(
        barrier, inc=1, device_id={"sp": where}, device_id_type=MESH))
    load("x", x_hbm, x_ref)
    load("iv", iv_hbm, iv_s)
    load("decay", decay_hbm, decay_ref)
    load("turn", turn_hbm, turn_ref)
    load("init", init_hbm, init_ref)
    load("gain", gain_hbm, gain_ref)
    load("inr", inr, in_v.at[0])
    load("ini", ini, in_v.at[1])
    load("rdr", rdr, rd_v.at[0])
    load("rdi", rdi, rd_v.at[1])
    for j, w in enumerate((wv, wm, wg, ws)):
        load("w%d" % j, w, w_all.at[:, pl.ds(j * channels, channels)])
    load("taps", taps_hbm, taps_ref)
    load("skip", skip_hbm, skip_ref)
    load("pc", pc, pc_v)
    load("ps", ps.at[:, pl.ds(pl.multiple_of(tp * width, width), width)], ps_v.at[tp])
    pl.semaphore_wait(barrier, n_tp - 1 + near_count(1))
    loaded("x")

    def remote(src, dst, send, recv, where):
        return pltpu.make_async_remote_copy(
            src_ref=src, dst_ref=dst, send_sem=send, recv_sem=recv,
            device_id=where, device_id_type=MESH)

    to_sib, to_oth, forward = [], [], []
    for c in range(CHUNKS):
        piece = x_ref.at[:, pl.ds(c * cw, cw)]
        to_oth.append(remote(piece, x_full.at[tp, c], bs_sem.at[c], br_sem.at[c], {"tp": oth}))
        to_sib.append(remote(piece, x_full.at[tp, c], as_sem.at[c], ar_sem.at[c], {"tp": sib}))
        forward.append(remote(x_full.at[oth, c], x_full.at[oth, c], fs_sem.at[c], fwr_sem.at[c],
                              {"tp": sib}))
    for c in range(CHUNKS):
        to_oth[c].start()
    for c in range(CHUNKS):
        to_sib[c].start()
    gain_copies = [
        remote(gain_hbm, gains.at[tp], gs_sem.at[j], grv_sem.at[j], {"tp": (tp + j) % n_tp})
        for j in range(1, n_tp)
    ]
    for copy in gain_copies:
        copy.start()
    greet(0)
    peers = (oth, diag, sib)
    weight_copies = [
        remote(ps.at[:, pl.ds(pl.multiple_of(peer * width, width), width)], ps_v.at[tp],
               ws_sem.at[i], wr_sem.at[i], {"tp": peer})
        for i, peer in enumerate(peers)
    ]
    for copy in weight_copies:
        copy.start()

    def pass_on(c):
        to_oth[c].wait_recv()
        forward[c].start()

    sub = lax.broadcasted_iota(jnp.int32, (8, 128), 0)
    top = sub < 4

    def pack(ref):
        even = ref[pl.ds(0, 8, stride=2), :]
        odd = ref[pl.ds(1, 8, stride=2), :]
        return jnp.concatenate([even, odd], axis=1)

    loaded("iv", "decay", "turn", "init")
    decay, turn = pack(decay_ref), pack(turn_ref)
    den = decay * decay + turn * turn
    td, dd = turn / den, decay / den

    def factors(k, carry):
        iv = jnp.where(top, iv_s[0, k], iv_s[0, rows - 1 - k])
        damp = -decay * iv
        square, sine = half_turns(turn * iv)
        e = jnp.exp(damp)
        cosine = 1.0 - 2.0 * square
        f_im = e * sine
        lift = expm1_of(damp, e) * cosine - 2.0 * square
        at = pl.ds(pl.multiple_of(k * 8, 8), 8)
        fr_ref[at, :] = e * cosine
        fi_ref[at, :] = f_im
        gr_ref[at, :] = td * f_im - dd * lift
        gi_ref[at, :] = -(dd * f_im + td * lift)
        return carry

    lax.fori_loop(0, rows, factors, 0, unroll=4)
    greeted(0)
    if rounds > 1:
        greet(1)

    def put(ref, k, value):
        ref[pl.ds(pl.multiple_of(k * 8, 8), 4), :] = value[:4]
        ref[pl.ds(pl.multiple_of((rows - 1 - k) * 8, 8) + 4, 4), :] = value[4:]

    def chain(k, carry):
        ar, ai, br, bi = carry
        at = pl.ds(pl.multiple_of(k * 8, 8), 8)
        back = pl.ds(pl.multiple_of((rows - 1 - k) * 8, 8), 8)
        fr, fi = fr_ref[at, :], fi_ref[at, :]
        ar, ai = fr * ar - fi * ai, fr * ai + fi * ar
        put(hr_ref, k, ar)
        put(hi_ref, k, ai)
        gr, gi = gr_ref[back, :], gi_ref[back, :]
        put(kr_ref, rows - 1 - k, gr * br - gi * bi)
        put(ki_ref, rows - 1 - k, gr * bi + gi * br)
        fr, fi = fr_ref[back, :], fi_ref[back, :]
        return ar, ai, fr * br - fi * bi, fr * bi + fi * br

    one, zero = jnp.ones((8, 128), F32), jnp.zeros((8, 128), F32)
    lax.fori_loop(0, rows, chain, (one, zero, one, zero), unroll=4)
    pass_on(0)
    for part, (k_ref, h_ref) in enumerate(((kr_ref, hr_ref), (ki_ref, hi_ref))):
        for j in range(8):
            lanes = slice(j * 128, (j + 1) * 128)
            k_row[part, :, lanes] = k_ref[pl.ds(j, rows, stride=8), :]
            p_row[part, :, lanes] = h_ref[pl.ds(j, rows, stride=8), :].astype(BF16)
    pass_on(1)
    if rounds > 1:
        greeted(1)
    for k in range(2, rounds):
        greet(k)
        if k < rounds - 1:
            greeted(k)

    loaded("inr", "ini", "rdr", "rdi")
    states = bt_ref.shape[2]
    per = rd_v.shape[2]
    half = states // 2
    group = channels * per // half
    spread = (lax.broadcasted_iota(jnp.int32, (per, half), 1) % per
              == lax.broadcasted_iota(jnp.int32, (per, half), 0)).astype(BF16)
    keep = ((lax.broadcasted_iota(jnp.int32, (channels, half), 1) // per)
            == (lax.broadcasted_iota(jnp.int32, (channels, half), 0) // group))
    left = lax.broadcasted_iota(jnp.int32, (group, 2 * per), 1) < per
    for part in range(2):
        for d in range(2):
            at, to = pl.ds(d * channels, channels), pl.ds(d * half, half)
            wide = dot(in_v[part, at, :].astype(BF16), spread)
            bt_ref[part, :, to] = jnp.where(keep, wide, 0.0).astype(BF16)
            wide = dot(rd_v[part, at, :].astype(BF16), spread)
            if part:
                wide = -wide
            rt_ref[part, :, to] = jnp.where(keep, wide, 0.0).astype(BF16)
            for g in range(channels // group):
                narrow = rd_v[part, pl.ds(d * channels + g * group, group), :]
                both = jnp.concatenate([narrow, narrow], axis=1)
                cc_ref[part, d, g] = jnp.where(left if g % 2 == 0 else ~left, both, 0.0)
    rc_ref[...] = jnp.zeros_like(rc_ref)

    pass_on(2)
    loaded("gain", "w0", "w1", "w2", "w3")
    for copy in gain_copies:
        copy.wait_recv()

    def project(value, gain, first):
        wide = value.astype(F32)
        scaled = (wide * gain).astype(BF16)
        k = value.shape[1]
        term = dot(scaled, w_all[pl.ds(pl.multiple_of(first, k), k), :])
        return term, jnp.sum(wide * wide, axis=1, keepdims=True)

    projected = jnp.zeros((rows, 4 * channels), F32)
    squares = jnp.zeros((rows, 1), F32)
    t, s = project(x_ref[...], gain_ref[...], tp * width)
    projected, squares = projected + t, squares + s

    def whole(owner, projected, squares):
        value = jnp.concatenate([x_full[owner, c] for c in range(CHUNKS)], axis=1)
        t, s = project(value, gains[owner], owner * width)
        return projected + t, squares + s

    for c in range(CHUNKS):
        to_sib[c].wait_recv()
    projected, squares = whole(sib, projected, squares)
    pass_on(3)
    projected, squares = whole(oth, projected, squares)
    if rounds > 2:
        greeted(rounds - 1)

    def interval_copy(r):
        return remote(iv_hbm, el_all.at[r], is_sem.at[r], ir_sem.at[r], {"sp": (sp + r) % n_sp})

    repeat(1, n_sp, lambda r: interval_copy(r).start())
    for c in range(CHUNKS):
        forward[c].wait_recv()
        t, s = project(x_full[diag, c], gains[diag][:, c * cw:(c + 1) * cw], diag * width + c * cw)
        projected, squares = projected + t, squares + s
    projected = projected * lax.rsqrt(squares / (width * n_tp) + EPSILON)
    state_input = projected[:, 3 * channels:].astype(BF16)
    conv_value = projected[:, :channels].astype(BF16).astype(F32)
    conv_mix = projected[:, channels:2 * channels].astype(BF16).astype(F32)
    conv_gate = projected[:, 2 * channels:3 * channels].astype(BF16).astype(F32)
    src_ref[...] = (conv_mix * conv_value).astype(BF16)

    for j in range(4):
        lanes = slice(j * 256, (j + 1) * 256)
        dr = dot(state_input, bt_ref[0, :, lanes])
        di = dot(state_input, bt_ref[1, :, lanes])
        d_row[0, :, lanes] = dr
        d_row[1, :, lanes] = di
        kr, ki = k_row[0, :, lanes], k_row[1, :, lanes]
        er = jnp.sum(kr * dr - ki * di, axis=0, keepdims=True)
        ei = jnp.sum(kr * di + ki * dr, axis=0, keepdims=True)
        for h in range(2):
            q = (j % 2) * 2 + h
            e_out[j // 2, q:q + 1, :] = er[:, h * 128:(h + 1) * 128]
            e_out[j // 2, 4 + q:5 + q, :] = ei[:, h * 128:(h + 1) * 128]


    def edge_copy(r):
        return remote(e_out.at[jnp.where(sp + r < n_sp, 0, 1)], e_all.at[r], es_sem.at[r],
                      er_sem.at[r], {"sp": (sp + r) % n_sp})

    halo_up = remote(src_ref.at[pl.ds(rows - 16, 16)], halo_ref.at[0], hs_sem.at[0], hr_sem.at[0],
                     {"sp": (sp + 1) % n_sp})
    halo_down = remote(src_ref.at[pl.ds(0, 16)], halo_ref.at[1], hs_sem.at[1], hr_sem.at[1],
                       {"sp": (sp + n_sp - 1) % n_sp})
    repeat(1, n_sp, lambda r: edge_copy(r).start())
    not_first, not_last = sp > 0, sp < n_sp - 1
    pl.when(not_last)(halo_up.start)
    pl.when(not_first)(halo_down.start)

    for part, ref in ((0, dr_ref), (1, di_ref)):
        for j in range(8):
            ref[pl.ds(j, rows, stride=8), :] = d_row[part, :, j * 128:(j + 1) * 128]


    def local(k, carry):
        hr, hi = carry
        at = pl.ds(pl.multiple_of(k * 8, 8), 8)
        back = pl.ds(pl.multiple_of((rows - 1 - k) * 8, 8), 8)
        dr = jnp.where(top, dr_ref[at, :], dr_ref[back, :])
        di = jnp.where(top, di_ref[at, :], di_ref[back, :])
        gr, gi = gr_ref[at, :], gi_ref[at, :]
        fr, fi = fr_ref[at, :], fi_ref[at, :]
        pr = gr * dr - gi * di
        pi = gr * di + gi * dr
        hr, hi = fr * hr + (pr - fi * hi), fr * hi + (pi + fi * hr)
        put(hr_ref, k, hr)
        put(hi_ref, k, hi)
        return hr, hi

    lax.fori_loop(0, rows, local, (zero, zero), unroll=8)
    loaded("taps", "skip", "pc", "ps")
    response = state_input.astype(F32) * skip_ref[...]
    for part, ref in ((0, hr_ref), (1, hi_ref)):
        history = jnp.concatenate(
            [ref[pl.ds(j, rows, stride=8), :].astype(BF16) for j in range(8)], axis=1)
        response = response + dot_t(history, rt_ref[part])

    pl.when(not_first)(halo_up.wait_recv)
    pl.when(not_last)(halo_down.wait_recv)
    source = src_ref[...].astype(F32)
    line = lax.broadcasted_iota(jnp.int32, (rows, channels), 0)
    before = jnp.where(not_first, halo_ref[0].astype(F32)[15:16, :], 0.0)
    after = jnp.where(not_last, halo_ref[1].astype(F32)[0:1, :], 0.0)
    previous = jnp.where(line == 0, before, pltpu.roll(source, 1, 0))
    following = jnp.where(line == rows - 1, after, pltpu.roll(source, rows - 1, 0))
    filtered = taps_ref[0:1, :] * previous + taps_ref[1:2, :] * source + taps_ref[2:3, :] * following
    conv_out = (conv_gate * filtered).astype(BF16)

    def partial(owner):
        return dot(conv_out, pc_v[:, pl.ds(pl.multiple_of(owner * width, width), width)])

    p1_out[...] = partial(diag).astype(BF16)
    first = remote(p1_out, p1_in, ps_sem.at[0], pr_sem.at[0], {"tp": sib})
    first.start()
    p2_out[...] = partial(sib).astype(BF16)
    second = remote(p2_out, p2_in, ps_sem.at[1], pr_sem.at[1], {"tp": sib})
    second.start()
    acc_ref[...] = partial(oth)

    repeat(1, n_sp, lambda r: interval_copy(r).wait_recv())

    def both_of(full, d):
        return jnp.concatenate([full[d * 4:d * 4 + 4], full[d * 4:d * 4 + 4]], axis=0)

    def init_of(d):
        parts = [
            jnp.concatenate([init_ref[pl.ds(d * 16 + part * 8, 4, stride=2), :],
                             init_ref[pl.ds(d * 16 + part * 8 + 1, 4, stride=2), :]], axis=1)
            for part in range(2)
        ]
        return jnp.concatenate(parts, axis=0)

    decays = [both_of(decay, d) for d in range(2)]
    turns = [both_of(turn, d) for d in range(2)]

    def weight(damping, turning, span):
        square, sine = half_turns(turning * span)
        e = jnp.exp(-damping * span)
        return e * (1.0 - 2.0 * square), jnp.where(top, -e * sine, e * sine)

    def apply(w, tile):
        return w[0] * tile + w[1] * pltpu.roll(tile, 4, 0)

    def elapsed(r):
        return jnp.sum(el_all[r], axis=1, keepdims=True)

    none = jnp.zeros((1, 1), F32)

    def ahead(r, carry):
        total, inside = carry
        span_ref[r] = jnp.broadcast_to(total, (1, 128))
        step = elapsed(r)
        return total + step, inside + step * jnp.where(sp - r >= 0, 1.0, 0.0)

    total, inside = fold(1, n_sp, ahead, (none, none))

    def behind(i, total):
        r = n_sp - i
        mine = sp - r >= 0
        span = jnp.where(mine, span_ref[r], jnp.broadcast_to(total, (1, 128)))
        w = weight(jnp.where(mine, decays[0], decays[1]), jnp.where(mine, turns[0], turns[1]), span)
        wa_ref[r] = w[0]
        wb_ref[r] = w[1]
        return total + elapsed(r)

    fold(1, n_sp, behind, none)
    outside = none

    def beyond(r, acc):
        return acc + elapsed(r) * jnp.where(sp - r >= 0, 0.0, 1.0)

    outside = fold(1, n_sp, beyond, none)
    h0 = apply(weight(decays[0], turns[0], inside), init_of(0))
    h1 = apply(weight(decays[1], turns[1], outside), init_of(1))

    first.wait_recv()
    c_out[...] = (acc_ref[...] + p1_in[...].astype(F32)).astype(BF16)
    cross = remote(c_out, c_in, ps_sem.at[2], pr_sem.at[2], {"tp": oth})
    cross.start()
    mine = partial(tp)
    second.wait_recv()
    acc_ref[...] = mine + p2_in[...].astype(F32)

    repeat(1, n_sp, lambda r: edge_copy(r).wait_recv())

    def combine(r, carry):
        h0, h1 = carry
        moved = apply((wa_ref[r], wb_ref[r]), e_all[r])
        mine = sp - r >= 0
        return h0 + jnp.where(mine, moved, 0.0), h1 + jnp.where(mine, 0.0, moved)

    entering = fold(1, n_sp, combine, (h0, h1))
    for d in range(2):
        for g in range(channels // group):
            q = g // 2
            hr, hi = entering[d][q:q + 1, :], entering[d][4 + q:5 + q, :]
            cr_, ci_ = cc_ref[0, d, g], cc_ref[1, d, g]
            at, lanes = pl.ds(g * group, group), pl.ds(d * half + q * 128, 128)
            rc_ref[0, at, lanes] = (cr_ * hr - ci_ * hi).astype(BF16)
            rc_ref[1, at, lanes] = (-(cr_ * hi + ci_ * hr)).astype(BF16)
    for part in range(2):
        response = response + dot_t(p_row[part], rc_ref[part])
    inner = 0.7978845608028654 * (response + 0.044715 * (response * response * response))
    state_out = (0.5 * response * (1.0 + jnp.tanh(inner))).astype(BF16)
    so_ref[...] = state_out
    state_copies = [
        remote(so_ref, so_all.at[tp], ss_sem.at[i], sr_sem.at[i], {"tp": peer})
        for i, peer in enumerate(peers)
    ]
    for copy in state_copies:
        copy.start()
    total = acc_ref[...] + dot(state_out, ps_v[tp])
    for copy in weight_copies:
        copy.wait_recv()
    cross.wait_recv()
    total = total + c_in[...].astype(F32)
    for i in (2, 0, 1):
        state_copies[i].wait_recv()
        total = total + dot(so_all[peers[i]], ps_v[peers[i]])
    out_ref[...] = total.astype(BF16)

    pl.when(not_last)(halo_up.wait_send)
    pl.when(not_first)(halo_down.wait_send)
    for copy in (to_sib + to_oth + forward + gain_copies + weight_copies + state_copies
                 + [first, second, cross]):
        copy.wait_send()
    repeat(1, n_sp, lambda r: interval_copy(r).wait_send())
    repeat(1, n_sp, lambda r: edge_copy(r).wait_send())


def per_device(
    n_sp, n_tp,
    stream, norm_gain, w_value, w_mix, w_gate, w_state, conv_taps, skip_gain, decay_rate, turn_rate,
    input_real, input_imag, read_real, read_imag, initial_state, intervals, proj_conv, proj_state,
):
    rows, width = stream.shape
    channels = w_value.shape[1]
    dirs, groups, per, group = input_real.shape
    states = dirs * groups * per
    cw = width // CHUNKS
    hbm = pl.BlockSpec(memory_space=pltpu.HBM)
    dma = lambda n: pltpu.SemaphoreType.DMA((n,))
    packed = pltpu.VMEM((rows * 8, 128), F32)
    rows_of = lambda m: jnp.swapaxes(m, 2, 3).reshape(dirs * groups * group, per)
    return pl.pallas_call(
        functools.partial(kernel, n_sp, n_tp),
        out_shape=jax.ShapeDtypeStruct((rows, width), BF16),
        in_specs=[hbm] * 18,
        out_specs=pl.BlockSpec(memory_space=pltpu.VMEM),
        scratch_shapes=[
            pltpu.VMEM((rows, width), BF16),
            pltpu.VMEM((1, width), F32),
            pltpu.VMEM(conv_taps.shape, F32),
            pltpu.VMEM((1, channels), F32),
            pltpu.VMEM((dirs * groups, per), F32),
            pltpu.VMEM((dirs * groups, per), F32),
            pltpu.VMEM((dirs * 2 * groups, per), F32),
            pltpu.SMEM((1, rows), F32),
            pltpu.VMEM((width * n_tp, 4 * channels), BF16),
            pltpu.VMEM((channels, width * n_tp), BF16),
            pltpu.VMEM((n_tp, channels, width), BF16),
            pltpu.VMEM((2, dirs * groups * group, per), F32),
            pltpu.VMEM((2, dirs * groups * group, per), F32),
            pltpu.VMEM((n_tp, CHUNKS, rows, cw), BF16),
            pltpu.VMEM((n_tp, 1, width), F32),
            pltpu.VMEM((n_sp, 1, rows), F32),
            packed, packed, packed, packed, packed, packed, packed, packed, packed, packed,
            pltpu.VMEM((2, rows, states), F32),
            pltpu.VMEM((2, rows, states), F32),
            pltpu.VMEM((2, rows, states), BF16),
            pltpu.VMEM((2, channels, states), BF16),
            pltpu.VMEM((2, channels, states), BF16),
            pltpu.VMEM((2, channels, states), BF16),
            pltpu.VMEM((2, dirs, groups, group, 2 * per), F32),
            pltpu.VMEM((rows, channels), BF16),
            pltpu.VMEM((2, 16, channels), BF16),
            pltpu.VMEM((2, 8, 128), F32),
            pltpu.VMEM((n_sp, 8, 128), F32),
            pltpu.VMEM((n_sp, 1, 128), F32),
            pltpu.VMEM((n_sp, 8, 128), F32),
            pltpu.VMEM((n_sp, 8, 128), F32),
        ] + [pltpu.VMEM((rows, width), BF16)] * 6 + [
            pltpu.VMEM((rows, width), F32),
            pltpu.VMEM((rows, channels), BF16),
            pltpu.VMEM((n_tp, rows, channels), BF16),
            dma(18),
            dma(CHUNKS), dma(CHUNKS), dma(CHUNKS), dma(CHUNKS), dma(CHUNKS), dma(CHUNKS),
            dma(n_tp), dma(n_tp), dma(n_sp), dma(n_sp), dma(2), dma(2), dma(n_sp), dma(n_sp),
            dma(3), dma(3), dma(3), dma(3), dma(3), dma(3),
            pltpu.SemaphoreType.REGULAR((max(2, (n_sp - 1).bit_length()),)),
        ],
        compiler_params=pltpu.CompilerParams(
            collective_id=0, has_side_effects=True, vmem_limit_bytes=48 * 1024 * 1024),
    )(*(pltpu.with_memory_space_constraint(a, pltpu.HBM) for a in (
        stream, norm_gain.reshape(1, width), w_value, w_mix, w_gate, w_state, conv_taps,
        skip_gain.reshape(1, channels),
        decay_rate.reshape(dirs * groups, per), turn_rate.reshape(dirs * groups, per),
        rows_of(input_real), rows_of(input_imag),
        read_real.reshape(dirs * groups * group, per), read_imag.reshape(dirs * groups * group, per),
        initial_state.reshape(dirs * 2 * groups, per), intervals.reshape(1, rows),
        proj_conv, proj_state,
    )))


def solution(mesh):
    return jax.shard_map(
        functools.partial(per_device, mesh.shape["sp"], mesh.shape["tp"]),
        mesh=mesh,
        in_specs=(
            P("sp", "tp"), P("tp"), P(None, "tp"), P(None, "tp"), P(None, "tp"), P(None, "tp"),
            P(None, "tp"), P("tp"), P(None, "tp", None), P(None, "tp", None),
            P(None, "tp", None, None), P(None, "tp", None, None), P(None, "tp", None, None),
            P(None, "tp", None, None), P(None, None, "tp", None), P("sp"), P("tp", None),
            P("tp", None),
        ),
        out_specs=P("sp", "tp"),
        check_vma=False,
    )
```

```python
import functools

import jax
import jax.numpy as jnp
from jax import lax
from jax.experimental import pallas as pl
from jax.experimental.pallas import tpu as pltpu
from jax.sharding import PartitionSpec as P

EPSILON = 1e-06
MESH = pl.DeviceIdType.MESH
F32 = jnp.float32
BF16 = jnp.bfloat16
CHUNKS = 4


def dot(a, b):
    return jnp.dot(a, b, preferred_element_type=F32)


def dot_t(a, b):
    return lax.dot_general(a, b, (((1,), (1,)), ((), ())), preferred_element_type=F32)


def half_turns(angle):
    theta = 0.5 * angle
    n = jnp.floor(theta * 0.6366197723675814 + 0.5)
    r = theta - n * 1.5703125
    r = r - n * 0.00048351287841796875
    r = r - n * 3.1385570764541626e-07
    r = r - n * 6.077100627776710e-11
    odd = (n - 2.0 * jnp.floor(0.5 * n)) > 0.5
    z = r * r
    s = r + r * z * ((-1.9515295891e-4 * z + 8.3321608736e-3) * z - 1.6666654611e-1)
    c = 1.0 - 0.5 * z + z * z * (
        (2.443315711809948e-5 * z - 1.388731625493765e-3) * z + 4.166664568298827e-2
    )
    square = jnp.where(odd, c * c, s * s)
    double = 2.0 * s * c
    return square, jnp.where(odd, -double, double)


def expm1_of(x, e):
    p = 1.0 + x * (1.0 / 7.0)
    for k in (6.0, 5.0, 4.0, 3.0, 2.0):
        p = 1.0 + x * p * (1.0 / k)
    return jnp.where(x > -0.35, x * p, e - 1.0)


def repeat(lo, hi, body):
    if hi - lo <= 16:
        for i in range(lo, hi):
            body(i)
    else:
        def step(i, carry):
            body(i)
            return carry
        lax.fori_loop(lo, hi, step, 0)


def fold(lo, hi, body, init):
    if hi - lo <= 16:
        for i in range(lo, hi):
            init = body(i, init)
        return init
    return lax.fori_loop(lo, hi, body, init)


def kernel(
    n_sp, n_tp,
    x_hbm, gain_hbm, wv, wm, wg, ws, taps_hbm, skip_hbm, decay_hbm, turn_hbm,
    inr, ini, rdr, rdi, init_hbm, iv_hbm, pc, ps,
    out_ref,
    x_ref, gain_ref, taps_ref, skip_ref, decay_ref, turn_ref, init_ref, iv_s, iv_v,
    w_all, pc_v, ps_v, in_v, rd_v, x_full, gains, el_all, fr_ref, fi_ref, gr_ref, gi_ref,
    dr_ref, di_ref, hr_ref, hi_ref, kr_ref, ki_ref, k_row, d_row, p_row,
    bt_ref, rt_ref, rc_ref, cq_ref, src_ref, halo_ref, e_out, e_all,
    span_ref, wa_ref, wb_ref, p1_out, p1_in, p2_out, p2_in, c_out, c_in, acc_ref, so_ref, so_in,
    rp_out, rp_in, kept_ref,
    load_sem, as_sem, ar_sem, bs_sem, br_sem, fs_sem, fwr_sem, gs_sem, grv_sem,
    is_sem, ir_sem, hs_sem, hr_sem, es_sem, er_sem, ps_sem, pr_sem, ws_sem, wr_sem, ss_sem, sr_sem, os_sem, or_sem, greet_sem,
):
    tp, sp = lax.axis_index("tp"), lax.axis_index("sp")
    rows, width = x_hbm.shape
    channels = wv.shape[1]
    y, core = tp // 2, tp % 2
    sib = y * 2 + 1 - core
    oth = (1 - y) * 2 + core
    diag = (1 - y) * 2 + 1 - core
    cw = width // CHUNKS

    loads = {}

    def load(name, src, dst):
        copy = pltpu.make_async_copy(src, dst, load_sem.at[len(loads)])
        copy.start()
        loads[name] = copy

    def loaded(*names):
        for name in names:
            loads[name].wait()

    def near(step, act):
        for s in (-step, step):
            @pl.when((sp + s >= 0) & (sp + s < n_sp))
            def _():
                act(sp + s)

    def near_count(step):
        return jnp.where(sp - step >= 0, 1, 0) + jnp.where(sp + step < n_sp, 1, 0)

    def greet(k):
        near(1 << k, lambda where: pl.semaphore_signal(
            greet_sem.at[k], inc=1, device_id={"sp": where}, device_id_type=MESH))

    def greeted(k):
        pl.semaphore_wait(greet_sem.at[k], near_count(1 << k))

    rounds = greet_sem.shape[0]
    barrier = pltpu.get_barrier_semaphore()
    for j in range(1, n_tp):
        pl.semaphore_signal(barrier, inc=1, device_id={"tp": (tp + j) % n_tp}, device_id_type=MESH)
    near(1, lambda where: pl.semaphore_signal(
        barrier, inc=1, device_id={"sp": where}, device_id_type=MESH))
    load("x", x_hbm, x_ref)
    load("iv", iv_hbm, iv_s)
    load("ivv", iv_hbm, iv_v)
    load("decay", decay_hbm, decay_ref.at[0])
    load("turn", turn_hbm, turn_ref.at[0])
    load("init", init_hbm, init_ref.at[0])
    load("gain", gain_hbm, gain_ref)
    load("inr", inr, in_v.at[0])
    load("ini", ini, in_v.at[1])
    load("rdr", rdr, rd_v.at[0])
    load("rdi", rdi, rd_v.at[1])
    for j, w in enumerate((wv, wm, wg, ws)):
        load("w%d" % j, w, w_all.at[:, pl.ds(j * channels, channels)])
    load("taps", taps_hbm, taps_ref)
    load("skip", skip_hbm, skip_ref)
    load("pc", pc, pc_v)
    load("ps", ps.at[:, pl.ds(pl.multiple_of(tp * width, width), width)], ps_v.at[pl.ds(0, channels)])
    pl.semaphore_wait(barrier, n_tp - 1 + near_count(1))
    loaded("x")

    def remote(src, dst, send, recv, where):
        return pltpu.make_async_remote_copy(
            src_ref=src, dst_ref=dst, send_sem=send, recv_sem=recv,
            device_id=where, device_id_type=MESH)

    to_sib, to_oth, forward = [], [], []
    for c in range(CHUNKS):
        piece = x_ref.at[:, pl.ds(c * cw, cw)]
        to_oth.append(remote(piece, x_full.at[tp, c], bs_sem.at[c], br_sem.at[c], {"tp": oth}))
        to_sib.append(remote(piece, x_full.at[tp, c], as_sem.at[c], ar_sem.at[c], {"tp": sib}))
        forward.append(remote(x_full.at[oth, c], x_full.at[oth, c], fs_sem.at[c], fwr_sem.at[c],
                              {"tp": sib}))
    for c in range(CHUNKS):
        to_oth[c].start()
    for c in range(CHUNKS):
        to_sib[c].start()
    gain_copies = [
        remote(gain_hbm, gains.at[tp], gs_sem.at[j], grv_sem.at[j], {"tp": (tp + j) % n_tp})
        for j in range(1, n_tp)
    ]
    for copy in gain_copies:
        copy.start()
    greet(0)
    part_rows = channels // 2
    my_part = pl.multiple_of((sp % 2) * part_rows, part_rows)
    twin = sp + 1 - 2 * (sp % 2)

    def columns(owner):
        return pl.ds(pl.multiple_of(owner * width, width), width)

    def slot(pos):
        return ps_v.at[pl.ds(pos * channels + my_part, part_rows)]

    weight_copies = [
        remote(ps.at[:, columns(sib)], ps_v.at[pl.ds(2 * channels, channels)],
               ws_sem.at[0], wr_sem.at[0], {"tp": sib}),
        remote(ps.at[pl.ds(my_part, part_rows), columns(oth)], slot(1), ws_sem.at[1], wr_sem.at[1],
               {"tp": oth}),
        remote(ps.at[pl.ds(my_part, part_rows), columns(diag)], slot(3), ws_sem.at[2], wr_sem.at[2],
               {"tp": diag}),
    ]
    weight_forward = [
        remote(slot(pos), slot(pos), ws_sem.at[3 + i], wr_sem.at[3 + i], {"sp": twin})
        for i, pos in enumerate((1, 3))
    ]
    other_copies = [
        remote(src, dst, os_sem.at[i], or_sem.at[i], {"tp": oth})
        for i, (src, dst) in enumerate((
            (decay_hbm, decay_ref.at[1]), (turn_hbm, turn_ref.at[1]), (init_hbm, init_ref.at[1]),
            (cq_ref.at[0], cq_ref.at[1])))
    ]
    rest_copy = remote(rp_out, rp_in, os_sem.at[4], or_sem.at[4], {"tp": oth})

    def pass_on(c):
        to_oth[c].wait_recv()
        forward[c].start()

    sub = lax.broadcasted_iota(jnp.int32, (8, 128), 0)
    top = sub < 4

    def pack(ref):
        even = ref[pl.ds(0, 8, stride=2), :]
        odd = ref[pl.ds(1, 8, stride=2), :]
        return jnp.concatenate([even, odd], axis=1)

    loaded("iv", "decay", "turn", "init")
    decay, turn = pack(decay_ref.at[0]), pack(turn_ref.at[0])
    den = decay * decay + turn * turn
    td, dd = turn / den, decay / den

    def factors(k, carry):
        iv = jnp.where(top, iv_s[0, k], iv_s[0, rows - 1 - k])
        damp = -decay * iv
        square, sine = half_turns(turn * iv)
        e = jnp.exp(damp)
        cosine = 1.0 - 2.0 * square
        f_im = e * sine
        lift = expm1_of(damp, e) * cosine - 2.0 * square
        at = pl.ds(pl.multiple_of(k * 8, 8), 8)
        fr_ref[at, :] = e * cosine
        fi_ref[at, :] = f_im
        gr_ref[at, :] = td * f_im - dd * lift
        gi_ref[at, :] = -(dd * f_im + td * lift)
        return carry

    lax.fori_loop(0, 3 * rows // 4, factors, 0, unroll=4)
    greeted(0)
    if rounds > 1:
        greet(1)
    lax.fori_loop(3 * rows // 4, rows, factors, 0, unroll=4)

    def put(ref, k, value):
        ref[pl.ds(pl.multiple_of(k * 8, 8), 4), :] = value[:4]
        ref[pl.ds(pl.multiple_of((rows - 1 - k) * 8, 8) + 4, 4), :] = value[4:]

    def chain(k, carry):
        ar, ai, br, bi = carry
        at = pl.ds(pl.multiple_of(k * 8, 8), 8)
        back = pl.ds(pl.multiple_of((rows - 1 - k) * 8, 8), 8)
        fr, fi = fr_ref[at, :], fi_ref[at, :]
        ar, ai = fr * ar - fi * ai, fr * ai + fi * ar
        put(hr_ref, k, ar)
        put(hi_ref, k, ai)
        gr, gi = gr_ref[back, :], gi_ref[back, :]
        put(kr_ref, rows - 1 - k, gr * br - gi * bi)
        put(ki_ref, rows - 1 - k, gr * bi + gi * br)
        fr, fi = fr_ref[back, :], fi_ref[back, :]
        return ar, ai, fr * br - fi * bi, fr * bi + fi * br

    one, zero = jnp.ones((8, 128), F32), jnp.zeros((8, 128), F32)
    lax.fori_loop(0, rows, chain, (one, zero, one, zero), unroll=4)
    if rounds > 1:
        greeted(1)
    for k in range(2, rounds):
        greet(k)
        if k < rounds - 1:
            greeted(k)
    pass_on(0)
    for part, (k_ref, h_ref) in enumerate(((kr_ref, hr_ref), (ki_ref, hi_ref))):
        for j in range(8):
            lanes = slice(j * 128, (j + 1) * 128)
            k_row[part, :, lanes] = k_ref[pl.ds(j, rows, stride=8), :]
            p_row[0, :, pl.ds(part * bt_ref.shape[2] + j * 128, 128)] = h_ref[pl.ds(j, rows, stride=8), :].astype(BF16)
    pass_on(1)
    for copy in to_oth:
        copy.wait_send()
    for copy in weight_copies:
        copy.start()

    loaded("inr", "ini", "rdr", "rdi")
    states = bt_ref.shape[2]
    per = rd_v.shape[2]
    half = states // 2
    group = channels * per // half
    spread = (lax.broadcasted_iota(jnp.int32, (per, half), 1) % per
              == lax.broadcasted_iota(jnp.int32, (per, half), 0)).astype(BF16)
    keep = ((lax.broadcasted_iota(jnp.int32, (channels, half), 1) // per)
            == (lax.broadcasted_iota(jnp.int32, (channels, half), 0) // group))
    left = lax.broadcasted_iota(jnp.int32, (group, 2 * per), 1) < per
    for part in range(2):
        for d in range(2):
            at, to = pl.ds(d * channels, channels), pl.ds(d * half, half)
            wide = dot(in_v[part, at, :].astype(BF16), spread)
            bt_ref[part, :, to] = jnp.where(keep, wide, 0.0).astype(BF16)
            wide = dot(rd_v[part, at, :].astype(BF16), spread)
            if part:
                wide = -wide
            rt_ref[part, :, to] = jnp.where(keep, wide, 0.0).astype(BF16)
            for q in range(channels // group // 2):
                pair = [rd_v[part, pl.ds(d * channels + g * group, group), :] for g in (2 * q, 2 * q + 1)]
                cq_ref[0, part, d, q] = jnp.concatenate(pair, axis=1).astype(BF16)
    rc_ref[...] = jnp.zeros_like(rc_ref)

    pass_on(2)
    for copy in other_copies:
        copy.start()
    loaded("gain", "w0", "w1", "w2", "w3")
    for copy in gain_copies:
        copy.wait_recv()

    def project(value, gain, first):
        wide = value.astype(F32)
        scaled = (wide * gain).astype(BF16)
        k = value.shape[1]
        term = dot(scaled, w_all[pl.ds(pl.multiple_of(first, k), k), :])
        return term, jnp.sum(wide * wide, axis=1, keepdims=True)

    projected = jnp.zeros((rows, 4 * channels), F32)
    squares = jnp.zeros((rows, 1), F32)
    t, s = project(x_ref[...], gain_ref[...], tp * width)
    projected, squares = projected + t, squares + s

    def whole(owner, projected, squares):
        value = jnp.concatenate([x_full[owner, c] for c in range(CHUNKS)], axis=1)
        t, s = project(value, gains[owner], owner * width)
        return projected + t, squares + s

    for c in range(CHUNKS):
        to_sib[c].wait_recv()
    projected, squares = whole(sib, projected, squares)
    pass_on(3)
    projected, squares = whole(oth, projected, squares)
    if rounds > 2:
        greeted(rounds - 1)

    def interval_copy(r):
        return remote(iv_hbm, el_all.at[r], is_sem.at[r], ir_sem.at[r], {"sp": (sp + r) % n_sp})

    repeat(1, n_sp, lambda r: interval_copy(r).start())
    for c in range(CHUNKS):
        forward[c].wait_recv()
        t, s = project(x_full[diag, c], gains[diag][:, c * cw:(c + 1) * cw], diag * width + c * cw)
        projected, squares = projected + t, squares + s
    projected = projected * lax.rsqrt(squares / (width * n_tp) + EPSILON)
    state_input = projected[:, 3 * channels:].astype(BF16)
    conv_value = projected[:, :channels].astype(BF16).astype(F32)
    conv_mix = projected[:, channels:2 * channels].astype(BF16).astype(F32)
    conv_gate = projected[:, 2 * channels:3 * channels].astype(BF16).astype(F32)
    src_ref[...] = (conv_mix * conv_value).astype(BF16)

    for j in range(4):
        lanes = slice(j * 256, (j + 1) * 256)
        dr = dot(state_input, bt_ref[0, :, lanes])
        di = dot(state_input, bt_ref[1, :, lanes])
        d_row[0, :, lanes] = dr
        d_row[1, :, lanes] = di
        kr, ki = k_row[0, :, lanes], k_row[1, :, lanes]
        er = jnp.sum(kr * dr - ki * di, axis=0, keepdims=True)
        ei = jnp.sum(kr * di + ki * dr, axis=0, keepdims=True)
        for h in range(2):
            q = (j % 2) * 2 + h
            e_out[j // 2, q:q + 1, :] = er[:, h * 128:(h + 1) * 128]
            e_out[j // 2, 4 + q:5 + q, :] = ei[:, h * 128:(h + 1) * 128]


    def edge_copy(r, s):
        return remote(e_out.at[jnp.where(sp + r < n_sp, 0, 1)], e_all.at[s, r], es_sem.at[s, r],
                      er_sem.at[s, r], {"sp": (sp + r) % n_sp, "tp": oth if s else tp})

    def edges(act):
        def at(r):
            act(edge_copy(r, 0))
            act(edge_copy(r, 1))
        repeat(1, n_sp, at)

    halo_up = remote(src_ref.at[pl.ds(rows - 16, 16)], halo_ref.at[0], hs_sem.at[0], hr_sem.at[0],
                     {"sp": (sp + 1) % n_sp})
    halo_down = remote(src_ref.at[pl.ds(0, 16)], halo_ref.at[1], hs_sem.at[1], hr_sem.at[1],
                       {"sp": (sp + n_sp - 1) % n_sp})
    edges(lambda copy: copy.start())
    not_first, not_last = sp > 0, sp < n_sp - 1
    pl.when(not_last)(halo_up.start)
    pl.when(not_first)(halo_down.start)

    loaded("taps", "skip", "pc", "ps")
    edge = 16
    inner_rows = rows - 2 * edge
    pieces = (pl.ds(0, inner_rows), pl.ds(inner_rows, 2 * edge))
    source = src_ref[...].astype(F32)
    line = lax.broadcasted_iota(jnp.int32, (rows, channels), 0)
    previous = jnp.where(line == 0, 0.0, pltpu.roll(source, 1, 0))
    following = jnp.where(line == rows - 1, 0.0, pltpu.roll(source, rows - 1, 0))
    filtered = taps_ref[0:1, :] * previous + taps_ref[1:2, :] * source + taps_ref[2:3, :] * following
    conv_out = (conv_gate * filtered).astype(BF16)[edge:rows - edge]

    def ends(a):
        return jnp.concatenate([a[:edge], a[rows - edge:]], axis=0)

    end_gate, end_filtered = ends(conv_gate), ends(filtered)

    def products(branch, i):
        at = pieces[i]
        copies = [
            remote(p1_out.at[at], p1_in.at[at], ps_sem.at[3 * i], pr_sem.at[3 * i], {"tp": sib}),
            remote(p2_out.at[at], p2_in.at[at], ps_sem.at[3 * i + 1], pr_sem.at[3 * i + 1], {"tp": sib}),
            remote(c_out.at[at], c_in.at[at], ps_sem.at[3 * i + 2], pr_sem.at[3 * i + 2], {"tp": oth}),
        ]
        p1_out[at, :] = dot(branch, pc_v[:, columns(diag)]).astype(BF16)
        copies[0].start()
        p2_out[at, :] = dot(branch, pc_v[:, columns(sib)]).astype(BF16)
        copies[1].start()
        kept = dot(branch, pc_v[:, columns(oth)])
        acc_ref[at, :] = dot(branch, pc_v[:, columns(tp)])
        return copies, kept

    def crossing(copies, kept, i):
        at = pieces[i]
        copies[0].wait_recv()
        c_out[at, :] = (kept + p1_in[at, :].astype(F32)).astype(BF16)
        copies[2].start()

    conv_a, kept = products(conv_out, 0)
    kept_ref[...] = kept

    for part, ref in ((0, dr_ref), (1, di_ref)):
        for j in range(8):
            ref[pl.ds(j, rows, stride=8), :] = d_row[part, :, j * 128:(j + 1) * 128]


    def local(k, carry):
        hr, hi = carry
        at = pl.ds(pl.multiple_of(k * 8, 8), 8)
        back = pl.ds(pl.multiple_of((rows - 1 - k) * 8, 8), 8)
        dr = jnp.where(top, dr_ref[at, :], dr_ref[back, :])
        di = jnp.where(top, di_ref[at, :], di_ref[back, :])
        gr, gi = gr_ref[at, :], gi_ref[at, :]
        fr, fi = fr_ref[at, :], fi_ref[at, :]
        pr = gr * dr - gi * di
        pi = gr * di + gi * dr
        hr, hi = fr * hr + (pr - fi * hi), fr * hi + (pi + fi * hr)
        put(hr_ref, k, hr)
        put(hi_ref, k, hi)
        return hr, hi

    lax.fori_loop(0, rows, local, (zero, zero), unroll=8)
    response = state_input.astype(F32) * skip_ref[...]
    for part, ref in ((0, hr_ref), (1, hi_ref)):
        history = jnp.concatenate(
            [ref[pl.ds(j, rows, stride=8), :].astype(BF16) for j in range(8)], axis=1)
        response = response + dot_t(history, rt_ref[part])

    rp_out[...] = response.astype(BF16)
    rest_copy.start()
    crossing(conv_a, kept_ref[...], 0)
    for copy in weight_copies:
        copy.wait_recv()
    for copy in weight_forward:
        copy.start()
    pl.when(not_first)(halo_up.wait_recv)
    pl.when(not_last)(halo_down.wait_recv)
    before = jnp.where(not_first, halo_ref[0].astype(F32)[15:16, :], 0.0) * taps_ref[0:1, :]
    after = jnp.where(not_last, halo_ref[1].astype(F32)[0:1, :], 0.0) * taps_ref[2:3, :]
    end_line = lax.broadcasted_iota(jnp.int32, (2 * edge, channels), 0)
    end_filtered = end_filtered + jnp.where(
        end_line == 0, before, jnp.where(end_line == 2 * edge - 1, after, 0.0))
    conv_b, kept_b = products((end_gate * end_filtered).astype(BF16), 1)

    for copy in other_copies:
        copy.wait_recv()
    decay_2, turn_2 = pack(decay_ref.at[1]), pack(turn_ref.at[1])
    at_t = lax.broadcasted_iota(jnp.int32, (rows, rows), 0)
    at_s = lax.broadcasted_iota(jnp.int32, (rows, rows), 1)
    loaded("ivv")
    steps = iv_v[...]
    reach = (jnp.sum(jnp.where(at_s <= at_t, steps, 0.0), axis=1, keepdims=True),
             jnp.sum(jnp.where(at_s >= at_t, steps, 0.0), axis=1, keepdims=True))
    for j in range(8):
        square, sine = half_turns(turn_2[j:j + 1, :] * reach[j // 4])
        e = jnp.exp(-decay_2[j:j + 1, :] * reach[j // 4])
        p_row[1, :, j * 128:(j + 1) * 128] = (e * (1.0 - 2.0 * square)).astype(BF16)
        p_row[1, :, states + j * 128:states + (j + 1) * 128] = (e * sine).astype(BF16)
    crossing(conv_b, kept_b, 1)

    repeat(1, n_sp, lambda r: interval_copy(r).wait_recv())

    def both_of(full, d):
        return jnp.concatenate([full[d * 4:d * 4 + 4], full[d * 4:d * 4 + 4]], axis=0)

    def init_of(s, d):
        ref = init_ref.at[s]
        parts = [
            jnp.concatenate([ref[pl.ds(d * 16 + part * 8, 4, stride=2), :],
                             ref[pl.ds(d * 16 + part * 8 + 1, 4, stride=2), :]], axis=1)
            for part in range(2)
        ]
        return jnp.concatenate(parts, axis=0)

    decays = [[both_of(full, d) for d in range(2)] for full in (decay, decay_2)]
    turns = [[both_of(full, d) for d in range(2)] for full in (turn, turn_2)]

    def weight(damping, turning, span):
        square, sine = half_turns(turning * span)
        e = jnp.exp(-damping * span)
        return e * (1.0 - 2.0 * square), jnp.where(top, -e * sine, e * sine)

    def apply(w, tile):
        return w[0] * tile + w[1] * pltpu.roll(tile, 4, 0)

    def elapsed(r):
        return jnp.sum(el_all[r], axis=1, keepdims=True)

    none = jnp.zeros((1, 1), F32)

    def ahead(r, carry):
        total, inside = carry
        span_ref[r] = jnp.broadcast_to(total, (1, 128))
        step = elapsed(r)
        return total + step, inside + step * jnp.where(sp - r >= 0, 1.0, 0.0)

    total, inside = fold(1, n_sp, ahead, (none, none))

    def behind(i, total):
        r = n_sp - i
        mine = sp - r >= 0
        span = jnp.where(mine, span_ref[r], jnp.broadcast_to(total, (1, 128)))
        for s in range(2):
            w = weight(jnp.where(mine, *decays[s]), jnp.where(mine, *turns[s]), span)
            wa_ref[s, r] = w[0]
            wb_ref[s, r] = w[1]
        return total + elapsed(r)

    fold(1, n_sp, behind, none)
    outside = none

    def beyond(r, acc):
        return acc + elapsed(r) * jnp.where(sp - r >= 0, 0.0, 1.0)

    outside = fold(1, n_sp, beyond, none)
    from_start = [
        tuple(apply(weight(decays[s][d], turns[s][d], (inside, outside)[d]), init_of(s, d))
              for d in range(2))
        for s in range(2)
    ]

    rest_copy.wait_recv()
    edges(lambda copy: copy.wait_recv())
    for s in range(2):
        def combine(r, carry):
            h0, h1 = carry
            moved = apply((wa_ref[s, r], wb_ref[s, r]), e_all[s, r])
            mine = sp - r >= 0
            return h0 + jnp.where(mine, moved, 0.0), h1 + jnp.where(mine, 0.0, moved)

        entering = fold(1, n_sp, combine, from_start[s])
        for d in range(2):
            for q in range(channels // group // 2):
                hr, hi = entering[d][q:q + 1, :], entering[d][4 + q:5 + q, :]
                cr, ci = (cq_ref[s, part, d, q].astype(F32) for part in range(2))
                for part, value in ((0, cr * hr - ci * hi), (1, -(cr * hi + ci * hr))):
                    for side in range(2):
                        at = pl.ds((2 * q + side) * group, group)
                        lanes = pl.ds(part * states + d * half + q * 128, 128)
                        rc_ref[s, at, lanes] = jnp.where(
                            left if side == 0 else ~left, value, 0.0).astype(BF16)
    gated = []
    for s in range(2):
        full = response if s == 0 else rp_in[...].astype(F32)
        full = full + dot_t(p_row[s], rc_ref[s])
        inner = 0.7978845608028654 * (full + 0.044715 * (full * full * full))
        gated.append((0.5 * full * (1.0 + jnp.tanh(inner))).astype(BF16))
    state_out = jnp.concatenate(gated, axis=1)
    so_ref[...] = state_out
    state_copy = remote(so_ref, so_in, ss_sem.at[0], sr_sem.at[0], {"tp": sib})
    state_copy.start()
    for copy in weight_forward:
        copy.wait_recv()
    total = dot(state_out, ps_v[:2 * channels])
    for copies in (conv_a, conv_b):
        for copy in copies[1:]:
            copy.wait_recv()
    base = acc_ref[...] + p2_in[...].astype(F32) + c_in[...].astype(F32)
    total = total + jnp.concatenate(
        [base[inner_rows:inner_rows + edge], base[:inner_rows], base[inner_rows + edge:]], axis=0)
    state_copy.wait_recv()
    out_ref[...] = (total + dot(so_in[...], ps_v[2 * channels:])).astype(BF16)

    pl.when(not_last)(halo_up.wait_send)
    pl.when(not_first)(halo_down.wait_send)
    for copy in (to_sib + forward + gain_copies + weight_copies + weight_forward + other_copies
                 + conv_a + conv_b + [rest_copy, state_copy]):
        copy.wait_send()
    repeat(1, n_sp, lambda r: interval_copy(r).wait_send())
    edges(lambda copy: copy.wait_send())


def per_device(
    n_sp, n_tp,
    stream, norm_gain, w_value, w_mix, w_gate, w_state, conv_taps, skip_gain, decay_rate, turn_rate,
    input_real, input_imag, read_real, read_imag, initial_state, intervals, proj_conv, proj_state,
):
    rows, width = stream.shape
    channels = w_value.shape[1]
    dirs, groups, per, group = input_real.shape
    states = dirs * groups * per
    cw = width // CHUNKS
    hbm = pl.BlockSpec(memory_space=pltpu.HBM)
    dma = lambda n: pltpu.SemaphoreType.DMA((n,))
    packed = pltpu.VMEM((rows * 8, 128), F32)
    rows_of = lambda m: jnp.swapaxes(m, 2, 3).reshape(dirs * groups * group, per)
    return pl.pallas_call(
        functools.partial(kernel, n_sp, n_tp),
        out_shape=jax.ShapeDtypeStruct((rows, width), BF16),
        in_specs=[hbm] * 18,
        out_specs=pl.BlockSpec(memory_space=pltpu.VMEM),
        scratch_shapes=[
            pltpu.VMEM((rows, width), BF16),
            pltpu.VMEM((1, width), F32),
            pltpu.VMEM(conv_taps.shape, F32),
            pltpu.VMEM((1, channels), F32),
            pltpu.VMEM((2, dirs * groups, per), F32),
            pltpu.VMEM((2, dirs * groups, per), F32),
            pltpu.VMEM((2, dirs * 2 * groups, per), F32),
            pltpu.SMEM((1, rows), F32),
            pltpu.VMEM((1, rows), F32),
            pltpu.VMEM((width * n_tp, 4 * channels), BF16),
            pltpu.VMEM((channels, width * n_tp), BF16),
            pltpu.VMEM((n_tp * channels, width), BF16),
            pltpu.VMEM((2, dirs * groups * group, per), F32),
            pltpu.VMEM((2, dirs * groups * group, per), F32),
            pltpu.VMEM((n_tp, CHUNKS, rows, cw), BF16),
            pltpu.VMEM((n_tp, 1, width), F32),
            pltpu.VMEM((n_sp, 1, rows), F32),
            packed, packed, packed, packed, packed, packed, packed, packed, packed, packed,
            pltpu.VMEM((2, rows, states), F32),
            pltpu.VMEM((2, rows, states), F32),
            pltpu.VMEM((2, rows, 2 * states), BF16),
            pltpu.VMEM((2, channels, states), BF16),
            pltpu.VMEM((2, channels, states), BF16),
            pltpu.VMEM((2, channels, 2 * states), BF16),
            pltpu.VMEM((2, 2, dirs, groups // 2, group, 2 * per), BF16),
            pltpu.VMEM((rows, channels), BF16),
            pltpu.VMEM((2, 16, channels), BF16),
            pltpu.VMEM((2, 8, 128), F32),
            pltpu.VMEM((2, n_sp, 8, 128), F32),
            pltpu.VMEM((n_sp, 1, 128), F32),
            pltpu.VMEM((2, n_sp, 8, 128), F32),
            pltpu.VMEM((2, n_sp, 8, 128), F32),
        ] + [pltpu.VMEM((rows, width), BF16)] * 6 + [
            pltpu.VMEM((rows, width), F32),
            pltpu.VMEM((rows, 2 * channels), BF16),
            pltpu.VMEM((rows, 2 * channels), BF16),
            pltpu.VMEM((rows, channels), BF16),
            pltpu.VMEM((rows, channels), BF16),
            pltpu.VMEM((rows - 32, width), F32),
        ] + [
            dma(19),
            dma(CHUNKS), dma(CHUNKS), dma(CHUNKS), dma(CHUNKS), dma(CHUNKS), dma(CHUNKS),
            dma(n_tp), dma(n_tp), dma(n_sp), dma(n_sp), dma(2), dma(2),
            pltpu.SemaphoreType.DMA((2, n_sp)), pltpu.SemaphoreType.DMA((2, n_sp)),
            dma(6), dma(6), dma(5), dma(5), dma(1), dma(1), dma(5), dma(5),
            pltpu.SemaphoreType.REGULAR((max(2, (n_sp - 1).bit_length()),)),
        ],
        compiler_params=pltpu.CompilerParams(
            collective_id=0, has_side_effects=True, vmem_limit_bytes=48 * 1024 * 1024),
    )(*(pltpu.with_memory_space_constraint(a, pltpu.HBM) for a in (
        stream, norm_gain.reshape(1, width), w_value, w_mix, w_gate, w_state, conv_taps,
        skip_gain.reshape(1, channels),
        decay_rate.reshape(dirs * groups, per), turn_rate.reshape(dirs * groups, per),
        rows_of(input_real), rows_of(input_imag),
        read_real.reshape(dirs * groups * group, per), read_imag.reshape(dirs * groups * group, per),
        initial_state.reshape(dirs * 2 * groups, per), intervals.reshape(1, rows),
        proj_conv, proj_state,
    )))


def solution(mesh):
    return jax.shard_map(
        functools.partial(per_device, mesh.shape["sp"], mesh.shape["tp"]),
        mesh=mesh,
        in_specs=(
            P("sp", "tp"), P("tp"), P(None, "tp"), P(None, "tp"), P(None, "tp"), P(None, "tp"),
            P(None, "tp"), P("tp"), P(None, "tp", None), P(None, "tp", None),
            P(None, "tp", None, None), P(None, "tp", None, None), P(None, "tp", None, None),
            P(None, "tp", None, None), P(None, None, "tp", None), P("sp"), P("tp", None),
            P("tp", None),
        ),
        out_specs=P("sp", "tp"),
        check_vma=False,
    )
```

```python
import functools

import jax
import jax.numpy as jnp
from jax import lax
from jax.experimental import pallas as pl
from jax.experimental.pallas import tpu as pltpu
from jax.sharding import PartitionSpec as P

EPSILON = 1e-06
MESH = pl.DeviceIdType.MESH
F32 = jnp.float32
BF16 = jnp.bfloat16
CHUNKS = 4


def dot(a, b):
    return jnp.dot(a, b, preferred_element_type=F32)


def dot_t(a, b):
    return lax.dot_general(a, b, (((1,), (1,)), ((), ())), preferred_element_type=F32)


def half_turns(angle):
    theta = 0.5 * angle
    n = jnp.floor(theta * 0.6366197723675814 + 0.5)
    r = theta - n * 1.5703125
    r = r - n * 0.00048351287841796875
    r = r - n * 3.1385570764541626e-07
    r = r - n * 6.077100627776710e-11
    odd = (n - 2.0 * jnp.floor(0.5 * n)) > 0.5
    z = r * r
    s = r + r * z * ((-1.9515295891e-4 * z + 8.3321608736e-3) * z - 1.6666654611e-1)
    c = 1.0 - 0.5 * z + z * z * (
        (2.443315711809948e-5 * z - 1.388731625493765e-3) * z + 4.166664568298827e-2
    )
    square = jnp.where(odd, c * c, s * s)
    double = 2.0 * s * c
    return square, jnp.where(odd, -double, double)


def expm1_of(x, e):
    p = 1.0 + x * (1.0 / 7.0)
    for k in (6.0, 5.0, 4.0, 3.0, 2.0):
        p = 1.0 + x * p * (1.0 / k)
    return jnp.where(x > -0.35, x * p, e - 1.0)


def repeat(lo, hi, body):
    if hi - lo <= 16:
        for i in range(lo, hi):
            body(i)
    else:
        def step(i, carry):
            body(i)
            return carry
        lax.fori_loop(lo, hi, step, 0)


def fold(lo, hi, body, init):
    if hi - lo <= 16:
        for i in range(lo, hi):
            init = body(i, init)
        return init
    return lax.fori_loop(lo, hi, body, init)


def kernel(
    n_sp, n_tp,
    x_hbm, gain_hbm, wv, wm, wg, ws, taps_hbm, skip_hbm, decay_hbm, turn_hbm,
    inr, ini, rdr, rdi, init_hbm, iv_hbm, pc, ps,
    out_ref,
    x_ref, gain_ref, taps_ref, skip_ref, par_ref, iv_s, iv_v,
    w_all, pc_v, ps_v, in_v, rd_v, x_full, gains, el_all, fr_ref, fi_ref, gr_ref, gi_ref,
    dr_ref, di_ref, hr_ref, hi_ref, kr_ref, ki_ref, k_row, d_row, p_row,
    bt_ref, rt_ref, rc_ref, cq_ref, src_ref, halo_ref, e_out, e_all,
    span_ref, wa_ref, wb_ref, po_ref, p1_in, pi_ref, acc_ref, so_ref, so_in,
    rp_out, rp_in, kept_ref,
    load_sem, fwr_sem, br_sem, one_sem, hs_sem, hr_sem, p1r_sem, greet_sem, pair_sem,
):
    tp, sp = lax.axis_index("tp"), lax.axis_index("sp")
    rows, width = x_hbm.shape
    channels = wv.shape[1]
    y, core = tp // 2, tp % 2
    sib = y * 2 + 1 - core
    oth = (1 - y) * 2 + core
    diag = (1 - y) * 2 + 1 - core
    cw = width // CHUNKS

    names = ("bs", "as", "ar", "fs", "gs", "gr", "is", "ir", "es", "er", "ps", "pr", "ws", "wr",
             "vs", "vr", "os", "or", "cs", "cr", "rs", "rr", "ss", "sr")
    one = {name: one_sem.at[i] for i, name in enumerate(names)}
    loads = {}

    def load(name, whole, *pairs):
        sem = load_sem.at[len(loads)]
        loads[name] = whole, sem
        for src, dst in pairs:
            pltpu.make_async_copy(src, dst, sem).start()

    def remote(src, dst, send, recv, where):
        return pltpu.make_async_remote_copy(
            src_ref=src, dst_ref=dst, send_sem=send, recv_sem=recv,
            device_id=where, device_id_type=MESH)

    def drain(ref, sem):
        remote(ref, ref, sem, sem, {"tp": sib}).wait_recv()

    def loaded(*names):
        for name in names:
            drain(*loads[name])

    def near(step, act):
        for s in (-step, step):
            @pl.when((sp + s >= 0) & (sp + s < n_sp))
            def _():
                act(sp + s)

    def near_count(step):
        return jnp.where(sp - step >= 0, 1, 0) + jnp.where(sp + step < n_sp, 1, 0)

    def greet(k):
        near(1 << k, lambda where: pl.semaphore_signal(
            greet_sem.at[k], inc=1, device_id={"sp": where}, device_id_type=MESH))

    def greeted(k):
        pl.semaphore_wait(greet_sem.at[k], near_count(1 << k))

    rounds = greet_sem.shape[0]
    barrier = pltpu.get_barrier_semaphore()
    for peer in (sib, oth):
        pl.semaphore_signal(barrier, inc=1, device_id={"tp": peer}, device_id_type=MESH)
    near(1, lambda where: pl.semaphore_signal(
        barrier, inc=1, device_id={"sp": where}, device_id_type=MESH))
    load("x", x_ref, (x_hbm, x_ref))
    iv_load = pltpu.make_async_copy(iv_hbm, iv_s, load_sem.at[len(loads)])
    iv_load.start()
    loads["iv"] = None
    dirs_groups = decay_hbm.shape[0]
    par_parts = (pl.ds(0, dirs_groups), pl.ds(dirs_groups, dirs_groups),
                 pl.ds(2 * dirs_groups, 2 * dirs_groups))
    par_hbm = (decay_hbm, turn_hbm, init_hbm)
    load("par", par_ref.at[0], *((src, par_ref.at[0, at]) for src, at in zip(par_hbm, par_parts)))
    load("ivv", iv_v, (iv_hbm, iv_v))
    load("gain", gain_ref, (gain_hbm, gain_ref))
    load("in", in_v, (inr, in_v.at[0]), (ini, in_v.at[1]))
    load("rd", rd_v, (rdr, rd_v.at[0]), (rdi, rd_v.at[1]))
    load("w", w_all, *((w, w_all.at[:, pl.ds(j * channels, channels)])
                       for j, w in enumerate((wv, wm, wg, ws))))
    load("taps", taps_ref, (taps_hbm, taps_ref))
    load("skip", skip_ref, (skip_hbm, skip_ref))
    load("pc", pc_v, (pc, pc_v))
    own = ps.at[:, pl.ds(pl.multiple_of(tp * width, width), width)]
    load("ps", ps_v.at[pl.ds(0, channels)], (own, ps_v.at[pl.ds(0, channels)]))
    pl.semaphore_wait(barrier, 2 + near_count(1))
    loaded("x")

    to_sib, to_oth, forward = [], [], []
    for c in range(CHUNKS):
        piece = x_ref.at[:, pl.ds(c * cw, cw)]
        to_oth.append(remote(piece, x_full.at[tp, c], one["bs"], br_sem.at[c], {"tp": oth}))
        to_sib.append(remote(piece, x_full.at[tp, c], one["as"], one["ar"], {"tp": sib}))
        forward.append(remote(x_full.at[oth, c], x_full.at[oth, c], one["fs"], fwr_sem.at[c],
                              {"tp": sib}))
    for c in range(CHUNKS):
        to_oth[c].start()
    for c in range(CHUNKS):
        to_sib[c].start()
    gain_copies = [
        remote(gain_hbm, gains.at[j], one["gs"], one["gr"], {"tp": (tp + j) % n_tp})
        for j in range(1, n_tp)
    ]
    pl.semaphore_signal(pair_sem, inc=1, device_id={"tp": sib}, device_id_type=MESH)
    greet(0)
    part_rows = channels // 2
    my_part = pl.multiple_of((sp % 2) * part_rows, part_rows)
    twin = sp + 1 - 2 * (sp % 2)

    def columns(owner):
        return pl.ds(pl.multiple_of(owner * width, width), width)

    def slot(pos):
        return ps_v.at[pl.ds(pos * channels + my_part, part_rows)]

    weight_copies = [
        remote(src, dst, one["ws"], one["wr"], {"tp": peer})
        for src, dst, peer in (
            (ps.at[pl.ds(my_part, part_rows), columns(oth)], slot(1), oth),
            (ps.at[pl.ds(my_part, part_rows), columns(diag)], slot(3), diag),
            (ps.at[:, columns(sib)], ps_v.at[pl.ds(2 * channels, channels)], sib),
        )
    ]
    weight_forward = [
        remote(slot(pos), slot(pos), one["vs"], one["vr"], {"sp": twin}) for pos in (1, 3)
    ]
    other_copies = [
        remote(src, par_ref.at[1, at], one["os"], one["or"], {"tp": oth})
        for src, at in zip(par_hbm, par_parts)
    ] + [remote(cq_ref.at[0], cq_ref.at[1], one["cs"], one["cr"], {"tp": oth})]
    rest_copy = remote(rp_out, rp_in, one["rs"], one["rr"], {"tp": oth})

    def pass_on(c):
        to_oth[c].wait_recv()
        forward[c].start()

    sub = lax.broadcasted_iota(jnp.int32, (8, 128), 0)
    top = sub < 4

    def pack(s, first):
        even = par_ref[s, pl.ds(first, 8, stride=2), :]
        odd = par_ref[s, pl.ds(first + 1, 8, stride=2), :]
        return jnp.concatenate([even, odd], axis=1)

    iv_load.wait()
    loaded("par")
    decay, turn = pack(0, 0), pack(0, dirs_groups)
    den = decay * decay + turn * turn
    td, dd = turn / den, decay / den

    def factors(k, carry):
        iv = jnp.where(top, iv_s[0, k], iv_s[0, rows - 1 - k])
        damp = -decay * iv
        square, sine = half_turns(turn * iv)
        e = jnp.exp(damp)
        cosine = 1.0 - 2.0 * square
        f_im = e * sine
        lift = expm1_of(damp, e) * cosine - 2.0 * square
        at = pl.ds(pl.multiple_of(k * 8, 8), 8)
        fr_ref[at, :] = e * cosine
        fi_ref[at, :] = f_im
        gr_ref[at, :] = td * f_im - dd * lift
        gi_ref[at, :] = -(dd * f_im + td * lift)
        return carry

    lax.fori_loop(0, 3 * rows // 4, factors, 0, unroll=4)
    greeted(0)
    if rounds > 1:
        greet(1)
    pl.semaphore_wait(pair_sem, 1)
    for copy in gain_copies:
        copy.start()
    lax.fori_loop(3 * rows // 4, rows, factors, 0, unroll=4)

    def put(ref, k, value):
        ref[pl.ds(pl.multiple_of(k * 8, 8), 4), :] = value[:4]
        ref[pl.ds(pl.multiple_of((rows - 1 - k) * 8, 8) + 4, 4), :] = value[4:]

    def chain(k, carry):
        ar, ai, br, bi = carry
        at = pl.ds(pl.multiple_of(k * 8, 8), 8)
        back = pl.ds(pl.multiple_of((rows - 1 - k) * 8, 8), 8)
        fr, fi = fr_ref[at, :], fi_ref[at, :]
        ar, ai = fr * ar - fi * ai, fr * ai + fi * ar
        put(hr_ref, k, ar)
        put(hi_ref, k, ai)
        gr, gi = gr_ref[back, :], gi_ref[back, :]
        put(kr_ref, rows - 1 - k, gr * br - gi * bi)
        put(ki_ref, rows - 1 - k, gr * bi + gi * br)
        fr, fi = fr_ref[back, :], fi_ref[back, :]
        return ar, ai, fr * br - fi * bi, fr * bi + fi * br

    unit, zero = jnp.ones((8, 128), F32), jnp.zeros((8, 128), F32)
    lax.fori_loop(0, rows, chain, (unit, zero, unit, zero), unroll=4)
    if rounds > 1:
        greeted(1)
    for k in range(2, rounds):
        greet(k)
        if k < rounds - 1:
            greeted(k)
    pass_on(0)
    for part, (k_ref, h_ref) in enumerate(((kr_ref, hr_ref), (ki_ref, hi_ref))):
        for j in range(8):
            lanes = slice(j * 128, (j + 1) * 128)
            k_row[part, :, lanes] = k_ref[pl.ds(j, rows, stride=8), :]
            p_row[0, :, pl.ds(part * bt_ref.shape[2] + j * 128, 128)] = h_ref[pl.ds(j, rows, stride=8), :].astype(BF16)
    pass_on(1)
    drain(x_ref, one["bs"])
    for copy in weight_copies:
        copy.start()

    loaded("in", "rd")
    states = bt_ref.shape[2]
    per = rd_v.shape[2]
    half = states // 2
    group = channels * per // half
    spread = (lax.broadcasted_iota(jnp.int32, (per, half), 1) % per
              == lax.broadcasted_iota(jnp.int32, (per, half), 0)).astype(BF16)
    keep = ((lax.broadcasted_iota(jnp.int32, (channels, half), 1) // per)
            == (lax.broadcasted_iota(jnp.int32, (channels, half), 0) // group))
    left = lax.broadcasted_iota(jnp.int32, (group, 2 * per), 1) < per
    for part in range(2):
        for d in range(2):
            at, to = pl.ds(d * channels, channels), pl.ds(d * half, half)
            wide = dot(in_v[part, at, :].astype(BF16), spread)
            bt_ref[part, :, to] = jnp.where(keep, wide, 0.0).astype(BF16)
            wide = dot(rd_v[part, at, :].astype(BF16), spread)
            if part:
                wide = -wide
            rt_ref[part, :, to] = jnp.where(keep, wide, 0.0).astype(BF16)
            for q in range(channels // group // 2):
                pair = [rd_v[part, pl.ds(d * channels + g * group, group), :] for g in (2 * q, 2 * q + 1)]
                cq_ref[0, part, d, q] = jnp.concatenate(pair, axis=1).astype(BF16)
    rc_ref[...] = jnp.zeros_like(rc_ref)

    pass_on(2)
    for copy in other_copies:
        copy.start()
    loaded("gain", "w")
    others = gains.at[pl.ds(1, n_tp - 1)]
    drain(others, one["gr"])

    def gain_of(owner):
        return gains[(tp - owner + n_tp) % n_tp]

    def project(value, gain, first):
        wide = value.astype(F32)
        scaled = (wide * gain).astype(BF16)
        k = value.shape[1]
        term = dot(scaled, w_all[pl.ds(pl.multiple_of(first, k), k), :])
        return term, jnp.sum(wide * wide, axis=1, keepdims=True)

    projected = jnp.zeros((rows, 4 * channels), F32)
    squares = jnp.zeros((rows, 1), F32)
    t, s = project(x_ref[...], gain_ref[...], tp * width)
    projected, squares = projected + t, squares + s

    def whole(owner, projected, squares):
        value = jnp.concatenate([x_full[owner, c] for c in range(CHUNKS)], axis=1)
        t, s = project(value, gain_of(owner), owner * width)
        return projected + t, squares + s

    drain(x_full.at[sib], one["ar"])
    projected, squares = whole(sib, projected, squares)
    pass_on(3)
    projected, squares = whole(oth, projected, squares)
    if rounds > 2:
        greeted(rounds - 1)

    def interval_copy(r):
        return remote(iv_hbm, el_all.at[r], one["is"], one["ir"], {"sp": (sp + r) % n_sp})

    repeat(1, n_sp, lambda r: interval_copy(r).start())
    for c in range(CHUNKS):
        forward[c].wait_recv()
        t, s = project(x_full[diag, c], gain_of(diag)[:, c * cw:(c + 1) * cw], diag * width + c * cw)
        projected, squares = projected + t, squares + s
    projected = projected * lax.rsqrt(squares / (width * n_tp) + EPSILON)
    state_input = projected[:, 3 * channels:].astype(BF16)
    conv_value = projected[:, :channels].astype(BF16).astype(F32)
    conv_mix = projected[:, channels:2 * channels].astype(BF16).astype(F32)
    conv_gate = projected[:, 2 * channels:3 * channels].astype(BF16).astype(F32)
    src_ref[...] = (conv_mix * conv_value).astype(BF16)

    for j in range(4):
        lanes = slice(j * 256, (j + 1) * 256)
        dr = dot(state_input, bt_ref[0, :, lanes])
        di = dot(state_input, bt_ref[1, :, lanes])
        d_row[0, :, lanes] = dr
        d_row[1, :, lanes] = di
        kr, ki = k_row[0, :, lanes], k_row[1, :, lanes]
        er = jnp.sum(kr * dr - ki * di, axis=0, keepdims=True)
        ei = jnp.sum(kr * di + ki * dr, axis=0, keepdims=True)
        for h in range(2):
            q = (j % 2) * 2 + h
            e_out[j // 2, q:q + 1, :] = er[:, h * 128:(h + 1) * 128]
            e_out[j // 2, 4 + q:5 + q, :] = ei[:, h * 128:(h + 1) * 128]


    def edge_copy(r, s):
        return remote(e_out.at[jnp.where(sp + r < n_sp, 0, 1)], e_all.at[s, r], one["es"], one["er"], {"sp": (sp + r) % n_sp, "tp": oth if s else tp})

    def edges(act):
        def at(r):
            act(edge_copy(r, 0))
            act(edge_copy(r, 1))
        repeat(1, n_sp, at)

    halo_up = remote(src_ref.at[pl.ds(rows - 16, 16)], halo_ref.at[0], hs_sem.at[0], hr_sem.at[0],
                     {"sp": (sp + 1) % n_sp})
    halo_down = remote(src_ref.at[pl.ds(0, 16)], halo_ref.at[1], hs_sem.at[1], hr_sem.at[1],
                       {"sp": (sp + n_sp - 1) % n_sp})
    edges(lambda copy: copy.start())
    not_first, not_last = sp > 0, sp < n_sp - 1
    pl.when(not_last)(halo_up.start)
    pl.when(not_first)(halo_down.start)

    loaded("taps", "skip", "pc", "ps")
    edge = 16
    inner_rows = rows - 2 * edge
    pieces = (pl.ds(0, inner_rows), pl.ds(inner_rows, 2 * edge))
    source = src_ref[...].astype(F32)
    line = lax.broadcasted_iota(jnp.int32, (rows, channels), 0)
    previous = jnp.where(line == 0, 0.0, pltpu.roll(source, 1, 0))
    following = jnp.where(line == rows - 1, 0.0, pltpu.roll(source, rows - 1, 0))
    filtered = taps_ref[0:1, :] * previous + taps_ref[1:2, :] * source + taps_ref[2:3, :] * following
    conv_out = (conv_gate * filtered).astype(BF16)[edge:rows - edge]

    def ends(a):
        return jnp.concatenate([a[:edge], a[rows - edge:]], axis=0)

    end_gate, end_filtered = ends(conv_gate), ends(filtered)

    def products(branch, i):
        at = pieces[i]
        copies = [
            remote(po_ref.at[0, at], p1_in.at[at], one["ps"], p1r_sem.at[i], {"tp": sib}),
            remote(po_ref.at[1, at], pi_ref.at[0, at], one["ps"], one["pr"], {"tp": sib}),
            remote(po_ref.at[2, at], pi_ref.at[1, at], one["ps"], one["pr"], {"tp": oth}),
        ]
        po_ref[0, at, :] = dot(branch, pc_v[:, columns(diag)]).astype(BF16)
        copies[0].start()
        po_ref[1, at, :] = dot(branch, pc_v[:, columns(sib)]).astype(BF16)
        copies[1].start()
        kept = dot(branch, pc_v[:, columns(oth)])
        acc_ref[at, :] = dot(branch, pc_v[:, columns(tp)])
        return copies, kept

    def crossing(copies, kept, i):
        at = pieces[i]
        copies[0].wait_recv()
        po_ref[2, at, :] = (kept + p1_in[at, :].astype(F32)).astype(BF16)
        copies[2].start()

    conv_a, kept = products(conv_out, 0)
    kept_ref[...] = kept

    for part, ref in ((0, dr_ref), (1, di_ref)):
        for j in range(8):
            ref[pl.ds(j, rows, stride=8), :] = d_row[part, :, j * 128:(j + 1) * 128]


    def local(k, carry):
        hr, hi = carry
        at = pl.ds(pl.multiple_of(k * 8, 8), 8)
        back = pl.ds(pl.multiple_of((rows - 1 - k) * 8, 8), 8)
        dr = jnp.where(top, dr_ref[at, :], dr_ref[back, :])
        di = jnp.where(top, di_ref[at, :], di_ref[back, :])
        gr, gi = gr_ref[at, :], gi_ref[at, :]
        fr, fi = fr_ref[at, :], fi_ref[at, :]
        pr = gr * dr - gi * di
        pi = gr * di + gi * dr
        hr, hi = fr * hr + (pr - fi * hi), fr * hi + (pi + fi * hr)
        put(hr_ref, k, hr)
        put(hi_ref, k, hi)
        return hr, hi

    lax.fori_loop(0, rows, local, (zero, zero), unroll=8)
    response = state_input.astype(F32) * skip_ref[...]
    for part, ref in ((0, hr_ref), (1, hi_ref)):
        history = jnp.concatenate(
            [ref[pl.ds(j, rows, stride=8), :].astype(BF16) for j in range(8)], axis=1)
        response = response + dot_t(history, rt_ref[part])

    rp_out[...] = response.astype(BF16)
    rest_copy.start()
    crossing(conv_a, kept_ref[...], 0)
    drain(ps_v.at[pl.ds(0, 2 * channels)], one["wr"])
    for copy in weight_forward:
        copy.start()
    drain(par_ref.at[1], one["or"])
    decay_2, turn_2 = pack(1, 0), pack(1, dirs_groups)
    at_t = lax.broadcasted_iota(jnp.int32, (rows, rows), 0)
    at_s = lax.broadcasted_iota(jnp.int32, (rows, rows), 1)
    loaded("ivv")
    steps = iv_v[...]
    reach = (jnp.sum(jnp.where(at_s <= at_t, steps, 0.0), axis=1, keepdims=True),
             jnp.sum(jnp.where(at_s >= at_t, steps, 0.0), axis=1, keepdims=True))
    for j in range(8):
        square, sine = half_turns(turn_2[j:j + 1, :] * reach[j // 4])
        e = jnp.exp(-decay_2[j:j + 1, :] * reach[j // 4])
        p_row[1, :, j * 128:(j + 1) * 128] = (e * (1.0 - 2.0 * square)).astype(BF16)
        p_row[1, :, states + j * 128:states + (j + 1) * 128] = (e * sine).astype(BF16)
    pl.when(not_first)(halo_up.wait_recv)
    pl.when(not_last)(halo_down.wait_recv)
    before = jnp.where(not_first, halo_ref[0].astype(F32)[15:16, :], 0.0) * taps_ref[0:1, :]
    after = jnp.where(not_last, halo_ref[1].astype(F32)[0:1, :], 0.0) * taps_ref[2:3, :]
    end_line = lax.broadcasted_iota(jnp.int32, (2 * edge, channels), 0)
    end_filtered = end_filtered + jnp.where(
        end_line == 0, before, jnp.where(end_line == 2 * edge - 1, after, 0.0))
    conv_b, kept_b = products((end_gate * end_filtered).astype(BF16), 1)

    far = pl.ds(1, n_sp - 1)
    drain(el_all.at[far], one["ir"])

    def both_of(full, d):
        return jnp.concatenate([full[d * 4:d * 4 + 4], full[d * 4:d * 4 + 4]], axis=0)

    def init_of(s, d):
        starts = [2 * dirs_groups + d * 16 + part * 8 for part in range(2)]
        parts = [
            jnp.concatenate([par_ref[s, pl.ds(at, 4, stride=2), :],
                             par_ref[s, pl.ds(at + 1, 4, stride=2), :]], axis=1)
            for at in starts
        ]
        return jnp.concatenate(parts, axis=0)

    decays = [[both_of(full, d) for d in range(2)] for full in (decay, decay_2)]
    turns = [[both_of(full, d) for d in range(2)] for full in (turn, turn_2)]

    def weight(damping, turning, span):
        square, sine = half_turns(turning * span)
        e = jnp.exp(-damping * span)
        return e * (1.0 - 2.0 * square), jnp.where(top, -e * sine, e * sine)

    def apply(w, tile):
        return w[0] * tile + w[1] * pltpu.roll(tile, 4, 0)

    def elapsed(r):
        return jnp.sum(el_all[r], axis=1, keepdims=True)

    none = jnp.zeros((1, 1), F32)

    def ahead(r, carry):
        total, inside = carry
        span_ref[r] = jnp.broadcast_to(total, (1, 128))
        step = elapsed(r)
        return total + step, inside + step * jnp.where(sp - r >= 0, 1.0, 0.0)

    total, inside = fold(1, n_sp, ahead, (none, none))

    def behind(i, total):
        r = n_sp - i
        mine = sp - r >= 0
        span = jnp.where(mine, span_ref[r], jnp.broadcast_to(total, (1, 128)))
        for s in range(2):
            w = weight(jnp.where(mine, *decays[s]), jnp.where(mine, *turns[s]), span)
            wa_ref[s, r] = w[0]
            wb_ref[s, r] = w[1]
        return total + elapsed(r)

    fold(1, n_sp, behind, none)
    outside = none

    def beyond(r, acc):
        return acc + elapsed(r) * jnp.where(sp - r >= 0, 0.0, 1.0)

    outside = fold(1, n_sp, beyond, none)
    from_start = [
        tuple(apply(weight(decays[s][d], turns[s][d], (inside, outside)[d]), init_of(s, d))
              for d in range(2))
        for s in range(2)
    ]

    crossing(conv_b, kept_b, 1)

    rest_copy.wait_recv()
    drain(cq_ref.at[1], one["cr"])
    drain(e_all.at[:, far], one["er"])
    for s in range(2):
        def combine(r, carry):
            h0, h1 = carry
            moved = apply((wa_ref[s, r], wb_ref[s, r]), e_all[s, r])
            mine = sp - r >= 0
            return h0 + jnp.where(mine, moved, 0.0), h1 + jnp.where(mine, 0.0, moved)

        entering = fold(1, n_sp, combine, from_start[s])
        for d in range(2):
            for q in range(channels // group // 2):
                hr, hi = entering[d][q:q + 1, :], entering[d][4 + q:5 + q, :]
                cr, ci = (cq_ref[s, part, d, q].astype(F32) for part in range(2))
                for part, value in ((0, cr * hr - ci * hi), (1, -(cr * hi + ci * hr))):
                    for side in range(2):
                        at = pl.ds((2 * q + side) * group, group)
                        lanes = pl.ds(part * states + d * half + q * 128, 128)
                        rc_ref[s, at, lanes] = jnp.where(
                            left if side == 0 else ~left, value, 0.0).astype(BF16)
    gated = []
    for s in range(2):
        full = response if s == 0 else rp_in[...].astype(F32)
        full = full + dot_t(p_row[s], rc_ref[s])
        inner = 0.7978845608028654 * (full + 0.044715 * (full * full * full))
        gated.append((0.5 * full * (1.0 + jnp.tanh(inner))).astype(BF16))
    state_out = jnp.concatenate(gated, axis=1)
    so_ref[...] = state_out
    state_copy = remote(so_ref, so_in, one["ss"], one["sr"], {"tp": sib})
    state_copy.start()
    drain(ps_v.at[pl.ds(0, channels)], one["vr"])
    total = dot(state_out, ps_v[:2 * channels])
    drain(pi_ref, one["pr"])
    base = acc_ref[...] + pi_ref[0].astype(F32) + pi_ref[1].astype(F32)
    total = total + jnp.concatenate(
        [base[inner_rows:inner_rows + edge], base[:inner_rows], base[inner_rows + edge:]], axis=0)
    state_copy.wait_recv()
    out_ref[...] = (total + dot(so_in[...], ps_v[2 * channels:])).astype(BF16)

    pl.when(not_last)(halo_up.wait_send)
    pl.when(not_first)(halo_down.wait_send)
    for ref, name in (
            (x_ref, "as"), (x_ref, "fs"), (others, "gs"), (el_all.at[far], "is"),
            (e_all.at[:, far], "es"), (po_ref, "ps"), (ps_v.at[pl.ds(0, 2 * channels)], "ws"),
            (ps_v.at[pl.ds(0, channels)], "vs"), (par_ref.at[0], "os"), (cq_ref.at[0], "cs"),
            (rp_out, "rs"), (so_ref, "ss")):
        drain(ref, one[name])


def per_device(
    n_sp, n_tp,
    stream, norm_gain, w_value, w_mix, w_gate, w_state, conv_taps, skip_gain, decay_rate, turn_rate,
    input_real, input_imag, read_real, read_imag, initial_state, intervals, proj_conv, proj_state,
):
    rows, width = stream.shape
    channels = w_value.shape[1]
    dirs, groups, per, group = input_real.shape
    states = dirs * groups * per
    cw = width // CHUNKS
    hbm = pl.BlockSpec(memory_space=pltpu.HBM)
    dma = lambda n: pltpu.SemaphoreType.DMA((n,))
    packed = pltpu.VMEM((rows * 8, 128), F32)
    rows_of = lambda m: jnp.swapaxes(m, 2, 3).reshape(dirs * groups * group, per)
    return pl.pallas_call(
        functools.partial(kernel, n_sp, n_tp),
        out_shape=jax.ShapeDtypeStruct((rows, width), BF16),
        in_specs=[hbm] * 18,
        out_specs=pl.BlockSpec(memory_space=pltpu.VMEM),
        scratch_shapes=[
            pltpu.VMEM((rows, width), BF16),
            pltpu.VMEM((1, width), F32),
            pltpu.VMEM(conv_taps.shape, F32),
            pltpu.VMEM((1, channels), F32),
            pltpu.VMEM((2, 4 * dirs * groups, per), F32),
            pltpu.SMEM((1, rows), F32),
            pltpu.VMEM((1, rows), F32),
            pltpu.VMEM((width * n_tp, 4 * channels), BF16),
            pltpu.VMEM((channels, width * n_tp), BF16),
            pltpu.VMEM((n_tp * channels, width), BF16),
            pltpu.VMEM((2, dirs * groups * group, per), F32),
            pltpu.VMEM((2, dirs * groups * group, per), F32),
            pltpu.VMEM((n_tp, CHUNKS, rows, cw), BF16),
            pltpu.VMEM((n_tp, 1, width), F32),
            pltpu.VMEM((n_sp, 1, rows), F32),
            packed, packed, packed, packed, packed, packed, packed, packed, packed, packed,
            pltpu.VMEM((2, rows, states), F32),
            pltpu.VMEM((2, rows, states), F32),
            pltpu.VMEM((2, rows, 2 * states), BF16),
            pltpu.VMEM((2, channels, states), BF16),
            pltpu.VMEM((2, channels, states), BF16),
            pltpu.VMEM((2, channels, 2 * states), BF16),
            pltpu.VMEM((2, 2, dirs, groups // 2, group, 2 * per), BF16),
            pltpu.VMEM((rows, channels), BF16),
            pltpu.VMEM((2, 16, channels), BF16),
            pltpu.VMEM((2, 8, 128), F32),
            pltpu.VMEM((2, n_sp, 8, 128), F32),
            pltpu.VMEM((n_sp, 1, 128), F32),
            pltpu.VMEM((2, n_sp, 8, 128), F32),
            pltpu.VMEM((2, n_sp, 8, 128), F32),
            pltpu.VMEM((3, rows, width), BF16),
            pltpu.VMEM((rows, width), BF16),
            pltpu.VMEM((2, rows, width), BF16),
            pltpu.VMEM((rows, width), F32),
            pltpu.VMEM((rows, 2 * channels), BF16),
            pltpu.VMEM((rows, 2 * channels), BF16),
            pltpu.VMEM((rows, channels), BF16),
            pltpu.VMEM((rows, channels), BF16),
            pltpu.VMEM((rows - 32, width), F32),
            dma(12), dma(CHUNKS), dma(CHUNKS), dma(24), dma(2), dma(2), dma(2),
            pltpu.SemaphoreType.REGULAR((max(2, (n_sp - 1).bit_length()),)),
            pltpu.SemaphoreType.REGULAR,
        ],
        compiler_params=pltpu.CompilerParams(
            collective_id=0, has_side_effects=True, vmem_limit_bytes=48 * 1024 * 1024),
    )(*(pltpu.with_memory_space_constraint(a, pltpu.HBM) for a in (
        stream, norm_gain.reshape(1, width), w_value, w_mix, w_gate, w_state, conv_taps,
        skip_gain.reshape(1, channels),
        decay_rate.reshape(dirs * groups, per), turn_rate.reshape(dirs * groups, per),
        rows_of(input_real), rows_of(input_imag),
        read_real.reshape(dirs * groups * group, per), read_imag.reshape(dirs * groups * group, per),
        initial_state.reshape(dirs * 2 * groups, per), intervals.reshape(1, rows),
        proj_conv, proj_state,
    )))


def solution(mesh):
    return jax.shard_map(
        functools.partial(per_device, mesh.shape["sp"], mesh.shape["tp"]),
        mesh=mesh,
        in_specs=(
            P("sp", "tp"), P("tp"), P(None, "tp"), P(None, "tp"), P(None, "tp"), P(None, "tp"),
            P(None, "tp"), P("tp"), P(None, "tp", None), P(None, "tp", None),
            P(None, "tp", None, None), P(None, "tp", None, None), P(None, "tp", None, None),
            P(None, "tp", None, None), P(None, None, "tp", None), P("sp"), P("tp", None),
            P("tp", None),
        ),
        out_specs=P("sp", "tp"),
        check_vma=False,
    )
```

```python
import functools

import jax
import jax.numpy as jnp
from jax import lax
from jax.experimental import pallas as pl
from jax.experimental.pallas import tpu as pltpu
from jax.sharding import PartitionSpec as P

EPSILON = 1e-06
MESH = pl.DeviceIdType.MESH
F32 = jnp.float32
BF16 = jnp.bfloat16
CHUNKS = 4
SHARE = 4


def dot(a, b):
    return jnp.dot(a, b, preferred_element_type=F32)


def dot_t(a, b):
    return lax.dot_general(a, b, (((1,), (1,)), ((), ())), preferred_element_type=F32)


def half_turns(angle):
    theta = 0.5 * angle
    n = jnp.floor(theta * 0.6366197723675814 + 0.5)
    r = theta - n * 1.5703125
    r = r - n * 0.00048351287841796875
    r = r - n * 3.1385570764541626e-07
    r = r - n * 6.077100627776710e-11
    odd = (n - 2.0 * jnp.floor(0.5 * n)) > 0.5
    z = r * r
    s = r + r * z * ((-1.9515295891e-4 * z + 8.3321608736e-3) * z - 1.6666654611e-1)
    c = 1.0 - 0.5 * z + z * z * (
        (2.443315711809948e-5 * z - 1.388731625493765e-3) * z + 4.166664568298827e-2
    )
    square = jnp.where(odd, c * c, s * s)
    double = 2.0 * s * c
    return square, jnp.where(odd, -double, double)


def expm1_of(x, e):
    p = 1.0 + x * (1.0 / 7.0)
    for k in (6.0, 5.0, 4.0, 3.0, 2.0):
        p = 1.0 + x * p * (1.0 / k)
    return jnp.where(x > -0.35, x * p, e - 1.0)


def repeat(lo, hi, body):
    if hi - lo <= 16:
        for i in range(lo, hi):
            body(i)
    else:
        def step(i, carry):
            body(i)
            return carry
        lax.fori_loop(lo, hi, step, 0)


def fold(lo, hi, body, init):
    if hi - lo <= 16:
        for i in range(lo, hi):
            init = body(i, init)
        return init
    return lax.fori_loop(lo, hi, body, init)


def kernel(
    n_sp, n_tp,
    x_hbm, gain_hbm, wv, wm, wg, ws, taps_hbm, skip_hbm, decay_hbm, turn_hbm,
    inr, ini, rdr, rdi, init_hbm, iv_hbm, pc, ps,
    out_ref,
    x_ref, gain_ref, taps_ref, skip_ref, par_ref, iv_s, iv_v,
    w_all, pc_v, ps_v, in_v, rd_v, x_full, gains, el_all, fr_ref, fi_ref, gr_ref, gi_ref,
    dr_ref, di_ref, hr_ref, hi_ref, kr_ref, ki_ref, k_row, d_row, p_row,
    bt_ref, rt_ref, rc_ref, cq_ref, src_ref, halo_ref, e_out, e_all,
    span_ref, wa_ref, wb_ref, po_ref, p1_in, pi_ref, pd_ref, acc_ref, so_ref, so_in,
    rp_out, rp_in, xs_ref,
    load_sem, fwr_sem, br_sem, gr_sem, one_sem, hs_sem, hr_sem, p1r_sem, greet_sem, pair_sem,
):
    tp, sp = lax.axis_index("tp"), lax.axis_index("sp")
    rows, width = x_hbm.shape
    channels = wv.shape[1]
    y, core = tp // 2, tp % 2
    sib = y * 2 + 1 - core
    oth = (1 - y) * 2 + core
    diag = (1 - y) * 2 + 1 - core
    cw = width // CHUNKS

    names = ("bs", "as", "ar", "fs", "gs", "ds", "dr", "is", "ir", "es", "er", "ps", "pr", "ws", "wr",
             "vs", "vr", "qr", "os", "or", "cs", "cr", "rs", "rr", "ss", "sr")
    one = {name: one_sem.at[i] for i, name in enumerate(names)}
    loads = {}

    def load(name, whole, *pairs):
        sem = load_sem.at[len(loads)]
        loads[name] = whole, sem
        for src, dst in pairs:
            pltpu.make_async_copy(src, dst, sem).start()

    def remote(src, dst, send, recv, where):
        return pltpu.make_async_remote_copy(
            src_ref=src, dst_ref=dst, send_sem=send, recv_sem=recv,
            device_id=where, device_id_type=MESH)

    def drain(ref, sem):
        remote(ref, ref, sem, sem, {"tp": sib}).wait_recv()

    def loaded(*names):
        for name in names:
            drain(*loads[name])

    def near(step, act):
        for s in (-step, step):
            @pl.when((sp + s >= 0) & (sp + s < n_sp))
            def _():
                act(sp + s)

    def near_count(step):
        return jnp.where(sp - step >= 0, 1, 0) + jnp.where(sp + step < n_sp, 1, 0)

    def greet(k):
        near(1 << k, lambda where: pl.semaphore_signal(
            greet_sem.at[k], inc=1, device_id={"sp": where}, device_id_type=MESH))

    def greeted(k):
        pl.semaphore_wait(greet_sem.at[k], near_count(1 << k))

    rounds = greet_sem.shape[0]
    barrier = pltpu.get_barrier_semaphore()
    for peer in (sib, oth):
        pl.semaphore_signal(barrier, inc=1, device_id={"tp": peer}, device_id_type=MESH)
    near(1, lambda where: pl.semaphore_signal(
        barrier, inc=1, device_id={"sp": where}, device_id_type=MESH))
    load("x", x_ref, (x_hbm, x_ref))
    iv_load = pltpu.make_async_copy(iv_hbm, iv_s, load_sem.at[len(loads)])
    iv_load.start()
    loads["iv"] = None
    dirs_groups = decay_hbm.shape[0]
    par_parts = (pl.ds(0, dirs_groups), pl.ds(dirs_groups, dirs_groups),
                 pl.ds(2 * dirs_groups, 2 * dirs_groups))
    par_hbm = (decay_hbm, turn_hbm, init_hbm)
    load("par", par_ref.at[0], *((src, par_ref.at[0, at]) for src, at in zip(par_hbm, par_parts)))
    load("ivv", iv_v, (iv_hbm, iv_v))
    load("gain", gain_ref, (gain_hbm, gain_ref))
    load("in", in_v, (inr, in_v.at[0]), (ini, in_v.at[1]))
    load("rd", rd_v, (rdr, rd_v.at[0]), (rdi, rd_v.at[1]))
    load("w", w_all, *((w, w_all.at[:, pl.ds(j * channels, channels)])
                       for j, w in enumerate((wv, wm, wg, ws))))
    load("taps", taps_ref, (taps_hbm, taps_ref))
    load("skip", skip_ref, (skip_hbm, skip_ref))
    load("pc", pc_v, (pc, pc_v))
    own = ps.at[:, pl.ds(pl.multiple_of(tp * width, width), width)]
    load("ps", ps_v.at[pl.ds(0, channels)], (own, ps_v.at[pl.ds(0, channels)]))
    pl.semaphore_wait(barrier, 2 + near_count(1))
    loaded("x", "gain")

    last = CHUNKS - 1
    half_rows = rows // 2
    upper, lower = pl.ds(0, half_rows), pl.ds(half_rows, half_rows)

    def block(ref, c, part=None):
        return ref.at[:, pl.ds(c * cw, cw)] if part is None else ref.at[part, pl.ds(c * cw, cw)]

    def landing(owner, c, part=None):
        return x_full.at[owner, c] if part is None else x_full.at[owner, c, part]

    spans = [(c, None) for c in range(last)] + [(last, upper), (last, lower)]
    to_oth = [
        remote(block(x_ref, *span), landing(tp, *span), one["bs"], br_sem.at[i], {"tp": oth})
        for i, span in enumerate(spans)
    ]
    to_sib = remote(x_ref, xs_ref, one["as"], one["ar"], {"tp": sib})
    forward = [
        remote(landing(oth, *span), landing(oth, *span), one["fs"], fwr_sem.at[i], {"tp": sib})
        for i, span in enumerate(spans[:-1])
    ]
    to_diag = remote(block(x_ref, *spans[-1]), landing(tp, *spans[-1]), one["ds"], one["dr"],
                     {"tp": diag})
    gain_copies = [
        remote(gain_ref, gains.at[j], one["gs"], gr_sem.at[j], {"tp": peer})
        for j, peer in enumerate((oth, sib, diag))
    ]
    gain_copies[0].start()
    for copy in to_oth:
        copy.start()
    gain_copies[1].start()
    to_sib.start()
    pl.semaphore_signal(pair_sem, inc=1, device_id={"tp": sib}, device_id_type=MESH)
    greet(0)
    part_rows = channels // SHARE
    my_part = pl.multiple_of((sp % SHARE) * part_rows, part_rows)
    mates = [sp // SHARE * SHARE + (sp + k) % SHARE for k in range(1, SHARE)]

    def columns(owner):
        return pl.ds(pl.multiple_of(owner * width, width), width)

    def slot(pos):
        return ps_v.at[pl.ds(pos * channels + my_part, part_rows)]

    weight_copies = [
        remote(src, dst, one["ws"], one["wr"], {"tp": peer})
        for src, dst, peer in (
            (ps.at[pl.ds(my_part, part_rows), columns(oth)], slot(1), oth),
            (ps.at[pl.ds(my_part, part_rows), columns(diag)], slot(3), diag),
            (ps.at[:, columns(sib)], ps_v.at[pl.ds(2 * channels, channels)], sib),
        )
    ]
    weight_forward = [
        remote(slot(pos), slot(pos), one["vs"], one["vr"], {"sp": mate})
        for mate in mates for pos in (1, 3)
    ]
    other_copies = [
        remote(src, par_ref.at[1, at], one["os"], one["or"], {"tp": oth})
        for src, at in zip(par_hbm, par_parts)
    ] + [remote(cq_ref.at[0], cq_ref.at[1], one["cs"], one["cr"], {"tp": oth})]
    rest_copy = remote(rp_out, rp_in, one["rs"], one["rr"], {"tp": oth})

    def pass_on(c):
        to_oth[c].wait_recv()
        forward[c].start()

    sub = lax.broadcasted_iota(jnp.int32, (8, 128), 0)
    top = sub < 4

    def pack(s, first):
        even = par_ref[s, pl.ds(first, 8, stride=2), :]
        odd = par_ref[s, pl.ds(first + 1, 8, stride=2), :]
        return jnp.concatenate([even, odd], axis=1)

    iv_load.wait()
    loaded("par")
    decay, turn = pack(0, 0), pack(0, dirs_groups)
    den = decay * decay + turn * turn
    td, dd = turn / den, decay / den

    def factors(k, carry):
        iv = jnp.where(top, iv_s[0, k], iv_s[0, rows - 1 - k])
        damp = -decay * iv
        square, sine = half_turns(turn * iv)
        e = jnp.exp(damp)
        cosine = 1.0 - 2.0 * square
        f_im = e * sine
        lift = expm1_of(damp, e) * cosine - 2.0 * square
        at = pl.ds(pl.multiple_of(k * 8, 8), 8)
        fr_ref[at, :] = e * cosine
        fi_ref[at, :] = f_im
        gr_ref[at, :] = td * f_im - dd * lift
        gi_ref[at, :] = -(dd * f_im + td * lift)
        return carry

    lax.fori_loop(0, 3 * rows // 4, factors, 0, unroll=4)
    greeted(0)
    if rounds > 1:
        greet(1)
    pl.semaphore_wait(pair_sem, 1)
    gain_copies[2].start()
    to_diag.start()
    for copy in other_copies[:-1]:
        copy.start()
    lax.fori_loop(3 * rows // 4, rows, factors, 0, unroll=4)

    def put(ref, k, value):
        ref[pl.ds(pl.multiple_of(k * 8, 8), 4), :] = value[:4]
        ref[pl.ds(pl.multiple_of((rows - 1 - k) * 8, 8) + 4, 4), :] = value[4:]

    def chain(k, carry):
        ar, ai, br, bi = carry
        at = pl.ds(pl.multiple_of(k * 8, 8), 8)
        back = pl.ds(pl.multiple_of((rows - 1 - k) * 8, 8), 8)
        fr, fi = fr_ref[at, :], fi_ref[at, :]
        ar, ai = fr * ar - fi * ai, fr * ai + fi * ar
        put(hr_ref, k, ar)
        put(hi_ref, k, ai)
        gr, gi = gr_ref[back, :], gi_ref[back, :]
        put(kr_ref, rows - 1 - k, gr * br - gi * bi)
        put(ki_ref, rows - 1 - k, gr * bi + gi * br)
        fr, fi = fr_ref[back, :], fi_ref[back, :]
        return ar, ai, fr * br - fi * bi, fr * bi + fi * br

    unit, zero = jnp.ones((8, 128), F32), jnp.zeros((8, 128), F32)
    lax.fori_loop(0, rows, chain, (unit, zero, unit, zero), unroll=4)
    if rounds > 1:
        greeted(1)
    for k in range(2, rounds):
        greet(k)
        if k < rounds - 1:
            greeted(k)

    for copy in weight_copies:
        copy.start()
    loaded("in", "rd")
    states = bt_ref.shape[2]
    per = rd_v.shape[2]
    half = states // 2
    group = channels * per // half
    spread = (lax.broadcasted_iota(jnp.int32, (per, half), 1) % per
              == lax.broadcasted_iota(jnp.int32, (per, half), 0)).astype(BF16)
    keep = ((lax.broadcasted_iota(jnp.int32, (channels, half), 1) // per)
            == (lax.broadcasted_iota(jnp.int32, (channels, half), 0) // group))
    left = lax.broadcasted_iota(jnp.int32, (group, 2 * per), 1) < per
    for part in range(2):
        for d in range(2):
            at, to = pl.ds(d * channels, channels), pl.ds(d * half, half)
            wide = dot(in_v[part, at, :].astype(BF16), spread)
            bt_ref[part, :, to] = jnp.where(keep, wide, 0.0).astype(BF16)
            wide = dot(rd_v[part, at, :].astype(BF16), spread)
            if part:
                wide = -wide
            rt_ref[part, :, to] = jnp.where(keep, wide, 0.0).astype(BF16)
            for q in range(channels // group // 2):
                pair = [rd_v[part, pl.ds(d * channels + g * group, group), :] for g in (2 * q, 2 * q + 1)]
                cq_ref[0, part, d, q] = jnp.concatenate(pair, axis=1).astype(BF16)
    rc_ref[...] = jnp.zeros_like(rc_ref)

    pass_on(0)
    for part, (k_ref, h_ref) in enumerate(((kr_ref, hr_ref), (ki_ref, hi_ref))):
        for j in range(8):
            lanes = slice(j * 128, (j + 1) * 128)
            k_row[part, :, lanes] = k_ref[pl.ds(j, rows, stride=8), :]
            p_row[0, :, pl.ds(part * states + j * 128, 128)] = h_ref[pl.ds(j, rows, stride=8), :].astype(BF16)
    pass_on(1)
    other_copies[-1].start()
    loaded("w")
    state_lanes = slice(3 * channels, None)
    conv_lanes = slice(0, 3 * channels)

    def scaled(value, gain):
        return (value.astype(F32) * gain).astype(BF16)

    def power(value):
        wide = value.astype(F32)
        return jnp.sum(wide * wide, axis=1, keepdims=True)

    def weight_rows(owner, first, count):
        return pl.ds(pl.multiple_of(owner * width + first, cw), count)

    def chunks_of(owner, count):
        return jnp.concatenate([x_full[owner, c] for c in range(count)], axis=1)

    def project(value, gain, owner, count):
        return dot(scaled(value, gain), w_all[weight_rows(owner, 0, count), :]), power(value)

    projected, squares = project(x_ref[...], gain_ref[...], tp, width)
    drain(xs_ref, one["ar"])
    gain_copies[1].wait_recv()
    t, s = project(xs_ref[...], gains[1], sib, width)
    projected, squares = projected + t, squares + s
    pass_on(2)
    gain_copies[0].wait_recv()
    t, s = project(chunks_of(oth, last), gains[0][:, :last * cw], oth, last * cw)
    projected, squares = projected + t, squares + s
    pass_on(3)
    if rounds > 2:
        greeted(rounds - 1)

    def interval_copy(r):
        return remote(iv_v, el_all.at[r], one["is"], one["ir"], {"sp": (sp + r) % n_sp})

    loaded("ivv")
    repeat(1, n_sp, lambda r: interval_copy(r).start())
    gain_copies[2].wait_recv()
    for c in range(last):
        forward[c].wait_recv()
    t, s = project(chunks_of(diag, last), gains[2][:, :last * cw], diag, last * cw)
    projected, squares = projected + t, squares + s
    to_oth[last + 1].wait_recv()
    tails = []
    for owner, at in ((oth, 0), (diag, 2)):
        if owner is diag:
            forward[last].wait_recv()
            to_diag.wait_recv()
        value = x_full[owner, last]
        squares = squares + power(value)
        tails.append((scaled(value, gains[at][:, last * cw:]), weight_rows(owner, last * cw, cw)))
    inv_rms = lax.rsqrt(squares / (width * n_tp) + EPSILON)

    def finish(lanes):
        total = projected[:, lanes]
        for value, at in tails:
            total = total + dot(value, w_all[at, lanes])
        return total * inv_rms

    state_input = finish(state_lanes).astype(BF16)


    def edge_copy(r, s):
        return remote(e_out.at[jnp.where(sp + r < n_sp, 0, 1)], e_all.at[s, r], one["es"], one["er"],
                      {"sp": (sp + r) % n_sp, "tp": oth if s else tp})

    def send_edges(lo, hi):
        def at(r, carry):
            edge_copy(r, 0).start()
            edge_copy(r, 1).start()
            return carry
        lax.fori_loop(lo, hi, at, 0)

    def find_edges(d):
        for i in range(2):
            lanes = slice(d * half + i * 256, d * half + (i + 1) * 256)
            dr = dot(state_input, bt_ref[0, :, lanes])
            di = dot(state_input, bt_ref[1, :, lanes])
            d_row[0, :, lanes] = dr
            d_row[1, :, lanes] = di
            kr, ki = k_row[0, :, lanes], k_row[1, :, lanes]
            er = jnp.sum(kr * dr - ki * di, axis=0, keepdims=True)
            ei = jnp.sum(kr * di + ki * dr, axis=0, keepdims=True)
            for h in range(2):
                q = i * 2 + h
                e_out[d, q:q + 1, :] = er[:, h * 128:(h + 1) * 128]
                e_out[d, 4 + q:5 + q, :] = ei[:, h * 128:(h + 1) * 128]

    find_edges(1)
    send_edges(n_sp - sp, n_sp)
    convs = finish(conv_lanes)
    conv_value = convs[:, :channels].astype(BF16).astype(F32)
    conv_mix = convs[:, channels:2 * channels].astype(BF16).astype(F32)
    conv_gate = convs[:, 2 * channels:].astype(BF16).astype(F32)
    src_ref[...] = (conv_mix * conv_value).astype(BF16)
    halo_up = remote(src_ref.at[pl.ds(rows - 16, 16)], halo_ref.at[0], hs_sem.at[0], hr_sem.at[0],
                     {"sp": (sp + 1) % n_sp})
    halo_down = remote(src_ref.at[pl.ds(0, 16)], halo_ref.at[1], hs_sem.at[1], hr_sem.at[1],
                       {"sp": (sp + n_sp - 1) % n_sp})
    not_first, not_last = sp > 0, sp < n_sp - 1
    pl.when(not_last)(halo_up.start)
    pl.when(not_first)(halo_down.start)
    loaded("taps", "skip", "pc", "ps")
    edge = 16
    inner_rows = rows - 2 * edge
    direct_rows = pd_ref.shape[0]
    inner, outer = (0, inner_rows), (inner_rows, 2 * edge)
    middle = (direct_rows, inner_rows - direct_rows)
    source = src_ref[...].astype(F32)
    line = lax.broadcasted_iota(jnp.int32, (rows, channels), 0)
    previous = jnp.where(line == 0, 0.0, pltpu.roll(source, 1, 0))
    following = jnp.where(line == rows - 1, 0.0, pltpu.roll(source, rows - 1, 0))
    filtered = taps_ref[0:1, :] * previous + taps_ref[1:2, :] * source + taps_ref[2:3, :] * following
    conv_out = (conv_gate * filtered).astype(BF16)[edge:rows - edge]

    def ends(a):
        return jnp.concatenate([a[:edge], a[rows - edge:]], axis=0)

    end_gate, end_filtered = ends(conv_gate), ends(filtered)

    def offer(branch, i, span):
        at = pl.ds(*span)
        po_ref[0, at, :] = dot(branch, pc_v[:, columns(diag)]).astype(BF16)
        copy = remote(po_ref.at[0, at], p1_in.at[at], one["ps"], p1r_sem.at[i], {"tp": sib})
        copy.start()
        return copy

    def crossing(branch, span):
        at = pl.ds(*span)
        kept = dot(branch, pc_v[:, columns(oth)])
        po_ref[2, at, :] = (kept + p1_in[at, :].astype(F32)).astype(BF16)
        copy = remote(po_ref.at[2, at], pi_ref.at[1, at], one["ps"], one["pr"], {"tp": oth})
        copy.start()

    def rest_of(branch, span):
        at = pl.ds(*span)
        po_ref[1, at, :] = dot(branch, pc_v[:, columns(sib)]).astype(BF16)
        copy = remote(po_ref.at[1, at], pi_ref.at[0, at], one["ps"], one["pr"], {"tp": sib})
        copy.start()
        acc_ref[at, :] = dot(branch, pc_v[:, columns(tp)])

    direct = pl.ds(0, direct_rows)
    direct_copies = [
        remote(po_ref.at[2, direct], pi_ref.at[1, direct], one["ps"], one["pr"], {"tp": oth}),
        remote(po_ref.at[0, direct], pd_ref, one["ps"], one["qr"], {"tp": diag}),
    ]
    for copy, at, owner in zip(direct_copies, (2, 0), (oth, diag)):
        po_ref[at, direct, :] = dot(conv_out[:direct_rows], pc_v[:, columns(owner)]).astype(BF16)
        copy.start()
    offered = offer(conv_out[direct_rows:], 0, middle)

    find_edges(0)

    for part, ref in ((0, dr_ref), (1, di_ref)):
        for j in range(8):
            ref[pl.ds(j, rows, stride=8), :] = d_row[part, :, j * 128:(j + 1) * 128]

    send_edges(1, n_sp - sp)
    drain(ps_v.at[pl.ds(0, channels + 2 * part_rows)], one["wr"])
    for copy in weight_forward:
        copy.start()

    def local(k, carry):
        hr, hi = carry
        at = pl.ds(pl.multiple_of(k * 8, 8), 8)
        back = pl.ds(pl.multiple_of((rows - 1 - k) * 8, 8), 8)
        dr = jnp.where(top, dr_ref[at, :], dr_ref[back, :])
        di = jnp.where(top, di_ref[at, :], di_ref[back, :])
        gr, gi = gr_ref[at, :], gi_ref[at, :]
        fr, fi = fr_ref[at, :], fi_ref[at, :]
        pr = gr * dr - gi * di
        pi = gr * di + gi * dr
        hr, hi = fr * hr + (pr - fi * hi), fr * hi + (pi + fi * hr)
        put(hr_ref, k, hr)
        put(hi_ref, k, hi)
        return hr, hi

    lax.fori_loop(0, rows, local, (zero, zero), unroll=8)
    response = state_input.astype(F32) * skip_ref[...]
    for part, ref in ((0, hr_ref), (1, hi_ref)):
        history = jnp.concatenate(
            [ref[pl.ds(j, rows, stride=8), :].astype(BF16) for j in range(8)], axis=1)
        response = response + dot_t(history, rt_ref[part])

    rp_out[...] = response.astype(BF16)
    rest_copy.start()
    offered.wait_recv()
    crossing(conv_out[direct_rows:], middle)
    pl.when(not_first)(halo_up.wait_recv)
    pl.when(not_last)(halo_down.wait_recv)
    before = jnp.where(not_first, halo_ref[0].astype(F32)[15:16, :], 0.0) * taps_ref[0:1, :]
    after = jnp.where(not_last, halo_ref[1].astype(F32)[0:1, :], 0.0) * taps_ref[2:3, :]
    end_line = lax.broadcasted_iota(jnp.int32, (2 * edge, channels), 0)
    end_filtered = end_filtered + jnp.where(
        end_line == 0, before, jnp.where(end_line == 2 * edge - 1, after, 0.0))
    conv_ends = (end_gate * end_filtered).astype(BF16)
    offered_ends = offer(conv_ends, 1, outer)
    rest_of(conv_out, inner)

    drain(par_ref.at[1], one["or"])
    decay_2, turn_2 = pack(1, 0), pack(1, dirs_groups)
    at_t = lax.broadcasted_iota(jnp.int32, (rows, rows), 0)
    at_s = lax.broadcasted_iota(jnp.int32, (rows, rows), 1)
    steps = iv_v[...]
    reach = (jnp.sum(jnp.where(at_s <= at_t, steps, 0.0), axis=1, keepdims=True),
             jnp.sum(jnp.where(at_s >= at_t, steps, 0.0), axis=1, keepdims=True))
    def reach_factors(j):
        square, sine = half_turns(turn_2[j:j + 1, :] * reach[j // 4])
        e = jnp.exp(-decay_2[j:j + 1, :] * reach[j // 4])
        p_row[1, :, j * 128:(j + 1) * 128] = (e * (1.0 - 2.0 * square)).astype(BF16)
        p_row[1, :, states + j * 128:states + (j + 1) * 128] = (e * sine).astype(BF16)
    for j in range(4):
        reach_factors(j)
    offered_ends.wait_recv()
    crossing(conv_ends, outer)
    for j in range(4, 8):
        reach_factors(j)
    rest_of(conv_ends, outer)
    far = pl.ds(1, n_sp - 1)
    drain(el_all.at[far], one["ir"])

    def both_of(full, d):
        return jnp.concatenate([full[d * 4:d * 4 + 4], full[d * 4:d * 4 + 4]], axis=0)

    def init_of(s, d):
        starts = [2 * dirs_groups + d * 16 + part * 8 for part in range(2)]
        parts = [
            jnp.concatenate([par_ref[s, pl.ds(at, 4, stride=2), :],
                             par_ref[s, pl.ds(at + 1, 4, stride=2), :]], axis=1)
            for at in starts
        ]
        return jnp.concatenate(parts, axis=0)

    decays = [[both_of(full, d) for d in range(2)] for full in (decay, decay_2)]
    turns = [[both_of(full, d) for d in range(2)] for full in (turn, turn_2)]

    def weight(damping, turning, span):
        square, sine = half_turns(turning * span)
        e = jnp.exp(-damping * span)
        return e * (1.0 - 2.0 * square), jnp.where(top, -e * sine, e * sine)

    def apply(w, tile):
        return w[0] * tile + w[1] * pltpu.roll(tile, 4, 0)

    def elapsed(r):
        return jnp.sum(el_all[r], axis=1, keepdims=True)

    none = jnp.zeros((1, 1), F32)

    def ahead(r, carry):
        total, inside = carry
        span_ref[r] = jnp.broadcast_to(total, (1, 128))
        step = elapsed(r)
        return total + step, inside + step * jnp.where(sp - r >= 0, 1.0, 0.0)

    total, inside = fold(1, n_sp, ahead, (none, none))

    def behind(i, total):
        r = n_sp - i
        mine = sp - r >= 0
        span = jnp.where(mine, span_ref[r], jnp.broadcast_to(total, (1, 128)))
        for s in range(2):
            w = weight(jnp.where(mine, *decays[s]), jnp.where(mine, *turns[s]), span)
            wa_ref[s, r] = w[0]
            wb_ref[s, r] = w[1]
        return total + elapsed(r)

    fold(1, n_sp, behind, none)
    outside = none

    def beyond(r, acc):
        return acc + elapsed(r) * jnp.where(sp - r >= 0, 0.0, 1.0)

    outside = fold(1, n_sp, beyond, none)
    from_start = [
        tuple(apply(weight(decays[s][d], turns[s][d], (inside, outside)[d]), init_of(s, d))
              for d in range(2))
        for s in range(2)
    ]

    rest_copy.wait_recv()
    drain(cq_ref.at[1], one["cr"])
    drain(e_all.at[:, far], one["er"])
    for s in range(2):
        def combine(r, carry):
            h0, h1 = carry
            moved = apply((wa_ref[s, r], wb_ref[s, r]), e_all[s, r])
            mine = sp - r >= 0
            return h0 + jnp.where(mine, moved, 0.0), h1 + jnp.where(mine, 0.0, moved)

        entering = fold(1, n_sp, combine, from_start[s])
        for d in range(2):
            for q in range(channels // group // 2):
                hr, hi = entering[d][q:q + 1, :], entering[d][4 + q:5 + q, :]
                cr, ci = (cq_ref[s, part, d, q].astype(F32) for part in range(2))
                for part, value in ((0, cr * hr - ci * hi), (1, -(cr * hi + ci * hr))):
                    for side in range(2):
                        at = pl.ds((2 * q + side) * group, group)
                        lanes = pl.ds(part * states + d * half + q * 128, 128)
                        rc_ref[s, at, lanes] = jnp.where(
                            left if side == 0 else ~left, value, 0.0).astype(BF16)
    gated = []
    for s in range(2):
        full = response if s == 0 else rp_in[...].astype(F32)
        full = full + dot_t(p_row[s], rc_ref[s])
        inner = 0.7978845608028654 * (full + 0.044715 * (full * full * full))
        gated.append((0.5 * full * (1.0 + jnp.tanh(inner))).astype(BF16))
    state_out = jnp.concatenate(gated, axis=1)
    so_ref[...] = state_out
    state_copy = remote(so_ref, so_in, one["ss"], one["sr"], {"tp": sib})
    state_copy.start()
    drain(ps_v.at[pl.ds(0, 2 * (channels - part_rows))], one["vr"])
    total = dot(state_out, ps_v[:2 * channels])
    drain(pi_ref, one["pr"])
    drain(pd_ref, one["qr"])
    base = acc_ref[...] + pi_ref[0].astype(F32) + pi_ref[1].astype(F32)
    total = total + jnp.concatenate(
        [base[inner_rows:inner_rows + edge], base[:direct_rows] + pd_ref[...].astype(F32),
         base[direct_rows:inner_rows], base[inner_rows + edge:]], axis=0)
    state_copy.wait_recv()
    out_ref[...] = (total + dot(so_in[...], ps_v[2 * channels:])).astype(BF16)

    pl.when(not_last)(halo_up.wait_send)
    pl.when(not_first)(halo_down.wait_send)
    forwarded = w_all.at[pl.ds(0, (2 * last + 1) * cw * half_rows // (4 * channels)), :]
    for ref, name in (
            (x_ref, "as"), (x_ref, "bs"), (forwarded, "fs"), (gains, "gs"), (x_full.at[0, 0, lower], "ds"), (el_all.at[far], "is"),
            (e_all.at[:, far], "es"), (po_ref, "ps"), (ps_v.at[pl.ds(0, channels + 2 * part_rows)], "ws"),
            (ps_v.at[pl.ds(0, 2 * (channels - part_rows))], "vs"), (par_ref.at[0], "os"), (cq_ref.at[0], "cs"),
            (rp_out, "rs"), (so_ref, "ss")):
        drain(ref, one[name])


def per_device(
    n_sp, n_tp,
    stream, norm_gain, w_value, w_mix, w_gate, w_state, conv_taps, skip_gain, decay_rate, turn_rate,
    input_real, input_imag, read_real, read_imag, initial_state, intervals, proj_conv, proj_state,
):
    rows, width = stream.shape
    channels = w_value.shape[1]
    dirs, groups, per, group = input_real.shape
    states = dirs * groups * per
    cw = width // CHUNKS
    hbm = pl.BlockSpec(memory_space=pltpu.HBM)
    dma = lambda n: pltpu.SemaphoreType.DMA((n,))
    packed = pltpu.VMEM((rows * 8, 128), F32)
    rows_of = lambda m: jnp.swapaxes(m, 2, 3).reshape(dirs * groups * group, per)
    return pl.pallas_call(
        functools.partial(kernel, n_sp, n_tp),
        out_shape=jax.ShapeDtypeStruct((rows, width), BF16),
        in_specs=[hbm] * 18,
        out_specs=pl.BlockSpec(memory_space=pltpu.VMEM),
        scratch_shapes=[
            pltpu.VMEM((rows, width), BF16),
            pltpu.VMEM((1, width), F32),
            pltpu.VMEM(conv_taps.shape, F32),
            pltpu.VMEM((1, channels), F32),
            pltpu.VMEM((2, 4 * dirs * groups, per), F32),
            pltpu.SMEM((1, rows), F32),
            pltpu.VMEM((1, rows), F32),
            pltpu.VMEM((width * n_tp, 4 * channels), BF16),
            pltpu.VMEM((channels, width * n_tp), BF16),
            pltpu.VMEM((n_tp * channels, width), BF16),
            pltpu.VMEM((2, dirs * groups * group, per), F32),
            pltpu.VMEM((2, dirs * groups * group, per), F32),
            pltpu.VMEM((n_tp, CHUNKS, rows, cw), BF16),
            pltpu.VMEM((n_tp - 1, 1, width), F32),
            pltpu.VMEM((n_sp, 1, rows), F32),
            packed, packed, packed, packed, packed, packed, packed, packed, packed, packed,
            pltpu.VMEM((2, rows, states), F32),
            pltpu.VMEM((2, rows, states), F32),
            pltpu.VMEM((2, rows, 2 * states), BF16),
            pltpu.VMEM((2, channels, states), BF16),
            pltpu.VMEM((2, channels, states), BF16),
            pltpu.VMEM((2, channels, 2 * states), BF16),
            pltpu.VMEM((2, 2, dirs, groups // 2, group, 2 * per), BF16),
            pltpu.VMEM((rows, channels), BF16),
            pltpu.VMEM((2, 16, channels), BF16),
            pltpu.VMEM((2, 8, 128), F32),
            pltpu.VMEM((2, n_sp, 8, 128), F32),
            pltpu.VMEM((n_sp, 1, 128), F32),
            pltpu.VMEM((2, n_sp, 8, 128), F32),
            pltpu.VMEM((2, n_sp, 8, 128), F32),
            pltpu.VMEM((3, rows, width), BF16),
            pltpu.VMEM((rows, width), BF16),
            pltpu.VMEM((2, rows, width), BF16),
            pltpu.VMEM((32, width), BF16),
            pltpu.VMEM((rows, width), F32),
            pltpu.VMEM((rows, 2 * channels), BF16),
            pltpu.VMEM((rows, 2 * channels), BF16),
            pltpu.VMEM((rows, channels), BF16),
            pltpu.VMEM((rows, channels), BF16),
            pltpu.VMEM((rows, width), BF16),
            dma(12), dma(CHUNKS), dma(CHUNKS + 1), dma(n_tp - 1), dma(26), dma(2), dma(2), dma(2),
            pltpu.SemaphoreType.REGULAR((max(2, (n_sp - 1).bit_length()),)),
            pltpu.SemaphoreType.REGULAR,
        ],
        compiler_params=pltpu.CompilerParams(
            collective_id=0, has_side_effects=True, vmem_limit_bytes=48 * 1024 * 1024),
    )(*(pltpu.with_memory_space_constraint(a, pltpu.HBM) for a in (
        stream, norm_gain.reshape(1, width), w_value, w_mix, w_gate, w_state, conv_taps,
        skip_gain.reshape(1, channels),
        decay_rate.reshape(dirs * groups, per), turn_rate.reshape(dirs * groups, per),
        rows_of(input_real), rows_of(input_imag),
        read_real.reshape(dirs * groups * group, per), read_imag.reshape(dirs * groups * group, per),
        initial_state.reshape(dirs * 2 * groups, per), intervals.reshape(1, rows),
        proj_conv, proj_state,
    )))


def solution(mesh):
    return jax.shard_map(
        functools.partial(per_device, mesh.shape["sp"], mesh.shape["tp"]),
        mesh=mesh,
        in_specs=(
            P("sp", "tp"), P("tp"), P(None, "tp"), P(None, "tp"), P(None, "tp"), P(None, "tp"),
            P(None, "tp"), P("tp"), P(None, "tp", None), P(None, "tp", None),
            P(None, "tp", None, None), P(None, "tp", None, None), P(None, "tp", None, None),
            P(None, "tp", None, None), P(None, None, "tp", None), P("sp"), P("tp", None),
            P("tp", None),
        ),
        out_specs=P("sp", "tp"),
        check_vma=False,
    )
```

```python
import functools

import jax
import jax.numpy as jnp
from jax import lax
from jax.experimental import pallas as pl
from jax.experimental.pallas import tpu as pltpu
from jax.sharding import PartitionSpec as P

EPSILON = 1e-06
MESH = pl.DeviceIdType.MESH
F32 = jnp.float32
BF16 = jnp.bfloat16
CHUNKS = 4
SHARE = 4


def dot(a, b):
    return jnp.dot(a, b, preferred_element_type=F32)


def dot_t(a, b):
    return lax.dot_general(a, b, (((1,), (1,)), ((), ())), preferred_element_type=F32)


def half_turns(angle):
    theta = 0.5 * angle
    n = jnp.floor(theta * 0.6366197723675814 + 0.5)
    r = theta - n * 1.5703125
    r = r - n * 0.00048351287841796875
    r = r - n * 3.1385570764541626e-07
    r = r - n * 6.077100627776710e-11
    odd = (n - 2.0 * jnp.floor(0.5 * n)) > 0.5
    z = r * r
    s = r + r * z * ((-1.9515295891e-4 * z + 8.3321608736e-3) * z - 1.6666654611e-1)
    c = 1.0 - 0.5 * z + z * z * (
        (2.443315711809948e-5 * z - 1.388731625493765e-3) * z + 4.166664568298827e-2
    )
    square = jnp.where(odd, c * c, s * s)
    double = 2.0 * s * c
    return square, jnp.where(odd, -double, double)


def expm1_of(x, e):
    p = 1.0 + x * (1.0 / 7.0)
    for k in (6.0, 5.0, 4.0, 3.0, 2.0):
        p = 1.0 + x * p * (1.0 / k)
    return jnp.where(x > -0.35, x * p, e - 1.0)


def repeat(lo, hi, body):
    if hi - lo <= 16:
        for i in range(lo, hi):
            body(i)
    else:
        def step(i, carry):
            body(i)
            return carry
        lax.fori_loop(lo, hi, step, 0)


def fold(lo, hi, body, init):
    if hi - lo <= 16:
        for i in range(lo, hi):
            init = body(i, init)
        return init
    return lax.fori_loop(lo, hi, body, init)


def kernel(
    n_sp, n_tp,
    x_hbm, gain_hbm, wv, wm, wg, ws, taps_hbm, skip_hbm, decay_hbm, turn_hbm,
    inr, ini, rdr, rdi, init_hbm, iv_hbm, pc, ps,
    out_ref,
    x_ref, gain_ref, taps_ref, skip_ref, par_ref, iv_s, iv_v,
    w_all, pc_v, ps_v, in_v, rd_v, x_full, gains, el_all, fr_ref, fi_ref, gr_ref, gi_ref,
    dr_ref, di_ref, hr_ref, hi_ref, kr_ref, ki_ref, k_row, p_row,
    bt_ref, rt_ref, rc_ref, cq_ref, src_ref, halo_ref, e_out, e_all,
    span_ref, wa_ref, wb_ref, po_ref, p1_in, pi_ref, pd_ref, acc_ref, so_ref, so_in,
    rp_out, rp_in, xs_ref,
    load_sem, fwr_sem, br_sem, gr_sem, one_sem, hs_sem, hr_sem, p1r_sem, greet_sem, pair_sem,
):
    tp, sp = lax.axis_index("tp"), lax.axis_index("sp")
    rows, width = x_hbm.shape
    channels = wv.shape[1]
    y, core = tp // 2, tp % 2
    sib = y * 2 + 1 - core
    oth = (1 - y) * 2 + core
    diag = (1 - y) * 2 + 1 - core
    cw = width // CHUNKS

    names = ("out", "gs", "os", "is", "es", "ar", "dr", "fr", "ir", "er", "pr", "wr", "vr", "or", "rr", "sr")
    one = {name: one_sem.at[i] for i, name in enumerate(names)}
    loads = {}

    def load(name, whole, *pairs):
        sem = load_sem.at[len(loads)]
        loads[name] = whole, sem
        for src, dst in pairs:
            pltpu.make_async_copy(src, dst, sem).start()

    def remote(src, dst, send, recv, where):
        return pltpu.make_async_remote_copy(
            src_ref=src, dst_ref=dst, send_sem=send, recv_sem=recv,
            device_id=where, device_id_type=MESH)

    def drain(ref, sem):
        remote(ref, ref, sem, sem, {"tp": sib}).wait_recv()

    def drain_rows(count, sem):
        drain(w_all.at[pl.ds(0, count)], sem)

    def loaded(*names):
        for name in names:
            drain(*loads[name])

    def near(step, act):
        for s in (-step, step):
            @pl.when((sp + s >= 0) & (sp + s < n_sp))
            def _():
                act(sp + s)

    def near_count(step):
        return jnp.where(sp - step >= 0, 1, 0) + jnp.where(sp + step < n_sp, 1, 0)

    def greet(k):
        near(1 << k, lambda where: pl.semaphore_signal(
            greet_sem.at[k], inc=1, device_id={"sp": where}, device_id_type=MESH))

    def greeted(k):
        pl.semaphore_wait(greet_sem.at[k], near_count(1 << k))

    rounds = greet_sem.shape[0]
    barrier = pltpu.get_barrier_semaphore()
    for peer in (sib, oth):
        pl.semaphore_signal(barrier, inc=1, device_id={"tp": peer}, device_id_type=MESH)
    near(1, lambda where: pl.semaphore_signal(
        barrier, inc=1, device_id={"sp": where}, device_id_type=MESH))
    load("x", x_ref, (x_hbm, x_ref))
    iv_load = pltpu.make_async_copy(iv_hbm, iv_s, load_sem.at[len(loads)])
    iv_load.start()
    loads["iv"] = None
    dirs_groups = decay_hbm.shape[0]
    par_parts = (pl.ds(0, dirs_groups), pl.ds(dirs_groups, dirs_groups),
                 pl.ds(2 * dirs_groups, 2 * dirs_groups))
    par_hbm = (decay_hbm, turn_hbm, init_hbm)
    load("par", par_ref.at[0], *((src, par_ref.at[0, at]) for src, at in zip(par_hbm, par_parts)))
    load("ivv", iv_v, (iv_hbm, iv_v))
    load("gain", gain_ref, (gain_hbm, gain_ref))
    load("in", in_v, (inr, in_v.at[0]), (ini, in_v.at[1]))
    load("rd", rd_v, (rdr, rd_v.at[0]), (rdi, rd_v.at[1]))
    load("w", w_all, *((w, w_all.at[:, pl.ds(j * channels, channels)])
                       for j, w in enumerate((wv, wm, wg, ws))))
    load("taps", taps_ref, (taps_hbm, taps_ref))
    load("skip", skip_ref, (skip_hbm, skip_ref))
    load("pc", pc_v, (pc, pc_v))
    own = ps.at[:, pl.ds(pl.multiple_of(tp * width, width), width)]
    load("ps", ps_v.at[pl.ds(0, channels)], (own, ps_v.at[pl.ds(0, channels)]))
    pl.semaphore_wait(barrier, 2 + near_count(1))
    loaded("x", "gain")

    last = CHUNKS - 1
    half_rows = rows // 2
    upper, lower = pl.ds(0, half_rows), pl.ds(half_rows, half_rows)

    def block(ref, c, part=None):
        return ref.at[:, pl.ds(c * cw, cw)] if part is None else ref.at[part, pl.ds(c * cw, cw)]

    def landing(owner, c, part=None):
        return x_full.at[owner, c] if part is None else x_full.at[owner, c, part]

    spans = [(c, None) for c in range(last)] + [(last, upper), (last, lower)]
    to_oth = [
        remote(block(x_ref, *span), landing(tp, *span), one["out"], br_sem.at[i], {"tp": oth})
        for i, span in enumerate(spans)
    ]
    to_sib = remote(x_ref, xs_ref, one["out"], one["ar"], {"tp": sib})
    forward = [
        remote(landing(oth, *span), landing(oth, *span), one["out"], one["fr"] if i < last else fwr_sem, {"tp": sib})
        for i, span in enumerate(spans[:-1])
    ]
    to_diag = remote(block(x_ref, *spans[-1]), landing(tp, *spans[-1]), one["out"], one["dr"],
                     {"tp": diag})
    gain_copies = [
        remote(gain_ref, gains.at[j], one["gs"], gr_sem.at[j], {"tp": peer})
        for j, peer in enumerate((oth, sib, diag))
    ]
    gain_copies[0].start()
    for copy in to_oth:
        copy.start()
    gain_copies[1].start()
    to_sib.start()
    pl.semaphore_signal(pair_sem, inc=1, device_id={"tp": sib}, device_id_type=MESH)
    greet(0)
    part_rows = channels // SHARE
    my_part = pl.multiple_of((sp % SHARE) * part_rows, part_rows)
    mates = [sp // SHARE * SHARE + (sp + k) % SHARE for k in range(1, SHARE)]

    def columns(owner):
        return pl.ds(pl.multiple_of(owner * width, width), width)

    def slot(pos):
        return ps_v.at[pl.ds(pos * channels + my_part, part_rows)]

    weight_copies = [
        remote(src, dst, one["out"], one["wr"], {"tp": peer})
        for src, dst, peer in (
            (ps.at[pl.ds(my_part, part_rows), columns(oth)], slot(1), oth),
            (ps.at[pl.ds(my_part, part_rows), columns(diag)], slot(3), diag),
            (ps.at[:, columns(sib)], ps_v.at[pl.ds(2 * channels, channels)], sib),
        )
    ]
    weight_forward = [
        remote(slot(pos), slot(pos), one["out"], one["vr"], {"sp": mate})
        for mate in mates for pos in (1, 3)
    ]
    other_copies = [
        remote(src, par_ref.at[1, at], one["os"], one["or"], {"tp": oth})
        for src, at in zip(par_hbm, par_parts)
    ] + [remote(cq_ref.at[0], cq_ref.at[1], one["out"], one["rr"], {"tp": oth})]
    rest_copy = remote(rp_out, rp_in, one["out"], one["rr"], {"tp": oth})

    def pass_on(c):
        to_oth[c].wait_recv()
        forward[c].start()

    sub = lax.broadcasted_iota(jnp.int32, (8, 128), 0)
    top = sub < 4

    def pack(s, first):
        even = par_ref[s, pl.ds(first, 8, stride=2), :]
        odd = par_ref[s, pl.ds(first + 1, 8, stride=2), :]
        return jnp.concatenate([even, odd], axis=1)

    iv_load.wait()
    loaded("par")
    decay, turn = pack(0, 0), pack(0, dirs_groups)
    den = decay * decay + turn * turn
    td, dd = turn / den, decay / den

    def factors(k, carry):
        iv = jnp.where(top, iv_s[0, k], iv_s[0, rows - 1 - k])
        damp = -decay * iv
        square, sine = half_turns(turn * iv)
        e = jnp.exp(damp)
        cosine = 1.0 - 2.0 * square
        f_im = e * sine
        lift = expm1_of(damp, e) * cosine - 2.0 * square
        at = pl.ds(pl.multiple_of(k * 8, 8), 8)
        fr_ref[at, :] = e * cosine
        fi_ref[at, :] = f_im
        gr_ref[at, :] = td * f_im - dd * lift
        gi_ref[at, :] = -(dd * f_im + td * lift)
        return carry

    lax.fori_loop(0, 3 * rows // 4, factors, 0, unroll=4)
    greeted(0)
    if rounds > 1:
        greet(1)
    pl.semaphore_wait(pair_sem, 1)
    gain_copies[2].start()
    to_diag.start()
    for copy in other_copies[:-1]:
        copy.start()
    lax.fori_loop(3 * rows // 4, rows, factors, 0, unroll=4)

    def put(ref, k, value):
        ref[pl.ds(pl.multiple_of(k * 8, 8), 4), :] = value[:4]
        ref[pl.ds(pl.multiple_of((rows - 1 - k) * 8, 8) + 4, 4), :] = value[4:]

    def chain(k, carry):
        ar, ai, br, bi = carry
        at = pl.ds(pl.multiple_of(k * 8, 8), 8)
        back = pl.ds(pl.multiple_of((rows - 1 - k) * 8, 8), 8)
        fr, fi = fr_ref[at, :], fi_ref[at, :]
        ar, ai = fr * ar - fi * ai, fr * ai + fi * ar
        put(hr_ref, k, ar)
        put(hi_ref, k, ai)
        gr, gi = gr_ref[back, :], gi_ref[back, :]
        put(kr_ref, rows - 1 - k, gr * br - gi * bi)
        put(ki_ref, rows - 1 - k, gr * bi + gi * br)
        fr, fi = fr_ref[back, :], fi_ref[back, :]
        return ar, ai, fr * br - fi * bi, fr * bi + fi * br

    unit, zero = jnp.ones((8, 128), F32), jnp.zeros((8, 128), F32)
    lax.fori_loop(0, rows, chain, (unit, zero, unit, zero), unroll=4)
    if rounds > 1:
        greeted(1)
    for k in range(2, rounds):
        greet(k)
        if k < rounds - 1:
            greeted(k)

    for copy in weight_copies:
        copy.start()
    loaded("in", "rd")
    states = bt_ref.shape[2]
    per = rd_v.shape[2]
    half = states // 2
    group = channels * per // half
    spread = (lax.broadcasted_iota(jnp.int32, (per, half), 1) % per
              == lax.broadcasted_iota(jnp.int32, (per, half), 0)).astype(BF16)
    keep = ((lax.broadcasted_iota(jnp.int32, (channels, half), 1) // per)
            == (lax.broadcasted_iota(jnp.int32, (channels, half), 0) // group))
    left = lax.broadcasted_iota(jnp.int32, (group, 2 * per), 1) < per
    for part in range(2):
        for d in range(2):
            at, to = pl.ds(d * channels, channels), pl.ds(d * half, half)
            wide = dot(in_v[part, at, :].astype(BF16), spread)
            bt_ref[part, :, to] = jnp.where(keep, wide, 0.0).astype(BF16)
            wide = dot(rd_v[part, at, :].astype(BF16), spread)
            if part:
                wide = -wide
            rt_ref[part, :, to] = jnp.where(keep, wide, 0.0).astype(BF16)
            for q in range(channels // group // 2):
                pair = [rd_v[part, pl.ds(d * channels + g * group, group), :] for g in (2 * q, 2 * q + 1)]
                cq_ref[0, part, d, q] = jnp.concatenate(pair, axis=1).astype(BF16)
    rc_ref[...] = jnp.zeros_like(rc_ref)

    pass_on(0)
    for part, (k_ref, h_ref) in enumerate(((kr_ref, hr_ref), (ki_ref, hi_ref))):
        for j in range(8):
            lanes = slice(j * 128, (j + 1) * 128)
            k_row[part, :, lanes] = k_ref[pl.ds(j, rows, stride=8), :]
            p_row[0, :, pl.ds(part * states + j * 128, 128)] = h_ref[pl.ds(j, rows, stride=8), :].astype(BF16)
    pass_on(1)
    other_copies[-1].start()
    loaded("w")
    state_lanes = slice(3 * channels, None)
    conv_lanes = slice(0, 3 * channels)

    def scaled(value, gain):
        return (value.astype(F32) * gain).astype(BF16)

    def power(value):
        wide = value.astype(F32)
        return jnp.sum(wide * wide, axis=1, keepdims=True)

    def weight_rows(owner, first, count):
        return pl.ds(pl.multiple_of(owner * width + first, cw), count)

    def chunks_of(owner, count):
        return jnp.concatenate([x_full[owner, c] for c in range(count)], axis=1)

    def project(value, gain, owner, count):
        return dot(scaled(value, gain), w_all[weight_rows(owner, 0, count), :]), power(value)

    projected, squares = project(x_ref[...], gain_ref[...], tp, width)
    drain(xs_ref, one["ar"])
    gain_copies[1].wait_recv()
    t, s = project(xs_ref[...], gains[1], sib, width)
    projected, squares = projected + t, squares + s
    pass_on(2)
    gain_copies[0].wait_recv()
    t, s = project(chunks_of(oth, last), gains[0][:, :last * cw], oth, last * cw)
    projected, squares = projected + t, squares + s
    pass_on(3)
    if rounds > 2:
        greeted(rounds - 1)

    def interval_copy(r):
        return remote(iv_v, el_all.at[r], one["is"], one["ir"], {"sp": (sp + r) % n_sp})

    loaded("ivv")
    repeat(1, n_sp, lambda r: interval_copy(r).start())
    gain_copies[2].wait_recv()
    drain(x_full.at[0, pl.ds(0, last)], one["fr"])
    t, s = project(chunks_of(diag, last), gains[2][:, :last * cw], diag, last * cw)
    projected, squares = projected + t, squares + s
    to_oth[last + 1].wait_recv()
    tails = []
    for owner, at in ((oth, 0), (diag, 2)):
        if owner is diag:
            forward[last].wait_recv()
            to_diag.wait_recv()
        value = x_full[owner, last]
        squares = squares + power(value)
        tails.append((scaled(value, gains[at][:, last * cw:]), weight_rows(owner, last * cw, cw)))
    inv_rms = lax.rsqrt(squares / (width * n_tp) + EPSILON)

    def finish(lanes):
        total = projected[:, lanes]
        for value, at in tails:
            total = total + dot(value, w_all[at, lanes])
        return total * inv_rms

    state_input = finish(state_lanes).astype(BF16)


    def edge_copy(r, s):
        return remote(e_out.at[jnp.where(sp + r < n_sp, 0, 1)], e_all.at[s, r], one["es"], one["er"],
                      {"sp": (sp + r) % n_sp, "tp": oth if s else tp})

    def send_edges(lo, hi):
        def at(r, carry):
            edge_copy(r, 0).start()
            edge_copy(r, 1).start()
            return carry
        lax.fori_loop(lo, hi, at, 0)

    def find_edges(d):
        for i in range(2):
            lanes = slice(d * half + i * 256, d * half + (i + 1) * 256)
            dr = dot(state_input, bt_ref[0, :, lanes])
            di = dot(state_input, bt_ref[1, :, lanes])
            for h in range(2):
                tile = pl.ds(d * 4 + i * 2 + h, rows, stride=8)
                dr_ref[tile, :] = dr[:, h * 128:(h + 1) * 128]
                di_ref[tile, :] = di[:, h * 128:(h + 1) * 128]
            kr, ki = k_row[0, :, lanes], k_row[1, :, lanes]
            er = jnp.sum(kr * dr - ki * di, axis=0, keepdims=True)
            ei = jnp.sum(kr * di + ki * dr, axis=0, keepdims=True)
            for h in range(2):
                q = i * 2 + h
                e_out[d, q:q + 1, :] = er[:, h * 128:(h + 1) * 128]
                e_out[d, 4 + q:5 + q, :] = ei[:, h * 128:(h + 1) * 128]

    find_edges(1)
    send_edges(n_sp - sp, n_sp)
    convs = finish(conv_lanes)
    conv_value = convs[:, :channels].astype(BF16).astype(F32)
    conv_mix = convs[:, channels:2 * channels].astype(BF16).astype(F32)
    conv_gate = convs[:, 2 * channels:].astype(BF16).astype(F32)
    src_ref[...] = (conv_mix * conv_value).astype(BF16)
    halo_up = remote(src_ref.at[pl.ds(rows - 16, 16)], halo_ref.at[0], hs_sem.at[0], hr_sem.at[0],
                     {"sp": (sp + 1) % n_sp})
    halo_down = remote(src_ref.at[pl.ds(0, 16)], halo_ref.at[1], hs_sem.at[1], hr_sem.at[1],
                       {"sp": (sp + n_sp - 1) % n_sp})
    not_first, not_last = sp > 0, sp < n_sp - 1
    pl.when(not_last)(halo_up.start)
    pl.when(not_first)(halo_down.start)
    loaded("taps", "skip", "pc", "ps")
    edge = 16
    inner_rows = rows - 2 * edge
    direct_rows = pd_ref.shape[0]
    inner, outer = (0, inner_rows), (inner_rows, 2 * edge)
    middle = (direct_rows, inner_rows - direct_rows)
    source = src_ref[...].astype(F32)
    line = lax.broadcasted_iota(jnp.int32, (rows, channels), 0)
    previous = jnp.where(line == 0, 0.0, pltpu.roll(source, 1, 0))
    following = jnp.where(line == rows - 1, 0.0, pltpu.roll(source, rows - 1, 0))
    filtered = taps_ref[0:1, :] * previous + taps_ref[1:2, :] * source + taps_ref[2:3, :] * following
    conv_out = (conv_gate * filtered).astype(BF16)[edge:rows - edge]

    def ends(a):
        return jnp.concatenate([a[:edge], a[rows - edge:]], axis=0)

    end_gate, end_filtered = ends(conv_gate), ends(filtered)

    def offer(branch, i, span):
        at = pl.ds(*span)
        po_ref[0, at, :] = dot(branch, pc_v[:, columns(diag)]).astype(BF16)
        copy = remote(po_ref.at[0, at], p1_in.at[at], one["out"], p1r_sem.at[i], {"tp": sib})
        copy.start()
        return copy

    def crossing(branch, span):
        at = pl.ds(*span)
        kept = dot(branch, pc_v[:, columns(oth)])
        po_ref[2, at, :] = (kept + p1_in[at, :].astype(F32)).astype(BF16)
        copy = remote(po_ref.at[2, at], pi_ref.at[1, at], one["out"], one["pr"], {"tp": oth})
        copy.start()

    def rest_of(branch, span):
        at = pl.ds(*span)
        po_ref[1, at, :] = dot(branch, pc_v[:, columns(sib)]).astype(BF16)
        copy = remote(po_ref.at[1, at], pi_ref.at[0, at], one["out"], one["pr"], {"tp": sib})
        copy.start()
        acc_ref[at, :] = dot(branch, pc_v[:, columns(tp)])

    direct = pl.ds(0, direct_rows)
    direct_copies = [
        remote(po_ref.at[2, direct], pi_ref.at[1, direct], one["out"], one["pr"], {"tp": oth}),
        remote(po_ref.at[0, direct], pd_ref, one["out"], one["pr"], {"tp": diag}),
    ]
    for copy, at, owner in zip(direct_copies, (2, 0), (oth, diag)):
        po_ref[at, direct, :] = dot(conv_out[:direct_rows], pc_v[:, columns(owner)]).astype(BF16)
        copy.start()
    offered = offer(conv_out[direct_rows:], 0, middle)

    find_edges(0)

    send_edges(1, n_sp - sp)
    drain(ps_v.at[pl.ds(0, channels + 2 * part_rows)], one["wr"])
    for copy in weight_forward:
        copy.start()

    def local(k, carry):
        hr, hi = carry
        at = pl.ds(pl.multiple_of(k * 8, 8), 8)
        back = pl.ds(pl.multiple_of((rows - 1 - k) * 8, 8), 8)
        dr = jnp.where(top, dr_ref[at, :], dr_ref[back, :])
        di = jnp.where(top, di_ref[at, :], di_ref[back, :])
        gr, gi = gr_ref[at, :], gi_ref[at, :]
        fr, fi = fr_ref[at, :], fi_ref[at, :]
        pr = gr * dr - gi * di
        pi = gr * di + gi * dr
        hr, hi = fr * hr + (pr - fi * hi), fr * hi + (pi + fi * hr)
        put(hr_ref, k, hr)
        put(hi_ref, k, hi)
        return hr, hi

    lax.fori_loop(0, rows, local, (zero, zero), unroll=8)
    response = state_input.astype(F32) * skip_ref[...]
    for part, ref in ((0, hr_ref), (1, hi_ref)):
        history = jnp.concatenate(
            [ref[pl.ds(j, rows, stride=8), :].astype(BF16) for j in range(8)], axis=1)
        response = response + dot_t(history, rt_ref[part])

    rp_out[...] = response.astype(BF16)
    rest_copy.start()
    offered.wait_recv()
    crossing(conv_out[direct_rows:], middle)
    pl.when(not_first)(halo_up.wait_recv)
    pl.when(not_last)(halo_down.wait_recv)
    before = jnp.where(not_first, halo_ref[0].astype(F32)[15:16, :], 0.0) * taps_ref[0:1, :]
    after = jnp.where(not_last, halo_ref[1].astype(F32)[0:1, :], 0.0) * taps_ref[2:3, :]
    end_line = lax.broadcasted_iota(jnp.int32, (2 * edge, channels), 0)
    end_filtered = end_filtered + jnp.where(
        end_line == 0, before, jnp.where(end_line == 2 * edge - 1, after, 0.0))
    conv_ends = (end_gate * end_filtered).astype(BF16)
    offered_ends = offer(conv_ends, 1, outer)
    rest_of(conv_out, inner)

    drain(par_ref.at[1], one["or"])
    decay_2, turn_2 = pack(1, 0), pack(1, dirs_groups)
    at_t = lax.broadcasted_iota(jnp.int32, (rows, rows), 0)
    at_s = lax.broadcasted_iota(jnp.int32, (rows, rows), 1)
    steps = iv_v[...]
    reach = (jnp.sum(jnp.where(at_s <= at_t, steps, 0.0), axis=1, keepdims=True),
             jnp.sum(jnp.where(at_s >= at_t, steps, 0.0), axis=1, keepdims=True))
    def reach_factors(j):
        square, sine = half_turns(turn_2[j:j + 1, :] * reach[j // 4])
        e = jnp.exp(-decay_2[j:j + 1, :] * reach[j // 4])
        p_row[1, :, j * 128:(j + 1) * 128] = (e * (1.0 - 2.0 * square)).astype(BF16)
        p_row[1, :, states + j * 128:states + (j + 1) * 128] = (e * sine).astype(BF16)
    for j in range(4):
        reach_factors(j)
    offered_ends.wait_recv()
    crossing(conv_ends, outer)
    for j in range(4, 8):
        reach_factors(j)
    rest_of(conv_ends, outer)
    far = pl.ds(1, n_sp - 1)
    drain(el_all.at[far], one["ir"])

    def both_of(full, d):
        return jnp.concatenate([full[d * 4:d * 4 + 4], full[d * 4:d * 4 + 4]], axis=0)

    def init_of(s, d):
        starts = [2 * dirs_groups + d * 16 + part * 8 for part in range(2)]
        parts = [
            jnp.concatenate([par_ref[s, pl.ds(at, 4, stride=2), :],
                             par_ref[s, pl.ds(at + 1, 4, stride=2), :]], axis=1)
            for at in starts
        ]
        return jnp.concatenate(parts, axis=0)

    decays = [[both_of(full, d) for d in range(2)] for full in (decay, decay_2)]
    turns = [[both_of(full, d) for d in range(2)] for full in (turn, turn_2)]

    def weight(damping, turning, span):
        square, sine = half_turns(turning * span)
        e = jnp.exp(-damping * span)
        return e * (1.0 - 2.0 * square), jnp.where(top, -e * sine, e * sine)

    def apply(w, tile):
        return w[0] * tile + w[1] * pltpu.roll(tile, 4, 0)

    def elapsed(r):
        return jnp.sum(el_all[r], axis=1, keepdims=True)

    none = jnp.zeros((1, 1), F32)

    def ahead(r, carry):
        total, inside = carry
        span_ref[r] = jnp.broadcast_to(total, (1, 128))
        step = elapsed(r)
        return total + step, inside + step * jnp.where(sp - r >= 0, 1.0, 0.0)

    total, inside = fold(1, n_sp, ahead, (none, none))

    def behind(i, total):
        r = n_sp - i
        mine = sp - r >= 0
        span = jnp.where(mine, span_ref[r], jnp.broadcast_to(total, (1, 128)))
        for s in range(2):
            w = weight(jnp.where(mine, *decays[s]), jnp.where(mine, *turns[s]), span)
            wa_ref[s, r] = w[0]
            wb_ref[s, r] = w[1]
        return total + elapsed(r)

    fold(1, n_sp, behind, none)
    outside = none

    def beyond(r, acc):
        return acc + elapsed(r) * jnp.where(sp - r >= 0, 0.0, 1.0)

    outside = fold(1, n_sp, beyond, none)
    from_start = [
        tuple(apply(weight(decays[s][d], turns[s][d], (inside, outside)[d]), init_of(s, d))
              for d in range(2))
        for s in range(2)
    ]

    drain_rows((rows * channels + cq_ref.size // 2) // width, one["rr"])
    drain(e_all.at[:, far], one["er"])
    for s in range(2):
        def combine(r, carry):
            h0, h1 = carry
            moved = apply((wa_ref[s, r], wb_ref[s, r]), e_all[s, r])
            mine = sp - r >= 0
            return h0 + jnp.where(mine, moved, 0.0), h1 + jnp.where(mine, 0.0, moved)

        entering = fold(1, n_sp, combine, from_start[s])
        for d in range(2):
            for q in range(channels // group // 2):
                hr, hi = entering[d][q:q + 1, :], entering[d][4 + q:5 + q, :]
                cr, ci = (cq_ref[s, part, d, q].astype(F32) for part in range(2))
                for part, value in ((0, cr * hr - ci * hi), (1, -(cr * hi + ci * hr))):
                    for side in range(2):
                        at = pl.ds((2 * q + side) * group, group)
                        lanes = pl.ds(part * states + d * half + q * 128, 128)
                        rc_ref[s, at, lanes] = jnp.where(
                            left if side == 0 else ~left, value, 0.0).astype(BF16)
    gated = []
    for s in range(2):
        full = response if s == 0 else rp_in[...].astype(F32)
        full = full + dot_t(p_row[s], rc_ref[s])
        inner = 0.7978845608028654 * (full + 0.044715 * (full * full * full))
        gated.append((0.5 * full * (1.0 + jnp.tanh(inner))).astype(BF16))
    state_out = jnp.concatenate(gated, axis=1)
    so_ref[...] = state_out
    state_copy = remote(so_ref, so_in, one["out"], one["sr"], {"tp": sib})
    state_copy.start()
    drain(ps_v.at[pl.ds(0, 2 * (channels - part_rows))], one["vr"])
    total = dot(state_out, ps_v[:2 * channels])
    drain_rows(2 * rows + direct_rows, one["pr"])
    base = acc_ref[...] + pi_ref[0].astype(F32) + pi_ref[1].astype(F32)
    total = total + jnp.concatenate(
        [base[inner_rows:inner_rows + edge], base[:direct_rows] + pd_ref[...].astype(F32),
         base[direct_rows:inner_rows], base[inner_rows + edge:]], axis=0)
    state_copy.wait_recv()
    out_ref[...] = (total + dot(so_in[...], ps_v[2 * channels:])).astype(BF16)

    pl.when(not_last)(halo_up.wait_send)
    pl.when(not_first)(halo_down.wait_send)
    sent = [(x_ref, 2), (x_full.at[0, pl.ds(0, last)], 1), (x_full.at[0, 0], 1), (po_ref, 1),
            (ps_v.at[pl.ds(0, channels + 2 * part_rows)], 1),
            (ps_v.at[pl.ds(0, 2 * (channels - part_rows))], 1), (cq_ref.at[0], 1), (rp_out, 1),
            (so_ref, 1)]
    count = sum(times * ref.size for ref, times in sent) // width
    drain_rows(count, one["out"])
    drain(par_ref.at[0], one["os"])
    drain(gains, one["gs"])
    drain(el_all.at[far], one["is"])
    drain(e_all.at[:, far], one["es"])


def per_device(
    n_sp, n_tp,
    stream, norm_gain, w_value, w_mix, w_gate, w_state, conv_taps, skip_gain, decay_rate, turn_rate,
    input_real, input_imag, read_real, read_imag, initial_state, intervals, proj_conv, proj_state,
):
    rows, width = stream.shape
    channels = w_value.shape[1]
    dirs, groups, per, group = input_real.shape
    states = dirs * groups * per
    cw = width // CHUNKS
    hbm = pl.BlockSpec(memory_space=pltpu.HBM)
    dma = lambda n: pltpu.SemaphoreType.DMA((n,))
    packed = pltpu.VMEM((rows * 8, 128), F32)
    rows_of = lambda m: jnp.swapaxes(m, 2, 3).reshape(dirs * groups * group, per)
    return pl.pallas_call(
        functools.partial(kernel, n_sp, n_tp),
        out_shape=jax.ShapeDtypeStruct((rows, width), BF16),
        in_specs=[hbm] * 18,
        out_specs=pl.BlockSpec(memory_space=pltpu.VMEM),
        scratch_shapes=[
            pltpu.VMEM((rows, width), BF16),
            pltpu.VMEM((1, width), F32),
            pltpu.VMEM(conv_taps.shape, F32),
            pltpu.VMEM((1, channels), F32),
            pltpu.VMEM((2, 4 * dirs * groups, per), F32),
            pltpu.SMEM((1, rows), F32),
            pltpu.VMEM((1, rows), F32),
            pltpu.VMEM((width * n_tp, 4 * channels), BF16),
            pltpu.VMEM((channels, width * n_tp), BF16),
            pltpu.VMEM((n_tp * channels, width), BF16),
            pltpu.VMEM((2, dirs * groups * group, per), F32),
            pltpu.VMEM((2, dirs * groups * group, per), F32),
            pltpu.VMEM((n_tp, CHUNKS, rows, cw), BF16),
            pltpu.VMEM((n_tp - 1, 1, width), F32),
            pltpu.VMEM((n_sp, 1, rows), F32),
            packed, packed, packed, packed, packed, packed, packed, packed, packed, packed,
            pltpu.VMEM((2, rows, states), F32),
            pltpu.VMEM((2, rows, 2 * states), BF16),
            pltpu.VMEM((2, channels, states), BF16),
            pltpu.VMEM((2, channels, states), BF16),
            pltpu.VMEM((2, channels, 2 * states), BF16),
            pltpu.VMEM((2, 2, dirs, groups // 2, group, 2 * per), BF16),
            pltpu.VMEM((rows, channels), BF16),
            pltpu.VMEM((2, 16, channels), BF16),
            pltpu.VMEM((2, 8, 128), F32),
            pltpu.VMEM((2, n_sp, 8, 128), F32),
            pltpu.VMEM((n_sp, 1, 128), F32),
            pltpu.VMEM((2, n_sp, 8, 128), F32),
            pltpu.VMEM((2, n_sp, 8, 128), F32),
            pltpu.VMEM((3, rows, width), BF16),
            pltpu.VMEM((rows, width), BF16),
            pltpu.VMEM((2, rows, width), BF16),
            pltpu.VMEM((32, width), BF16),
            pltpu.VMEM((rows, width), F32),
            pltpu.VMEM((rows, 2 * channels), BF16),
            pltpu.VMEM((rows, 2 * channels), BF16),
            pltpu.VMEM((rows, channels), BF16),
            pltpu.VMEM((rows, channels), BF16),
            pltpu.VMEM((rows, width), BF16),
            dma(12), pltpu.SemaphoreType.DMA, dma(CHUNKS + 1), dma(n_tp - 1), dma(16), dma(2), dma(2), dma(2),
            pltpu.SemaphoreType.REGULAR((max(2, (n_sp - 1).bit_length()),)),
            pltpu.SemaphoreType.REGULAR,
        ],
        compiler_params=pltpu.CompilerParams(
            collective_id=0, has_side_effects=True, vmem_limit_bytes=48 * 1024 * 1024),
    )(*(pltpu.with_memory_space_constraint(a, pltpu.HBM) for a in (
        stream, norm_gain.reshape(1, width), w_value, w_mix, w_gate, w_state, conv_taps,
        skip_gain.reshape(1, channels),
        decay_rate.reshape(dirs * groups, per), turn_rate.reshape(dirs * groups, per),
        rows_of(input_real), rows_of(input_imag),
        read_real.reshape(dirs * groups * group, per), read_imag.reshape(dirs * groups * group, per),
        initial_state.reshape(dirs * 2 * groups, per), intervals.reshape(1, rows),
        proj_conv, proj_state,
    )))


def solution(mesh):
    return jax.shard_map(
        functools.partial(per_device, mesh.shape["sp"], mesh.shape["tp"]),
        mesh=mesh,
        in_specs=(
            P("sp", "tp"), P("tp"), P(None, "tp"), P(None, "tp"), P(None, "tp"), P(None, "tp"),
            P(None, "tp"), P("tp"), P(None, "tp", None), P(None, "tp", None),
            P(None, "tp", None, None), P(None, "tp", None, None), P(None, "tp", None, None),
            P(None, "tp", None, None), P(None, None, "tp", None), P("sp"), P("tp", None),
            P("tp", None),
        ),
        out_specs=P("sp", "tp"),
        check_vma=False,
    )
```

```python
import functools

import jax
import jax.numpy as jnp
from jax import lax
from jax.experimental import pallas as pl
from jax.experimental.pallas import tpu as pltpu
from jax.sharding import PartitionSpec as P

EPSILON = 1e-06
MESH = pl.DeviceIdType.MESH
F32 = jnp.float32
BF16 = jnp.bfloat16
CHUNKS = 4
SHARE = 4


def dot(a, b):
    return jnp.dot(a, b, preferred_element_type=F32)


def dot_t(a, b):
    return lax.dot_general(a, b, (((1,), (1,)), ((), ())), preferred_element_type=F32)


def half_turns(angle):
    theta = 0.5 * angle
    n = jnp.floor(theta * 0.6366197723675814 + 0.5)
    r = theta - n * 1.5703125
    r = r - n * 0.00048351287841796875
    r = r - n * 3.1385570764541626e-07
    r = r - n * 6.077100627776710e-11
    odd = (n - 2.0 * jnp.floor(0.5 * n)) > 0.5
    z = r * r
    s = r + r * z * ((-1.9515295891e-4 * z + 8.3321608736e-3) * z - 1.6666654611e-1)
    c = 1.0 - 0.5 * z + z * z * (
        (2.443315711809948e-5 * z - 1.388731625493765e-3) * z + 4.166664568298827e-2
    )
    square = jnp.where(odd, c * c, s * s)
    double = 2.0 * s * c
    return square, jnp.where(odd, -double, double)


def expm1_of(x, e):
    p = 1.0 + x * (1.0 / 7.0)
    for k in (6.0, 5.0, 4.0, 3.0, 2.0):
        p = 1.0 + x * p * (1.0 / k)
    return jnp.where(x > -0.35, x * p, e - 1.0)


def repeat(lo, hi, body):
    if hi - lo <= 16:
        for i in range(lo, hi):
            body(i)
    else:
        def step(i, carry):
            body(i)
            return carry
        lax.fori_loop(lo, hi, step, 0)


def fold(lo, hi, body, init):
    if hi - lo <= 16:
        for i in range(lo, hi):
            init = body(i, init)
        return init
    return lax.fori_loop(lo, hi, body, init)


def kernel(
    n_sp, n_tp,
    x_hbm, gain_hbm, wv, wm, wg, ws, taps_hbm, skip_hbm, decay_hbm, turn_hbm,
    inr, ini, rdr, rdi, init_hbm, iv_hbm, pc, ps,
    out_ref,
    x_ref, gain_ref, taps_ref, skip_ref, par_ref, iv_s, iv_v,
    w_all, pc_v, ps_v, in_v, rd_v, x_full, gains, el_all, fr_ref, fi_ref, gr_ref, gi_ref,
    dr_ref, di_ref, hr_ref, hi_ref, kr_ref, ki_ref, k_row, p_row,
    bt_ref, rt_ref, rc_ref, cq_ref, src_ref, halo_ref, e_f32, e_out, e_all,
    span_ref, wa_ref, wb_ref, po_ref, p1_in, pi_ref, pd_ref, acc_ref, so_ref, so_in,
    rp_out, rp_in, xs_ref,
    load_sem, fwr_sem, br_sem, gr_sem, one_sem, hs_sem, hr_sem, p1r_sem, greet_sem, pair_sem,
):
    tp, sp = lax.axis_index("tp"), lax.axis_index("sp")
    rows, width = x_hbm.shape
    channels = wv.shape[1]
    y, core = tp // 2, tp % 2
    sib = y * 2 + 1 - core
    oth = (1 - y) * 2 + core
    diag = (1 - y) * 2 + 1 - core
    cw = width // CHUNKS

    names = ("out", "gs", "os", "is", "es", "ar", "dr", "fr", "ir", "er", "pr", "wr", "vr", "or", "rr", "sr")
    one = {name: one_sem.at[i] for i, name in enumerate(names)}
    loads = {}

    def load(name, whole, *pairs):
        sem = load_sem.at[len(loads)]
        loads[name] = whole, sem
        for src, dst in pairs:
            pltpu.make_async_copy(src, dst, sem).start()

    def remote(src, dst, send, recv, where):
        return pltpu.make_async_remote_copy(
            src_ref=src, dst_ref=dst, send_sem=send, recv_sem=recv,
            device_id=where, device_id_type=MESH)

    def drain(ref, sem):
        remote(ref, ref, sem, sem, {"tp": sib}).wait_recv()

    def drain_rows(count, sem):
        drain(w_all.at[pl.ds(0, count)], sem)

    def loaded(*names):
        for name in names:
            drain(*loads[name])

    def near(step, act):
        for s in (-step, step):
            @pl.when((sp + s >= 0) & (sp + s < n_sp))
            def _():
                act(sp + s)

    def near_count(step):
        return jnp.where(sp - step >= 0, 1, 0) + jnp.where(sp + step < n_sp, 1, 0)

    def greet(k):
        near(1 << k, lambda where: pl.semaphore_signal(
            greet_sem.at[k], inc=1, device_id={"sp": where}, device_id_type=MESH))

    def greeted(k):
        pl.semaphore_wait(greet_sem.at[k], near_count(1 << k))

    rounds = greet_sem.shape[0]
    load("x", x_ref, (x_hbm, x_ref))
    barrier = pltpu.get_barrier_semaphore()
    for peer in (sib, oth):
        pl.semaphore_signal(barrier, inc=1, device_id={"tp": peer}, device_id_type=MESH)
    near(1, lambda where: pl.semaphore_signal(
        barrier, inc=1, device_id={"sp": where}, device_id_type=MESH))
    iv_load = pltpu.make_async_copy(iv_hbm, iv_s, load_sem.at[len(loads)])
    iv_load.start()
    loads["iv"] = None
    dirs_groups = decay_hbm.shape[0]
    par_parts = (pl.ds(0, dirs_groups), pl.ds(dirs_groups, dirs_groups),
                 pl.ds(2 * dirs_groups, 2 * dirs_groups))
    par_hbm = (decay_hbm, turn_hbm, init_hbm)
    load("par", par_ref.at[0], *((src, par_ref.at[0, at]) for src, at in zip(par_hbm, par_parts)))
    load("ivv", iv_v, (iv_hbm, iv_v))
    load("gain", gain_ref, (gain_hbm, gain_ref))
    load("in", in_v, (inr, in_v.at[0]), (ini, in_v.at[1]))
    load("rd", rd_v, (rdr, rd_v.at[0]), (rdi, rd_v.at[1]))
    load("w", w_all, *((w, w_all.at[:, pl.ds(j * channels, channels)])
                       for j, w in enumerate((wv, wm, wg, ws))))
    load("taps", taps_ref, (taps_hbm, taps_ref))
    load("skip", skip_ref, (skip_hbm, skip_ref))
    load("pc", pc_v, (pc, pc_v))
    own = ps.at[:, pl.ds(pl.multiple_of(tp * width, width), width)]
    load("ps", ps_v.at[pl.ds(0, channels)], (own, ps_v.at[pl.ds(0, channels)]))
    pl.semaphore_wait(barrier, 2 + near_count(1))
    loaded("x", "gain")

    last = CHUNKS - 1
    half_rows = rows // 2
    upper, lower = pl.ds(0, half_rows), pl.ds(half_rows, half_rows)

    def block(ref, c, part=None):
        return ref.at[:, pl.ds(c * cw, cw)] if part is None else ref.at[part, pl.ds(c * cw, cw)]

    def landing(owner, c, part=None):
        return x_full.at[owner, c] if part is None else x_full.at[owner, c, part]

    spans = [(c, None) for c in range(last)] + [(last, upper), (last, lower)]
    to_oth = [
        remote(block(x_ref, *span), landing(tp, *span), one["out"], br_sem.at[i], {"tp": oth})
        for i, span in enumerate(spans)
    ]
    to_sib = remote(x_ref, xs_ref, one["out"], one["ar"], {"tp": sib})
    forward = [
        remote(landing(oth, *span), landing(oth, *span), one["out"], one["fr"] if i < last else fwr_sem, {"tp": sib})
        for i, span in enumerate(spans[:-1])
    ]
    to_diag = remote(block(x_ref, *spans[-1]), landing(tp, *spans[-1]), one["out"], one["dr"],
                     {"tp": diag})
    gain_copies = [
        remote(gain_ref, gains.at[j], one["gs"], gr_sem.at[j], {"tp": peer})
        for j, peer in enumerate((oth, sib, diag))
    ]
    gain_copies[0].start()
    for copy in to_oth:
        copy.start()
    gain_copies[1].start()
    to_sib.start()
    pl.semaphore_signal(pair_sem, inc=1, device_id={"tp": sib}, device_id_type=MESH)
    greet(0)
    part_rows = channels // SHARE
    my_part = pl.multiple_of((sp % SHARE) * part_rows, part_rows)
    mates = [sp // SHARE * SHARE + (sp + k) % SHARE for k in range(1, SHARE)]

    def columns(owner):
        return pl.ds(pl.multiple_of(owner * width, width), width)

    def slot(pos):
        return ps_v.at[pl.ds(pos * channels + my_part, part_rows)]

    weight_copies = [
        remote(src, dst, one["out"], one["wr"], {"tp": peer})
        for src, dst, peer in (
            (ps.at[pl.ds(my_part, part_rows), columns(oth)], slot(1), oth),
            (ps.at[pl.ds(my_part, part_rows), columns(diag)], slot(3), diag),
            (ps.at[:, columns(sib)], ps_v.at[pl.ds(2 * channels, channels)], sib),
        )
    ]
    weight_forward = [
        remote(slot(pos), slot(pos), one["out"], one["vr"], {"sp": mate})
        for mate in mates for pos in (1, 3)
    ]
    other_copies = [
        remote(src, par_ref.at[1, at], one["os"], one["or"], {"tp": oth})
        for src, at in zip(par_hbm, par_parts)
    ] + [remote(cq_ref.at[0], cq_ref.at[1], one["out"], one["rr"], {"tp": oth})]
    rest_copy = remote(rp_out, rp_in, one["out"], one["rr"], {"tp": oth})

    def pass_on(c):
        to_oth[c].wait_recv()
        forward[c].start()

    sub = lax.broadcasted_iota(jnp.int32, (8, 128), 0)
    top = sub < 4

    def pack(s, first):
        even = par_ref[s, pl.ds(first, 8, stride=2), :]
        odd = par_ref[s, pl.ds(first + 1, 8, stride=2), :]
        return jnp.concatenate([even, odd], axis=1)

    iv_load.wait()
    loaded("par")
    decay, turn = pack(0, 0), pack(0, dirs_groups)
    den = decay * decay + turn * turn
    td, dd = turn / den, decay / den

    def factors(k, carry):
        iv = jnp.where(top, iv_s[0, k], iv_s[0, rows - 1 - k])
        damp = -decay * iv
        square, sine = half_turns(turn * iv)
        e = jnp.exp(damp)
        cosine = 1.0 - 2.0 * square
        f_im = e * sine
        lift = expm1_of(damp, e) * cosine - 2.0 * square
        at = pl.ds(pl.multiple_of(k * 8, 8), 8)
        fr_ref[at, :] = e * cosine
        fi_ref[at, :] = f_im
        gr_ref[at, :] = td * f_im - dd * lift
        gi_ref[at, :] = -(dd * f_im + td * lift)
        return carry

    lax.fori_loop(0, 3 * rows // 4, factors, 0, unroll=4)
    greeted(0)
    if rounds > 1:
        greet(1)
    pl.semaphore_wait(pair_sem, 1)
    gain_copies[2].start()
    to_diag.start()
    for copy in other_copies[:-1]:
        copy.start()
    lax.fori_loop(3 * rows // 4, rows, factors, 0, unroll=4)

    def put(ref, k, value):
        ref[pl.ds(pl.multiple_of(k * 8, 8), 4), :] = value[:4]
        ref[pl.ds(pl.multiple_of((rows - 1 - k) * 8, 8) + 4, 4), :] = value[4:]

    def chain(k, carry):
        ar, ai, br, bi = carry
        at = pl.ds(pl.multiple_of(k * 8, 8), 8)
        back = pl.ds(pl.multiple_of((rows - 1 - k) * 8, 8), 8)
        fr, fi = fr_ref[at, :], fi_ref[at, :]
        ar, ai = fr * ar - fi * ai, fr * ai + fi * ar
        put(hr_ref, k, ar)
        put(hi_ref, k, ai)
        gr, gi = gr_ref[back, :], gi_ref[back, :]
        put(kr_ref, rows - 1 - k, gr * br - gi * bi)
        put(ki_ref, rows - 1 - k, gr * bi + gi * br)
        fr, fi = fr_ref[back, :], fi_ref[back, :]
        return ar, ai, fr * br - fi * bi, fr * bi + fi * br

    unit, zero = jnp.ones((8, 128), F32), jnp.zeros((8, 128), F32)
    lax.fori_loop(0, rows, chain, (unit, zero, unit, zero), unroll=4)
    if rounds > 1:
        greeted(1)
    for k in range(2, rounds):
        greet(k)
        if k < rounds - 1:
            greeted(k)

    for copy in weight_copies:
        copy.start()
    loaded("in", "rd")
    states = bt_ref.shape[2]
    per = rd_v.shape[2]
    half = states // 2
    group = channels * per // half
    spread = (lax.broadcasted_iota(jnp.int32, (per, half), 1) % per
              == lax.broadcasted_iota(jnp.int32, (per, half), 0)).astype(BF16)
    keep = ((lax.broadcasted_iota(jnp.int32, (channels, half), 1) // per)
            == (lax.broadcasted_iota(jnp.int32, (channels, half), 0) // group))
    left = lax.broadcasted_iota(jnp.int32, (group, 2 * per), 1) < per
    for part in range(2):
        for d in range(2):
            at, to = pl.ds(d * channels, channels), pl.ds(d * half, half)
            wide = dot(in_v[part, at, :].astype(BF16), spread)
            bt_ref[part, :, to] = jnp.where(keep, wide, 0.0).astype(BF16)
            wide = dot(rd_v[part, at, :].astype(BF16), spread)
            if part:
                wide = -wide
            rt_ref[part, :, to] = jnp.where(keep, wide, 0.0).astype(BF16)
            for q in range(channels // group // 2):
                pair = [rd_v[part, pl.ds(d * channels + g * group, group), :] for g in (2 * q, 2 * q + 1)]
                cq_ref[0, part, d, q] = jnp.concatenate(pair, axis=1).astype(BF16)
    rc_ref[...] = jnp.zeros_like(rc_ref)

    pass_on(0)
    for part, (k_ref, h_ref) in enumerate(((kr_ref, hr_ref), (ki_ref, hi_ref))):
        for j in range(8):
            lanes = slice(j * 128, (j + 1) * 128)
            k_row[part, :, lanes] = k_ref[pl.ds(j, rows, stride=8), :]
            p_row[0, :, pl.ds(part * states + j * 128, 128)] = h_ref[pl.ds(j, rows, stride=8), :].astype(BF16)
    pass_on(1)
    other_copies[-1].start()
    loaded("w")
    state_lanes = slice(3 * channels, None)
    conv_lanes = slice(0, 3 * channels)

    def scaled(value, gain):
        return (value.astype(F32) * gain).astype(BF16)

    def power(value):
        wide = value.astype(F32)
        return jnp.sum(wide * wide, axis=1, keepdims=True)

    def weight_rows(owner, first, count):
        return pl.ds(pl.multiple_of(owner * width + first, cw), count)

    def chunks_of(owner, count):
        return jnp.concatenate([x_full[owner, c] for c in range(count)], axis=1)

    def project(value, gain, owner, count):
        return dot(scaled(value, gain), w_all[weight_rows(owner, 0, count), :]), power(value)

    projected, squares = project(x_ref[...], gain_ref[...], tp, width)
    drain(xs_ref, one["ar"])
    gain_copies[1].wait_recv()
    t, s = project(xs_ref[...], gains[1], sib, width)
    projected, squares = projected + t, squares + s
    pass_on(2)
    gain_copies[0].wait_recv()
    t, s = project(chunks_of(oth, last), gains[0][:, :last * cw], oth, last * cw)
    projected, squares = projected + t, squares + s
    pass_on(3)
    if rounds > 2:
        greeted(rounds - 1)

    def interval_copy(r):
        return remote(iv_v, el_all.at[r], one["is"], one["ir"], {"sp": (sp + r) % n_sp})

    loaded("ivv")
    repeat(1, n_sp, lambda r: interval_copy(r).start())
    gain_copies[2].wait_recv()
    drain(x_full.at[0, pl.ds(0, last)], one["fr"])
    t, s = project(chunks_of(diag, last), gains[2][:, :last * cw], diag, last * cw)
    projected, squares = projected + t, squares + s
    to_oth[last + 1].wait_recv()
    tails = []
    for owner, at in ((oth, 0), (diag, 2)):
        if owner is diag:
            forward[last].wait_recv()
            to_diag.wait_recv()
        value = x_full[owner, last]
        squares = squares + power(value)
        tails.append((scaled(value, gains[at][:, last * cw:]), weight_rows(owner, last * cw, cw)))
    inv_rms = lax.rsqrt(squares / (width * n_tp) + EPSILON)

    def finish(lanes):
        total = projected[:, lanes]
        for value, at in tails:
            total = total + dot(value, w_all[at, lanes])
        return total * inv_rms

    state_input = finish(state_lanes).astype(BF16)


    def edge_copy(r, s):
        return remote(e_out.at[jnp.where(sp + r < n_sp, 0, 1)], e_all.at[s, r], one["es"], one["er"],
                      {"sp": (sp + r) % n_sp, "tp": oth if s else tp})

    def send_edges(lo, hi):
        def at(r, carry):
            edge_copy(r, 0).start()
            edge_copy(r, 1).start()
            return carry
        lax.fori_loop(lo, hi, at, 0)

    def find_edges(d):
        for i in range(2):
            lanes = slice(d * half + i * 256, d * half + (i + 1) * 256)
            dr = dot(state_input, bt_ref[0, :, lanes])
            di = dot(state_input, bt_ref[1, :, lanes])
            for h in range(2):
                tile = pl.ds(d * 4 + i * 2 + h, rows, stride=8)
                dr_ref[tile, :] = dr[:, h * 128:(h + 1) * 128]
                di_ref[tile, :] = di[:, h * 128:(h + 1) * 128]
            kr, ki = k_row[0, :, lanes], k_row[1, :, lanes]
            er = jnp.sum(kr * dr - ki * di, axis=0, keepdims=True)
            ei = jnp.sum(kr * di + ki * dr, axis=0, keepdims=True)
            for h in range(2):
                q = i * 2 + h
                e_f32[d, q:q + 1, :] = er[:, h * 128:(h + 1) * 128]
                e_f32[d, 4 + q:5 + q, :] = ei[:, h * 128:(h + 1) * 128]
        e_out[d] = e_f32[d].astype(BF16)

    find_edges(1)
    send_edges(n_sp - sp, n_sp)
    convs = finish(conv_lanes)
    conv_value = convs[:, :channels].astype(BF16).astype(F32)
    conv_mix = convs[:, channels:2 * channels].astype(BF16).astype(F32)
    conv_gate = convs[:, 2 * channels:].astype(BF16).astype(F32)
    src_ref[...] = (conv_mix * conv_value).astype(BF16)
    halo_up = remote(src_ref.at[pl.ds(rows - 16, 16)], halo_ref.at[0], hs_sem.at[0], hr_sem.at[0],
                     {"sp": (sp + 1) % n_sp})
    halo_down = remote(src_ref.at[pl.ds(0, 16)], halo_ref.at[1], hs_sem.at[1], hr_sem.at[1],
                       {"sp": (sp + n_sp - 1) % n_sp})
    not_first, not_last = sp > 0, sp < n_sp - 1
    pl.when(not_last)(halo_up.start)
    pl.when(not_first)(halo_down.start)
    loaded("taps", "skip", "pc", "ps")
    edge = 16
    inner_rows = rows - 2 * edge
    direct_rows = pd_ref.shape[0]
    inner, outer = (0, inner_rows), (inner_rows, 2 * edge)
    middle = (direct_rows, inner_rows - direct_rows)
    source = src_ref[...].astype(F32)
    line = lax.broadcasted_iota(jnp.int32, (rows, channels), 0)
    previous = jnp.where(line == 0, 0.0, pltpu.roll(source, 1, 0))
    following = jnp.where(line == rows - 1, 0.0, pltpu.roll(source, rows - 1, 0))
    filtered = taps_ref[0:1, :] * previous + taps_ref[1:2, :] * source + taps_ref[2:3, :] * following
    conv_out = (conv_gate * filtered).astype(BF16)[edge:rows - edge]

    def ends(a):
        return jnp.concatenate([a[:edge], a[rows - edge:]], axis=0)

    end_gate, end_filtered = ends(conv_gate), ends(filtered)

    def offer(branch, i, span):
        at = pl.ds(*span)
        po_ref[0, at, :] = dot(branch, pc_v[:, columns(diag)]).astype(BF16)
        copy = remote(po_ref.at[0, at], p1_in.at[at], one["out"], p1r_sem.at[i], {"tp": sib})
        copy.start()
        return copy

    def crossing(branch, span):
        at = pl.ds(*span)
        kept = dot(branch, pc_v[:, columns(oth)])
        po_ref[2, at, :] = (kept + p1_in[at, :].astype(F32)).astype(BF16)
        copy = remote(po_ref.at[2, at], pi_ref.at[1, at], one["out"], one["pr"], {"tp": oth})
        copy.start()

    def rest_of(branch, span):
        at = pl.ds(*span)
        po_ref[1, at, :] = dot(branch, pc_v[:, columns(sib)]).astype(BF16)
        copy = remote(po_ref.at[1, at], pi_ref.at[0, at], one["out"], one["pr"], {"tp": sib})
        copy.start()
        acc_ref[at, :] = dot(branch, pc_v[:, columns(tp)])

    direct = pl.ds(0, direct_rows)
    direct_copies = [
        remote(po_ref.at[2, direct], pi_ref.at[1, direct], one["out"], one["pr"], {"tp": oth}),
        remote(po_ref.at[0, direct], pd_ref, one["out"], one["pr"], {"tp": diag}),
    ]
    for copy, at, owner in zip(direct_copies, (2, 0), (oth, diag)):
        po_ref[at, direct, :] = dot(conv_out[:direct_rows], pc_v[:, columns(owner)]).astype(BF16)
        copy.start()
    offered = offer(conv_out[direct_rows:], 0, middle)

    find_edges(0)

    send_edges(1, n_sp - sp)
    drain(ps_v.at[pl.ds(0, channels + 2 * part_rows)], one["wr"])
    for copy in weight_forward:
        copy.start()

    def local(k, carry):
        hr, hi = carry
        at = pl.ds(pl.multiple_of(k * 8, 8), 8)
        back = pl.ds(pl.multiple_of((rows - 1 - k) * 8, 8), 8)
        dr = jnp.where(top, dr_ref[at, :], dr_ref[back, :])
        di = jnp.where(top, di_ref[at, :], di_ref[back, :])
        gr, gi = gr_ref[at, :], gi_ref[at, :]
        fr, fi = fr_ref[at, :], fi_ref[at, :]
        pr = gr * dr - gi * di
        pi = gr * di + gi * dr
        hr, hi = fr * hr + (pr - fi * hi), fr * hi + (pi + fi * hr)
        put(hr_ref, k, hr)
        put(hi_ref, k, hi)
        return hr, hi

    lax.fori_loop(0, rows, local, (zero, zero), unroll=8)
    response = state_input.astype(F32) * skip_ref[...]
    for part, ref in ((0, hr_ref), (1, hi_ref)):
        history = jnp.concatenate(
            [ref[pl.ds(j, rows, stride=8), :].astype(BF16) for j in range(8)], axis=1)
        response = response + dot_t(history, rt_ref[part])

    rp_out[...] = response.astype(BF16)
    rest_copy.start()
    offered.wait_recv()
    crossing(conv_out[direct_rows:], middle)
    pl.when(not_first)(halo_up.wait_recv)
    pl.when(not_last)(halo_down.wait_recv)
    before = jnp.where(not_first, halo_ref[0].astype(F32)[15:16, :], 0.0) * taps_ref[0:1, :]
    after = jnp.where(not_last, halo_ref[1].astype(F32)[0:1, :], 0.0) * taps_ref[2:3, :]
    end_line = lax.broadcasted_iota(jnp.int32, (2 * edge, channels), 0)
    end_filtered = end_filtered + jnp.where(
        end_line == 0, before, jnp.where(end_line == 2 * edge - 1, after, 0.0))
    conv_ends = (end_gate * end_filtered).astype(BF16)
    offered_ends = offer(conv_ends, 1, outer)
    rest_of(conv_out, inner)

    drain(par_ref.at[1], one["or"])
    decay_2, turn_2 = pack(1, 0), pack(1, dirs_groups)
    at_t = lax.broadcasted_iota(jnp.int32, (rows, rows), 0)
    at_s = lax.broadcasted_iota(jnp.int32, (rows, rows), 1)
    steps = iv_v[...]
    reach = (jnp.sum(jnp.where(at_s <= at_t, steps, 0.0), axis=1, keepdims=True),
             jnp.sum(jnp.where(at_s >= at_t, steps, 0.0), axis=1, keepdims=True))
    def reach_factors(j):
        square, sine = half_turns(turn_2[j:j + 1, :] * reach[j // 4])
        e = jnp.exp(-decay_2[j:j + 1, :] * reach[j // 4])
        p_row[1, :, j * 128:(j + 1) * 128] = (e * (1.0 - 2.0 * square)).astype(BF16)
        p_row[1, :, states + j * 128:states + (j + 1) * 128] = (e * sine).astype(BF16)
    for j in range(4):
        reach_factors(j)
    offered_ends.wait_recv()
    crossing(conv_ends, outer)
    for j in range(4, 8):
        reach_factors(j)
    rest_of(conv_ends, outer)
    far = pl.ds(1, n_sp - 1)
    drain(el_all.at[far], one["ir"])

    def both_of(full, d):
        return jnp.concatenate([full[d * 4:d * 4 + 4], full[d * 4:d * 4 + 4]], axis=0)

    def init_of(s, d):
        starts = [2 * dirs_groups + d * 16 + part * 8 for part in range(2)]
        parts = [
            jnp.concatenate([par_ref[s, pl.ds(at, 4, stride=2), :],
                             par_ref[s, pl.ds(at + 1, 4, stride=2), :]], axis=1)
            for at in starts
        ]
        return jnp.concatenate(parts, axis=0)

    decays = [[both_of(full, d) for d in range(2)] for full in (decay, decay_2)]
    turns = [[both_of(full, d) for d in range(2)] for full in (turn, turn_2)]

    def weight(damping, turning, span):
        square, sine = half_turns(turning * span)
        e = jnp.exp(-damping * span)
        return e * (1.0 - 2.0 * square), jnp.where(top, -e * sine, e * sine)

    def apply(w, tile):
        return w[0] * tile + w[1] * pltpu.roll(tile, 4, 0)

    def elapsed(r):
        return jnp.sum(el_all[r], axis=1, keepdims=True)

    none = jnp.zeros((1, 1), F32)

    def ahead(r, carry):
        total, inside = carry
        span_ref[r] = jnp.broadcast_to(total, (1, 128))
        step = elapsed(r)
        return total + step, inside + step * jnp.where(sp - r >= 0, 1.0, 0.0)

    total, inside = fold(1, n_sp, ahead, (none, none))

    def behind(i, total):
        r = n_sp - i
        mine = sp - r >= 0
        span = jnp.where(mine, span_ref[r], jnp.broadcast_to(total, (1, 128)))
        for s in range(2):
            w = weight(jnp.where(mine, *decays[s]), jnp.where(mine, *turns[s]), span)
            wa_ref[s, r] = w[0]
            wb_ref[s, r] = w[1]
        return total + elapsed(r)

    fold(1, n_sp, behind, none)
    outside = none

    def beyond(r, acc):
        return acc + elapsed(r) * jnp.where(sp - r >= 0, 0.0, 1.0)

    outside = fold(1, n_sp, beyond, none)
    from_start = [
        tuple(apply(weight(decays[s][d], turns[s][d], (inside, outside)[d]), init_of(s, d))
              for d in range(2))
        for s in range(2)
    ]

    drain_rows((rows * channels + cq_ref.size // 2) // width, one["rr"])
    drain(e_all.at[:, far], one["er"])
    for s in range(2):
        def combine(r, carry):
            h0, h1 = carry
            moved = apply((wa_ref[s, r], wb_ref[s, r]), e_all[s, r].astype(F32))
            mine = sp - r >= 0
            return h0 + jnp.where(mine, moved, 0.0), h1 + jnp.where(mine, 0.0, moved)

        entering = fold(1, n_sp, combine, from_start[s])
        for d in range(2):
            for q in range(channels // group // 2):
                hr, hi = entering[d][q:q + 1, :], entering[d][4 + q:5 + q, :]
                cr, ci = (cq_ref[s, part, d, q].astype(F32) for part in range(2))
                for part, value in ((0, cr * hr - ci * hi), (1, -(cr * hi + ci * hr))):
                    for side in range(2):
                        at = pl.ds((2 * q + side) * group, group)
                        lanes = pl.ds(part * states + d * half + q * 128, 128)
                        rc_ref[s, at, lanes] = jnp.where(
                            left if side == 0 else ~left, value, 0.0).astype(BF16)
    gated = []
    for s in range(2):
        full = response if s == 0 else rp_in[...].astype(F32)
        full = full + dot_t(p_row[s], rc_ref[s])
        inner = 0.7978845608028654 * (full + 0.044715 * (full * full * full))
        gated.append((0.5 * full * (1.0 + jnp.tanh(inner))).astype(BF16))
    state_out = jnp.concatenate(gated, axis=1)
    so_ref[...] = state_out
    state_copy = remote(so_ref, so_in, one["out"], one["sr"], {"tp": sib})
    state_copy.start()
    drain(ps_v.at[pl.ds(0, 2 * (channels - part_rows))], one["vr"])
    total = dot(state_out, ps_v[:2 * channels])
    drain_rows(2 * rows + direct_rows, one["pr"])
    base = acc_ref[...] + pi_ref[0].astype(F32) + pi_ref[1].astype(F32)
    total = total + jnp.concatenate(
        [base[inner_rows:inner_rows + edge], base[:direct_rows] + pd_ref[...].astype(F32),
         base[direct_rows:inner_rows], base[inner_rows + edge:]], axis=0)
    state_copy.wait_recv()
    out_ref[...] = (total + dot(so_in[...], ps_v[2 * channels:])).astype(BF16)

    pl.when(not_last)(halo_up.wait_send)
    pl.when(not_first)(halo_down.wait_send)
    sent = [(x_ref, 2), (x_full.at[0, pl.ds(0, last)], 1), (x_full.at[0, 0], 1), (po_ref, 1),
            (ps_v.at[pl.ds(0, channels + 2 * part_rows)], 1),
            (ps_v.at[pl.ds(0, 2 * (channels - part_rows))], 1), (cq_ref.at[0], 1), (rp_out, 1),
            (so_ref, 1)]
    count = sum(times * ref.size for ref, times in sent) // width
    drain_rows(count, one["out"])
    drain(par_ref.at[0], one["os"])
    drain(gains, one["gs"])
    drain(el_all.at[far], one["is"])
    drain(e_all.at[:, far], one["es"])


def per_device(
    n_sp, n_tp,
    stream, norm_gain, w_value, w_mix, w_gate, w_state, conv_taps, skip_gain, decay_rate, turn_rate,
    input_real, input_imag, read_real, read_imag, initial_state, intervals, proj_conv, proj_state,
):
    rows, width = stream.shape
    channels = w_value.shape[1]
    dirs, groups, per, group = input_real.shape
    states = dirs * groups * per
    cw = width // CHUNKS
    hbm = pl.BlockSpec(memory_space=pltpu.HBM)
    dma = lambda n: pltpu.SemaphoreType.DMA((n,))
    packed = pltpu.VMEM((rows * 8, 128), F32)
    rows_of = lambda m: jnp.swapaxes(m, 2, 3).reshape(dirs * groups * group, per)
    return pl.pallas_call(
        functools.partial(kernel, n_sp, n_tp),
        out_shape=jax.ShapeDtypeStruct((rows, width), BF16),
        in_specs=[hbm] * 18,
        out_specs=pl.BlockSpec(memory_space=pltpu.VMEM),
        scratch_shapes=[
            pltpu.VMEM((rows, width), BF16),
            pltpu.VMEM((1, width), F32),
            pltpu.VMEM(conv_taps.shape, F32),
            pltpu.VMEM((1, channels), F32),
            pltpu.VMEM((2, 4 * dirs * groups, per), F32),
            pltpu.SMEM((1, rows), F32),
            pltpu.VMEM((1, rows), F32),
            pltpu.VMEM((width * n_tp, 4 * channels), BF16),
            pltpu.VMEM((channels, width * n_tp), BF16),
            pltpu.VMEM((n_tp * channels, width), BF16),
            pltpu.VMEM((2, dirs * groups * group, per), F32),
            pltpu.VMEM((2, dirs * groups * group, per), F32),
            pltpu.VMEM((n_tp, CHUNKS, rows, cw), BF16),
            pltpu.VMEM((n_tp - 1, 1, width), F32),
            pltpu.VMEM((n_sp, 1, rows), F32),
            packed, packed, packed, packed, packed, packed, packed, packed, packed, packed,
            pltpu.VMEM((2, rows, states), F32),
            pltpu.VMEM((2, rows, 2 * states), BF16),
            pltpu.VMEM((2, channels, states), BF16),
            pltpu.VMEM((2, channels, states), BF16),
            pltpu.VMEM((2, channels, 2 * states), BF16),
            pltpu.VMEM((2, 2, dirs, groups // 2, group, 2 * per), BF16),
            pltpu.VMEM((rows, channels), BF16),
            pltpu.VMEM((2, 16, channels), BF16),
            pltpu.VMEM((2, 8, 128), F32),
            pltpu.VMEM((2, 8, 128), BF16),
            pltpu.VMEM((2, n_sp, 8, 128), BF16),
            pltpu.VMEM((n_sp, 1, 128), F32),
            pltpu.VMEM((2, n_sp, 8, 128), F32),
            pltpu.VMEM((2, n_sp, 8, 128), F32),
            pltpu.VMEM((3, rows, width), BF16),
            pltpu.VMEM((rows, width), BF16),
            pltpu.VMEM((2, rows, width), BF16),
            pltpu.VMEM((32, width), BF16),
            pltpu.VMEM((rows, width), F32),
            pltpu.VMEM((rows, 2 * channels), BF16),
            pltpu.VMEM((rows, 2 * channels), BF16),
            pltpu.VMEM((rows, channels), BF16),
            pltpu.VMEM((rows, channels), BF16),
            pltpu.VMEM((rows, width), BF16),
            dma(12), pltpu.SemaphoreType.DMA, dma(CHUNKS + 1), dma(n_tp - 1), dma(16), dma(2), dma(2), dma(2),
            pltpu.SemaphoreType.REGULAR((max(2, (n_sp - 1).bit_length()),)),
            pltpu.SemaphoreType.REGULAR,
        ],
        compiler_params=pltpu.CompilerParams(
            collective_id=0, has_side_effects=True, vmem_limit_bytes=48 * 1024 * 1024),
    )(*(pltpu.with_memory_space_constraint(a, pltpu.HBM) for a in (
        stream, norm_gain.reshape(1, width), w_value, w_mix, w_gate, w_state, conv_taps,
        skip_gain.reshape(1, channels),
        decay_rate.reshape(dirs * groups, per), turn_rate.reshape(dirs * groups, per),
        rows_of(input_real), rows_of(input_imag),
        read_real.reshape(dirs * groups * group, per), read_imag.reshape(dirs * groups * group, per),
        initial_state.reshape(dirs * 2 * groups, per), intervals.reshape(1, rows),
        proj_conv, proj_state,
    )))


def solution(mesh):
    return jax.shard_map(
        functools.partial(per_device, mesh.shape["sp"], mesh.shape["tp"]),
        mesh=mesh,
        in_specs=(
            P("sp", "tp"), P("tp"), P(None, "tp"), P(None, "tp"), P(None, "tp"), P(None, "tp"),
            P(None, "tp"), P("tp"), P(None, "tp", None), P(None, "tp", None),
            P(None, "tp", None, None), P(None, "tp", None, None), P(None, "tp", None, None),
            P(None, "tp", None, None), P(None, None, "tp", None), P("sp"), P("tp", None),
            P("tp", None),
        ),
        out_specs=P("sp", "tp"),
        check_vma=False,
    )
```
